128 devices in a mesh: sp: 16 (over z, x), tp: 8 (over y, core).
Axes of the slice: x: 4, y: 4, z: 4, core: 2. Of those that a mesh axis runs over, the one named last changes fastest.
Arguments:
- resid: bfloat16 [12288, 3072], P('sp', 'tp'), may hold values from -12 to 12
- query: bfloat16 [12288, 1536], P('sp', 'tp'), may hold values from -6 to 6
- keys: bfloat16 [12288, 1536], P('sp', 'tp'), may hold values from -6 to 6
- values: bfloat16 [12288, 1536], P('sp', 'tp'), may hold values from -6 to 6
- out_gate: bfloat16 [12288, 1536], P('sp', 'tp'), may hold values from -6 to 6
- in_gate: float32 [16, 12288], P('tp', 'sp'), may hold values from -6 to 110
- forget: float32 [16, 12288], P('tp', 'sp'), may hold values from -1 to 16
- doc_ids: int32 [12288], P('sp'), may hold values from 0 to 7, never falling along the last dimension, each value on 1 to 3072 neighbouring positions
- head_gain: float32 [1536], P('tp'), may hold values from 0.1 to 1.9
- w_out: bfloat16 [1536, 3072], P('tp'), may hold values from -0.15625 to 0.15625
- ffn_gain: float32 [3072], replicated, may hold values from 0.1 to 1.9
- w_gate: bfloat16 [3072, 8448], P('sp', 'tp'), may hold values from -0.109375 to 0.109375
- w_value: bfloat16 [3072, 8448], P('sp', 'tp'), may hold values from -0.109375 to 0.109375
- conv_taps: float32 [3, 8448], P(None, 'tp'), may hold values from -3.5 to 3.5
- w_down: bfloat16 [8448, 3072], P('tp', 'sp'), may hold values from -0.0625 to 0.0625
Outputs:
- layer_out: bfloat16 [12288, 3072], P('sp', 'tp')
The draws below stay inside these ranges and needn't reach their ends.
Inputs may be any that keep to these rules, and one draw needn't show every extreme that they name: `doc_ids`: document numbers never fall along the positions; each document is 1 to 3072 positions long.
All inputs are finite; a program needn't handle non-finite values.
Results may differ from the reference program's by a relative error of at most 0.02.
Values may be sent and summed in bfloat16 or wider, within the bound.
A program may use at most 128 MiB of HBM per device.

```python
import math
import jax
import jax.numpy as jnp
import numpy as np
from jax import lax

D = 3072
H = 16
DH = 96
FF = 8448
BLOCK = 64
TAPS = 3
TOK_DEV = 768
TOKENS = 12288
DOCS = 8
N_TP = 8


def draw_resid(key, part):
    base = jnp.clip(jax.random.normal(key, (TOKENS, D), jnp.float32), -6.0, 6.0)
    phase = jax.random.uniform(jax.random.fold_in(key, 1), (), jnp.float32, 0.0, 6.2832)
    columns = jnp.arange(D, dtype=jnp.float32)
    scale = 0.35 * jnp.exp(0.6 * jnp.sin(6.2832 * columns / D + phase))
    return (base * scale).astype(jnp.bfloat16)


def draw_in_gate(key, part):
    base = jnp.clip(jax.random.normal(key, (H, TOKENS), jnp.float32), -6.0, 6.0)
    return base


def draw_forget(key, part):
    limit = 4
    quick = jax.random.randint(jax.random.fold_in(key, 1), (H, 1), 0, 8) < limit
    rate = jnp.where(quick, 1.0 / 40.0, 1.0 / (4.0 * TOK_DEV))
    factor = jnp.exp(jax.random.uniform(jax.random.fold_in(key, 2), (H, TOKENS // 128), jnp.float32, -1.05, 1.05))
    factor = jnp.repeat(factor, 128, axis=1)
    noise = 0.5 * jnp.clip(jax.random.normal(jax.random.fold_in(key, 3), (H, TOKENS), jnp.float32), -6.0, 6.0)
    return -jnp.log(rate * factor) + noise


def steps_of(stream_key, extent, cuts, least, top_value):
    def one(position, blocks):
        draws = jax.random.uniform(jax.random.fold_in(jax.random.fold_in(stream_key, 6), position), (blocks,), jnp.float32, least / len(cuts), top_value / len(cuts))
        return jnp.repeat(jnp.exp(draws), extent[position] // blocks).reshape((-1,) + (1,) * (len(extent) - position - 1))

    gain = one(*cuts[0])
    for cut in cuts[1:]:
        gain = gain * one(*cut)
    return gain


def length_profile(count, total, most, skew):
    loads = [(1 << 20) // math.isqrt(rank ** skew) + 1 for rank in range(2, count + 1)]
    spare, counts = total - most - (count - 1), [1] * (count - 1)
    while spare > 0:
        free = [i for i in range(count - 1) if counts[i] < most]
        mass, remaining = sum([loads[i] for i in free]), spare
        for i in free:
            addition = min(most - counts[i], max(1, remaining * loads[i] // mass), spare)
            counts[i] = counts[i] + addition
            spare = spare - addition
    return np.array([most] + counts)


def uneven(stream_key, amount, total, reach, skew):
    if amount == 2:
        one = jax.random.randint(stream_key, (), max(1, total - reach), min(reach, total - 1) + 1)
        return jnp.stack([one, total - one])
    sizes = jnp.asarray(length_profile(amount, total, reach, skew), jnp.int32)
    pairs = (amount - 1) // 2
    giver, taker = sizes[1:1 + 2 * pairs:2], sizes[2:2 + 2 * pairs:2]
    margin = jnp.minimum(giver - 1, reach - taker)
    moved = jax.random.randint(jax.random.fold_in(stream_key, 1), (pairs,), 0, 1 << 20) % (margin + 1)
    sizes = sizes.at[1:1 + 2 * pairs:2].set(giver - moved).at[2:2 + 2 * pairs:2].set(taker + moved)
    return sizes[jax.random.permutation(jax.random.fold_in(stream_key, 2), amount)]


def centred(rng, dims, scale, most, shards=(), held_as=jnp.bfloat16):
    gain = steps_of(rng, dims, shards, -0.22, 0.18) if shards else 1.0
    entries = jax.random.normal(rng, dims, jnp.float32) * scale * gain
    return jnp.minimum(jnp.maximum(entries, -most), most).astype(held_as)


def setup_inputs(seed: int = 0) -> dict:
    splits = jax.random.split(jax.random.key(seed), 16)
    return {
        "resid": draw_resid(jax.random.fold_in(splits[15], 71), 0),
        "query": centred(splits[1], (TOKENS, H * DH), 1.0, 6.0, ((0, 16), (1, 8))),
        "keys": centred(splits[2], (TOKENS, H * DH), 1.0, 6.0, ((0, 16), (1, 8))),
        "values": centred(splits[3], (TOKENS, H * DH), 1.0, 6.0, ((0, 16), (1, 8))),
        "out_gate": centred(splits[4], (TOKENS, H * DH), 1.0, 6.0, ((0, 16), (1, 8))),
        "in_gate": draw_in_gate(jax.random.fold_in(splits[15], 71), 0),
        "forget": draw_forget(jax.random.fold_in(splits[15], 71), 0),
        "doc_ids": jnp.searchsorted(jnp.cumsum(uneven(splits[7], DOCS, TOKENS, 4 * TOK_DEV, 0)), jnp.arange(TOKENS), side="right").astype(jnp.int32),
        "head_gain": jnp.clip(1.0 + 0.18 * jax.random.normal(splits[8], (H * DH,), jnp.float32), 0.1, 1.9),
        "w_out": centred(splits[9], (H * DH, D), (H * DH) ** -0.5, 0.15625, ((0, 8),)),
        "ffn_gain": jnp.clip(1.0 + 0.18 * jax.random.normal(splits[10], (D,), jnp.float32), 0.1, 1.9),
        "w_gate": centred(splits[11], (D, FF), D ** -0.5, 0.109375, ((0, 16), (1, 8))),
        "w_value": centred(splits[12], (D, FF), D ** -0.5, 0.109375, ((0, 16), (1, 8))),
        "conv_taps": centred(splits[13], (TAPS, FF), TAPS ** -0.5, 3.5, ((1, 8),), jnp.float32),
        "w_down": centred(splits[14], (FF, D), FF ** -0.5, 0.0625, ((0, 8), (1, 16))),
    }


ABSENT = -1e+30
epsilon = 1e-06
head_floor = 1.0
HIGHEST = lax.Precision.HIGHEST

def combine(early, late):
    state_early, peak_early, decay_early, first_early, last_early, second_early = early
    state_late, peak_late, decay_late, first_late, last_late, second_late = late
    early_empty = last_early < 0.0
    late_empty = first_late < 0.0
    cut = (first_late != last_early) & jnp.logical_not(early_empty) & jnp.logical_not(late_empty)
    passed = jnp.where(cut, ABSENT, decay_late)
    peak = jnp.maximum(passed + peak_early, peak_late)
    keep = jnp.exp(passed + peak_early - peak)
    fresh = jnp.exp(peak_late - peak)
    state = keep[..., None, None] * state_early + fresh[..., None, None] * state_late
    return (state, peak, decay_early + passed, jnp.where(early_empty, first_late, first_early), jnp.where(late_empty, last_early, last_late), jnp.where(late_empty, second_early, second_late))

def empty_state(heads, width):
    return (jnp.zeros((heads, width, width), jnp.float32), jnp.full((heads,), ABSENT, jnp.float32), jnp.zeros((heads,), jnp.float32), jnp.full((1,), -1.0, jnp.float32), jnp.full((1,), -1.0, jnp.float32), jnp.full((1,), -1.0, jnp.float32))

def advance(carry, item):
    return (combine(carry, item), carry)

def block_parts(query, keys, values, in_gate, forget, seg):
    length, heads, width = query.shape
    count = length // BLOCK
    query_blocks = query.reshape(count, BLOCK, heads, width)
    key_blocks = (keys * width ** (-0.5)).reshape(count, BLOCK, heads, width)
    value_blocks = values.reshape(count, BLOCK, heads, width)
    gate_in = in_gate.T.reshape(count, BLOCK, heads)
    cumul = jnp.cumsum(jax.nn.log_sigmoid(forget.T).reshape(count, BLOCK, heads), axis=1)
    seg_blocks = seg.reshape(count, BLOCK)
    total = cumul[:, -1]
    in_last = (seg_blocks == seg_blocks[:, -1:])[:, :, None]
    weight_log = jnp.where(in_last, total[:, None] - cumul + gate_in, ABSENT)
    local_peak = lax.optimization_barrier(jnp.max(weight_log, axis=1))
    weights = jnp.exp(weight_log - local_peak[:, None])
    update = jnp.einsum('nchk,nchv->nhkv', weights[..., None] * key_blocks, value_blocks, precision=HIGHEST)
    whole = jnp.all(seg_blocks == seg_blocks[:, :1], axis=1)[:, None]
    decay = jnp.where(whole, total, ABSENT)
    elements = (update, local_peak, decay, seg_blocks[:, :1], seg_blocks[:, -1:], seg_blocks[:, -2:-1])
    return (elements, (query_blocks, key_blocks, value_blocks, gate_in, cumul, seg_blocks))

def block_outputs(before, parts):
    state, peak_prev, _, _, last_prev, _ = before
    query_blocks, key_blocks, value_blocks, gate_in, cumul, seg_blocks = parts
    count, span, heads, width = query_blocks.shape
    carried = (seg_blocks == last_prev)[:, :, None]
    inter = jnp.where(carried, cumul + peak_prev[:, None], ABSENT)
    places = jnp.arange(span)
    causal = (places[:, None] >= places[None, :])[None, :, :, None]
    same = (seg_blocks[:, :, None] == seg_blocks[:, None, :])[..., None]
    diff_log = jnp.where(causal & same, cumul[:, :, None] - cumul[:, None] + gate_in[:, None], ABSENT)
    top = jnp.maximum(inter, lax.optimization_barrier(jnp.max(diff_log, axis=2)))
    scores = jnp.einsum('nthd,nshd->ntsh', query_blocks, key_blocks, precision=HIGHEST) * jnp.exp(diff_log - top[:, :, None])
    result = jnp.einsum('ntsh,nshd->nthd', scores, value_blocks, precision=HIGHEST)
    result = result + jnp.exp(inter - top)[..., None] * jnp.einsum('nthk,nhkv->nthv', query_blocks, state, precision=HIGHEST)
    return result.reshape(count * span, heads, width)

def reference(resid, query, keys, values, out_gate, in_gate, forget, doc_ids, head_gain, w_out, ffn_gain, w_gate, w_value, conv_taps, w_down):
    length = query.shape[0]
    seg = doc_ids.astype(jnp.float32)
    query_f = query.astype(jnp.float32).reshape(length, H, DH)
    keys_f = keys.astype(jnp.float32).reshape(length, H, DH)
    values_f = values.astype(jnp.float32).reshape(length, H, DH)
    elements, parts = block_parts(query_f, keys_f, values_f, in_gate, forget, seg)
    _, before = lax.scan(advance, empty_state(H, DH), elements)
    memory_out = block_outputs(before, parts)
    normed = memory_out * lax.rsqrt(lax.optimization_barrier(jnp.mean(memory_out * memory_out, axis=-1, keepdims=True)) + head_floor)
    normed = normed.reshape(length, H * DH) * head_gain * jax.nn.sigmoid(out_gate.astype(jnp.float32))
    mix = normed.astype(jnp.bfloat16)
    width_group = H // N_TP * DH
    attended = jnp.zeros((length, D), jnp.float32)
    for index in range(N_TP):
        share = jnp.dot(mix[:, index * width_group:(index + 1) * width_group], w_out[index * width_group:(index + 1) * width_group], preferred_element_type=jnp.float32).astype(jnp.bfloat16)
        attended = attended + lax.optimization_barrier(share).astype(jnp.float32)
    residual_one = resid.astype(jnp.float32) + attended
    scale = lax.rsqrt(lax.optimization_barrier(jnp.mean(residual_one * residual_one, axis=1, keepdims=True)) + epsilon)
    normed_rows = (residual_one * scale * ffn_gain).astype(jnp.bfloat16)
    gate = jnp.dot(normed_rows, w_gate, preferred_element_type=jnp.float32).astype(jnp.bfloat16)
    value = jnp.dot(normed_rows, w_value, preferred_element_type=jnp.float32).astype(jnp.bfloat16)
    extended = jnp.concatenate([jnp.zeros((2, FF), jnp.bfloat16), gate], axis=0).astype(jnp.float32)
    ids = jnp.concatenate([jnp.full((2,), -1.0, jnp.float32), seg])
    near = (ids[1:-1] == seg)[:, None]
    far = (ids[:-2] == seg)[:, None]
    conv = conv_taps[2] * extended[2:] + conv_taps[1] * jnp.where(near, extended[1:-1], 0.0) + conv_taps[0] * jnp.where(far, extended[:-2], 0.0)
    hidden = (jax.nn.silu(conv) * value.astype(jnp.float32)).astype(jnp.bfloat16)
    group = FF // N_TP
    down = jnp.zeros((length, D), jnp.float32)
    for index in range(N_TP):
        partial_rows = jnp.dot(hidden[:, index * group:(index + 1) * group], w_down[index * group:(index + 1) * group], preferred_element_type=jnp.float32).astype(jnp.bfloat16)
        down = down + lax.optimization_barrier(partial_rows).astype(jnp.float32)
    return (residual_one + down).astype(jnp.bfloat16)
```

```python
import jax
import jax.numpy as jnp
from jax import lax
from jax.experimental import pallas as pl
from jax.experimental.pallas import tpu as pltpu
from jax.sharding import Mesh
from jax.sharding import PartitionSpec as P

MESH = pl.DeviceIdType.MESH
F32 = jnp.float32
BF16 = jnp.bfloat16
ABSENT = -1e30
DH = 96
TOK = 768
OWN = 384
HW = 192
MAIN = 1024
GW = 1152
LANES = 3200
DOWN0 = 2176
EPS = 1e-6
SEMS = 160

GATE_P = dict(rows=(0, 192), lanes=(0, GW), cut=(96, 96), first="x")
VALUE_P = dict(rows=(0, 192), lanes=(GW, MAIN), cut=(96, 96), first="z")
DOWN_A = dict(rows=(0, 96), lanes=(DOWN0, MAIN), cut=(48, 48), first="x")
DOWN_B = dict(rows=(96, 96), lanes=(DOWN0, MAIN), cut=(48, 48), first="z")


def mod4(v):
    return lax.rem(v + 8, 4)


def dot(a, b, **kw):
    return lax.dot_general(a, b, (((1,), (0,)), ((), ())), preferred_element_type=F32, **kw)


def dot_t(a, b, **kw):
    return lax.dot_general(a, b, (((1,), (1,)), ((), ())), preferred_element_type=F32, **kw)


def kernel(
    pk,
    q_ref,
    k_ref,
    v_ref,
    og_ref,
    gates_ref,
    wo_ref,
    resid_ref,
    hg_ref,
    gain_ref,
    taps_ref,
    out_ref,
    W,
    X,
    MIX,
    WO,
    VP,
    OI,
    MF,
    NF,
    ST,
    SR,
    SS,
    RES,
    GT,
    EDGE,
    HD,
    SP,
    RP,
    PO,
    ZS,
    RL,
    RV,
    ssem,
    rsem,
    lsem,
):
    z, x = lax.axis_index("z"), lax.axis_index("x")
    y, c = lax.axis_index("y"), lax.axis_index("c")
    sp = z * 4 + x
    tp = y * 2 + c
    o = 1 - c
    table = {}
    started = []

    def slot(key):
        return table.setdefault(key, len(table))

    def send(key, src, dst, dev):
        i = slot(key)
        d = pltpu.make_async_remote_copy(
            src_ref=src,
            dst_ref=dst,
            send_sem=ssem.at[i],
            recv_sem=rsem.at[i],
            device_id=dev,
            device_id_type=MESH,
        )
        d.start()
        started.append(d)

    def recv(key, dst):
        i = slot(key)
        pltpu.make_async_remote_copy(
            src_ref=dst,
            dst_ref=dst,
            send_sem=ssem.at[i],
            recv_sem=rsem.at[i],
            device_id=(z, x, y, o),
            device_id_type=MESH,
        ).wait_recv()

    def at_sp(n):
        s = lax.rem(sp + n + 16, 16)
        return (s // 4, lax.rem(s, 4), y, c)

    def at_x(d):
        return (z, mod4(x + d), y, c)

    def at_z(d):
        return (mod4(z + d), x, y, c)

    def at_y(d):
        return (z, x, mod4(y + d), c)

    def at_tp(n):
        t = lax.rem(tp + n, 8)
        return (z, x, t // 2, lax.rem(t, 2))

    partner = (z, x, y, o)

    peers = [at_x(1), at_x(-1), at_z(1), at_z(-1)]
    peers += [at_tp(n) for n in range(1, 8)]
    peers += [at_sp(n) for n in (1, 2, 3, -1, -2, -3)]
    barrier = pltpu.get_barrier_semaphore()
    for dev in peers:
        pl.semaphore_signal(barrier, inc=1, device_id=dev, device_id_type=MESH)
    pl.semaphore_wait(barrier, len(peers))

    def place(part, dp, ds, half=None):
        if part["first"] == "x":
            zz, xx = mod4(z + ds), mod4(x + dp)
        else:
            zz, xx = mod4(z + dp), mod4(x + ds)
        r0, nr = part["rows"]
        if half is not None:
            r0, nr = r0 + (part["cut"][0] if half else 0), part["cut"][half]
        row = pl.multiple_of((zz * 4 + xx) * HW + r0, 16)
        l0, nl = part["lanes"]
        return W.at[pl.ds(row, nr), pl.ds(l0, nl)]

    def stage(name, part):
        first = part["first"] == "x"
        prim = at_x if first else at_z
        secd = at_z if first else at_x
        steps = (0, -1, 1, 2)

        def own():
            r0, nr = part["rows"]
            l0, nl = part["lanes"]
            src = pk.at[pl.ds(r0, nr), pl.ds(l0, nl)]
            dst = place(part, 0, 0)
            for d in (1, -1):
                send((name, "p", d), src, dst, prim(d))
            for d in (1, -1):
                send((name, "s", d, 0), src, dst, secd(d))

        def second(m):
            dst = place(part, steps[m], 0)
            for d in (1, -1):
                send((name, "s", d, m), dst, dst, secd(d))

        def e1():
            for d in (1, -1):
                recv((name, "p", d), place(part, -d, 0))
                half = 0 if d == 1 else 1
                piece = place(part, -d, 0, half)
                send((name, "pf", d), piece, piece, prim(d))
            second(1)
            second(2)

        def across(m):
            for d in (1, -1):
                recv((name, "s", d, m), place(part, steps[m], -d))
                half = 0 if d == 1 else 1
                piece = place(part, steps[m], -d, half)
                send((name, "sf", d, m), piece, piece, secd(d))

        def e3():
            for d in (1, -1):
                recv((name, "pf", d), place(part, 2, 0, 0 if d == 1 else 1))
            second(3)

        def e7():
            for m in range(4):
                for d in (1, -1):
                    recv((name, "sf", d, m), place(part, steps[m], 2, 0 if d == 1 else 1))

        return [own, e1, lambda: across(0), e3, lambda: across(1), lambda: across(2), lambda: across(3), e7]

    def pair(a, b):
        return [lambda f=f, g=g: (f(), g()) for f, g in zip(a, b)]

    gv = pair(stage("g", GATE_P), stage("v", VALUE_P))
    dn = pair(stage("da", DOWN_A), stage("db", DOWN_B))

    def over_tp(name, blk):
        def g0():
            b = blk(y, c)
            send((name, "o"), b, b, partner)
            for d in (1, -1):
                send((name, "y", d), b, b, at_y(d))

        def g1():
            for d in (1, -1):
                src = mod4(y - d)
                recv((name, "y", d), blk(src, c))
                h = blk(src, c, 0 if d == 1 else 1)
                send((name, "f", d), h, h, at_y(d))
                send((name, "of", d), blk(src, c), blk(src, c), partner)

        def g2():
            far = mod4(y + 2)
            for d in (1, -1):
                h = blk(far, c, 0 if d == 1 else 1)
                recv((name, "f", d), h)
                send((name, "oh", d), h, h, partner)

        def g3():
            far = mod4(y + 2)
            recv((name, "o"), blk(y, o))
            for d in (1, -1):
                recv((name, "of", d), blk(mod4(y - d), o))
                recv((name, "oh", d), blk(far, o, 0 if d == 1 else 1))

        return g0, g1, g2, g3

    def block_of(ref, width):
        def blk(yy, cc, half=None):
            rows = slice(None) if half is None else pl.ds(half * OWN, OWN)
            return ref.at[rows, pl.ds(pl.multiple_of((yy * 2 + cc) * width, 128), width)]

        return blk

    mix_g = over_tp("m", block_of(MIX, 256))
    x_g = over_tp("x", block_of(X, OWN))

    gv[0]()
    for n in range(1, 8):
        t = lax.rem(tp + n, 8)
        src = wo_ref.at[:, pl.ds(pl.multiple_of(t * OWN, 128), OWN)]
        dst = WO.at[pl.ds(pl.multiple_of(tp * 256, 16), HW), :]
        send(("w", n), src, dst, at_tp(n))
    local_w = pltpu.make_async_copy(
        pk, W.at[pl.ds(pl.multiple_of(sp * HW, 16), HW), :], lsem.at[0]
    )
    local_w.start()
    local_o = pltpu.make_async_copy(
        wo_ref.at[:, pl.ds(pl.multiple_of(tp * OWN, 128), OWN)],
        WO.at[pl.ds(pl.multiple_of(tp * 256, 16), HW), :],
        lsem.at[1],
    )
    local_o.start()
    for j in range(8):
        WO[j * 256 + HW : (j + 1) * 256, :] = jnp.zeros((64, OWN), BF16)

    gates = gates_ref[...]
    lane = lax.broadcasted_iota(jnp.int32, (8, TOK), 1)
    row8 = lax.broadcasted_iota(jnp.int32, (8, TOK), 0)
    e = jnp.exp(-jnp.abs(gates))
    log1p = jnp.where(e < 1e-2, e * (1.0 - e * (0.5 - e * (1.0 / 3.0))), jnp.log(1.0 + e))
    cum = jnp.minimum(gates, 0.0) - log1p
    shift = 1
    while shift < TOK:
        cum = cum + jnp.where(lane >= shift, pltpu.roll(cum, shift, 1), 0.0)
        shift *= 2
    seg = gates[4:5]
    b = [gates[h : h + 1] - cum[2 + h : 3 + h] for h in range(2)]
    end = [cum[2 + h : 3 + h, TOK - 1 :] for h in range(2)]
    first, last, second_last = seg[:, :1], seg[:, TOK - 1 :], seg[:, TOK - 2 : TOK - 1]
    rows = jnp.where(row8 == 0, b[0], jnp.where(row8 == 1, b[1], seg))
    cols = jnp.transpose(jnp.concatenate([rows, jnp.zeros((120, TOK), F32)], axis=0))
    seg_c = cols[:, 2:3]
    lane256 = lax.broadcasted_iota(jnp.int32, (TOK, 256), 1)
    in0 = lane256 < DH
    in1 = (lane256 >= DH) & (lane256 < HW)

    VP[...] = jnp.zeros_like(VP)
    VP[:, 0:HW] = v_ref[...]
    keys = k_ref[...]
    lane_k = lax.broadcasted_iota(jnp.int32, (TOK, HW), 1)
    zero_k = jnp.zeros_like(keys)
    key_h = [jnp.where(lane_k < DH, keys, zero_k), jnp.where(lane_k < DH, zero_k, keys)]
    peak = []
    weight = []
    for h in range(2):
        top = jnp.max(jnp.where(seg == last, b[h], ABSENT), axis=1, keepdims=True)
        peak.append(top)
        weight.append(jnp.where(seg_c == last, jnp.exp(jnp.minimum(cols[:, h : h + 1] - top, 0.0)), 0.0))
    scaled = keys.astype(F32) * (jnp.where(lane_k < DH, weight[0], weight[1]) * DH**-0.5)
    state = lax.dot_general(
        scaled.astype(BF16), VP[...], (((0,), (0,)), ((), ())), preferred_element_type=F32
    )
    r192 = lax.broadcasted_iota(jnp.int32, (HW, 128), 0)
    l192 = lax.broadcasted_iota(jnp.int32, (HW, 128), 1)
    folded = jnp.where(r192 < DH, state[:, :128], pltpu.roll(state, 256 - DH, 1)[:, :128])
    ST[0:HW, :] = jnp.where(l192 < DH, folded, 0.0)
    meta_row = lax.broadcasted_iota(jnp.int32, (8, 128), 0)
    meta = jnp.zeros((8, 128), F32)
    for n, value in enumerate((end[0] + peak[0], end[1] + peak[1], end[0], end[1], first, last, second_last)):
        meta = jnp.where(meta_row == n, value, meta)
    ST[HW : HW + 8, :] = meta
    for n in range(1, 5):
        send(("st", n), ST, SR.at[n - 1], at_sp(n))

    for i in range(3):
        t0, ns = i * 256, (i + 1) * 256
        qb = q_ref[t0 : t0 + 256, :]
        s_at = lax.broadcasted_iota(jnp.int32, (256, ns), 1)
        t_at = lax.broadcasted_iota(jnp.int32, (256, ns), 0) + t0
        mask = (seg_c[t0 : t0 + 256] == seg[:, :ns]) & (s_at <= t_at)
        parts, tops = [], []
        for h in range(2):
            masked = jnp.where(mask, b[h][:, :ns], ABSENT)
            top = jnp.max(masked, axis=1, keepdims=True)
            scores = dot_t(qb, key_h[h][:ns]) * (jnp.exp(masked - top) * DH**-0.5)
            parts.append(dot(scores.astype(BF16), VP[0:ns, :]))
            tops.append(top)
        left = in0[t0 : t0 + 256]
        OI[t0 : t0 + 256, :] = jnp.where(left, parts[0], parts[1])
        MF[t0 : t0 + 256, :] = jnp.where(left, tops[0], tops[1])

    gv[1]()

    dec = [jnp.zeros((1, 128), F32)] * 2
    cand = [[], []]
    first_l = jnp.broadcast_to(first, (1, 128))
    for n in range(1, 5):
        recv(("st", n), SR.at[n - 1])
        m = SR[n - 1, HW : HW + 8, :]
        valid = (m[5:6] == first_l) & (sp >= n)
        for h in range(2):
            cand[h].append(jnp.where(valid, m[h : h + 1] + dec[h], ABSENT))
            dec[h] = dec[h] + m[2 + h : 3 + h]
    pin = [jnp.maximum(jnp.maximum(p[0], p[1]), jnp.maximum(p[2], p[3])) for p in cand]
    carried = jnp.zeros((HW, 128), F32)
    for n in range(4):
        f = [jnp.exp(cand[h][n] - pin[h]) for h in range(2)]
        carried = carried + jnp.where(r192 < DH, f[0], f[1]) * SR[n, 0:HW, :]
    wide = jnp.concatenate([carried, jnp.zeros((HW, 128), F32)], axis=1)
    r256 = lax.broadcasted_iota(jnp.int32, (HW, 256), 0)
    spread = jnp.where(r256 < DH, wide, pltpu.roll(wide, DH, 1)).astype(BF16)
    inter = dot(q_ref[...], spread)
    pin_l = jnp.where(in0, pin[0][:, :1], pin[1][:, :1])
    pin_t = jnp.where(seg_c == first, pin_l, ABSENT)
    top = jnp.maximum(MF[...], pin_t)
    memory = jnp.exp(MF[...] - top) * OI[...] + jnp.exp(pin_t - top) * inter
    square = memory * memory
    mean0 = jnp.sum(jnp.where(in0, square, 0.0), axis=1, keepdims=True) * (1.0 / DH)
    mean1 = jnp.sum(jnp.where(in1, square, 0.0), axis=1, keepdims=True) * (1.0 / DH)
    normed = memory * lax.rsqrt(jnp.where(in0, mean0, mean1) + 1.0)
    mix = normed[:, :HW] * hg_ref[...] * jax.nn.sigmoid(og_ref[...].astype(F32))
    own_mix = pl.multiple_of(tp * 256, 128)
    MIX[:, pl.ds(own_mix, 256)] = jnp.zeros((TOK, 256), BF16)
    VP[:, 0:HW] = mix.astype(BF16)
    MIX[:, pl.ds(own_mix, 256)] = VP[...]
    mix_g[0]()

    before = SR[0, HW : HW + 8, :]
    there = sp >= 1
    last_before = jnp.where(there, before[5:6, :1], -1.0)
    second_before = jnp.where(there, before[6:7, :1], -1.0)
    one_back = jnp.where(lane == 0, last_before, pltpu.roll(gates, 1, 1))[4:5]
    two_back = jnp.where(
        lane == 0, second_before, jnp.where(lane == 1, last_before, pltpu.roll(gates, 2, 1))
    )[4:5]
    flags = jnp.where(
        row8 == 0, jnp.where(one_back == seg, 1.0, 0.0), jnp.where(two_back == seg, 1.0, 0.0)
    )
    NF[...] = jnp.transpose(jnp.concatenate([flags, jnp.zeros((120, TOK), F32)], axis=0))

    gv[2]()
    gv[3]()
    mix_g[1]()
    mix_g[2]()
    gv[4]()
    mix_g[3]()

    local_o.wait()
    for n in range(1, 8):
        t = lax.rem(tp + 8 - n, 8)
        recv(("w", n), WO.at[pl.ds(pl.multiple_of(t * 256, 16), HW), :])
    gain = gain_ref[:, pl.ds(pl.multiple_of(tp * OWN, 128), OWN)]
    res = resid_ref[...].astype(F32) + dot(MIX[...], WO[...])
    RES[...] = res
    X[:, pl.ds(pl.multiple_of(tp * OWN, 128), OWN)] = (res * gain).astype(BF16)
    SS[tp] = dot_t(jnp.ones((8, OWN), F32), res * res, precision=lax.Precision.HIGHEST)
    x_g[0]()
    for n in range(1, 8):
        send(("q", n), SS.at[tp], SS.at[tp], at_tp(n))
    gv[5]()
    x_g[1]()
    gv[6]()
    dn[0]()
    x_g[2]()
    x_g[3]()
    total = SS[tp]
    for n in range(1, 8):
        t = lax.rem(tp + 8 - n, 8)
        recv(("q", n), SS.at[t])
        total = total + SS[t]
    scale_row = lax.rsqrt(total * (1.0 / 3072.0) + EPS)
    OI[:, 0:128] = jnp.transpose(jnp.concatenate([scale_row, jnp.zeros((120, TOK), F32)], axis=0))
    local_w.wait()
    gv[7]()
    dn[1]()

    scale = OI[:, 0:1]

    def gate_tile(n, _):
        l = pl.ds(pl.multiple_of(n * 256, 256), 256)
        GT[:, l] = (dot(X[...], W[:, l]) * scale).astype(BF16)
        return 0

    lax.fori_loop(0, 4, gate_tile, 0)
    GT[:, MAIN:GW] = (dot(X[...], W[:, MAIN:GW]) * scale).astype(BF16)
    send(("e",), GT.at[TOK - 16 : TOK, :], EDGE, at_sp(1))
    dn[2]()
    dn[3]()

    def hidden_of(lanes, width, value):
        g = GT[:, lanes].astype(F32)
        edge = EDGE[:, lanes].astype(F32)
        taps = taps_ref[:, lanes]
        t_at = lax.broadcasted_iota(jnp.int32, (TOK, width), 0)
        near = NF[:, 0:1] > 0.5
        far = NF[:, 1:2] > 0.5
        g1 = jnp.where(t_at == 0, edge[15:16], pltpu.roll(g, 1, 0))
        g2 = jnp.where(
            t_at == 0, edge[14:15], jnp.where(t_at == 1, edge[15:16], pltpu.roll(g, 2, 0))
        )
        conv = taps[2:3] * g + taps[1:2] * jnp.where(near, g1, 0.0) + taps[0:1] * jnp.where(far, g2, 0.0)
        return conv / (1.0 + jnp.exp(-conv)) * value

    recv(("e",), EDGE)

    def value_tile(n, _):
        l = pl.ds(pl.multiple_of(n * 256, 256), 256)
        w = pl.ds(pl.multiple_of(n * 256 + GW, 128), 256)
        value = (dot(X[...], W[:, w]) * scale).astype(BF16).astype(F32)
        HD[:, l] = hidden_of(l, 256, value).astype(BF16)
        return 0

    lax.fori_loop(0, 4, value_tile, 0)
    tail = slice(MAIN, GW)
    value_tail = pltpu.roll(GT[:, tail].astype(F32), 96, 1)
    HD[:, tail] = pltpu.roll(hidden_of(tail, 128, value_tail), 64, 1).astype(BF16)
    dn[4]()
    dn[5]()
    dn[6]()
    dn[7]()

    def partial(yy, cc):
        r = pl.ds(pl.multiple_of((yy * 2 + cc) * OWN, 128), OWN)
        return dot_t(HD[:, 0:MAIN], W[r, DOWN0:LANES]) + dot_t(HD[:, MAIN:GW], W[r, MAIN:GW])

    order = (2, 1, -1, 0)
    for n, d in enumerate(order):
        yy = mod4(y + d)
        SP[n] = partial(yy, o).astype(BF16)
        send(("sp", n), SP.at[n], RP.at[n], partner)
        PO[n % 2] = partial(yy, c)
        recv(("sp", n), RP.at[n])
        both = PO[n % 2] + RP[n].astype(F32)
        if d == 2:
            ZS[0] = both.astype(BF16)
            send(("rl", 1), ZS.at[0, pl.ds(0, OWN), :], RL.at[0], at_y(1))
            send(("rl", -1), ZS.at[0, pl.ds(OWN, OWN), :], RL.at[1], at_y(-1))
        elif d == 0:
            RES[...] = RES[...] + both
        else:
            k = 1 if d == 1 else 2
            free = OWN if d == 1 else 0
            ZS[k] = both.astype(BF16)
            PO[2 + (k - 1)] = both
            send(("rv", d), ZS.at[k, pl.ds(free, OWN), :], RV.at[k - 1, pl.ds(free, OWN), :], at_y(d))
    for d in (1, -1):
        k = 1 if d == 1 else 2
        held = OWN - (OWN if d == 1 else 0)
        recv(("rl", d), RL.at[k - 1])
        r = pl.ds(held, OWN)
        ZS[3, r, :] = (PO[2 + (k - 1), r, :] + RL[k - 1].astype(F32)).astype(BF16)
        send(("rw", d), ZS.at[3, r, :], RV.at[k - 1, r, :], at_y(d))
    for d in (1, -1):
        k = 1 if d == 1 else 2
        free = OWN if d == 1 else 0
        recv(("rv", d), RV.at[k - 1, pl.ds(free, OWN), :])
        recv(("rw", d), RV.at[k - 1, pl.ds(OWN - free, OWN), :])
    out_ref[...] = (RES[...] + RV[0].astype(F32) + RV[1].astype(F32)).astype(BF16)
    for d in started:
        d.wait_send()


def body(
    resid,
    query,
    keys,
    values,
    out_gate,
    in_gate,
    forget,
    doc_ids,
    head_gain,
    w_out,
    ffn_gain,
    w_gate,
    w_value,
    conv_taps,
    w_down,
):
    wd = w_down.T
    packed = jnp.concatenate(
        [
            w_gate,
            w_value[:, MAIN:],
            wd[:, MAIN:],
            jnp.zeros((HW, 32), BF16),
            w_value[:, :MAIN],
            wd[:, :MAIN],
        ],
        axis=1,
    )
    seg = doc_ids.astype(F32)[None]
    gates = jnp.concatenate([in_gate, forget, seg, jnp.zeros((3, TOK), F32)], axis=0)
    taps = jnp.pad(conv_taps, ((0, 0), (0, GW - conv_taps.shape[1])))
    vmem = pl.BlockSpec(memory_space=pltpu.VMEM)
    hbm = pl.BlockSpec(memory_space=pl.ANY)
    return pl.pallas_call(
        kernel,
        out_shape=jax.ShapeDtypeStruct((TOK, OWN), BF16),
        in_specs=[hbm, vmem, vmem, vmem, vmem, vmem, hbm, vmem, vmem, vmem, vmem],
        out_specs=vmem,
        scratch_shapes=[
            pltpu.VMEM((3072, LANES), BF16),
            pltpu.VMEM((TOK, 3072), BF16),
            pltpu.VMEM((TOK, 2048), BF16),
            pltpu.VMEM((2048, OWN), BF16),
            pltpu.VMEM((TOK, 256), BF16),
            pltpu.VMEM((TOK, 256), F32),
            pltpu.VMEM((TOK, 256), F32),
            pltpu.VMEM((TOK, 128), F32),
            pltpu.VMEM((200, 128), F32),
            pltpu.VMEM((4, 200, 128), F32),
            pltpu.VMEM((8, 8, TOK), F32),
            pltpu.VMEM((TOK, OWN), F32),
            pltpu.VMEM((TOK, GW), BF16),
            pltpu.VMEM((16, GW), BF16),
            pltpu.VMEM((TOK, GW), BF16),
            pltpu.VMEM((4, TOK, OWN), BF16),
            pltpu.VMEM((4, TOK, OWN), BF16),
            pltpu.VMEM((4, TOK, OWN), F32),
            pltpu.VMEM((4, TOK, OWN), BF16),
            pltpu.VMEM((2, OWN, OWN), BF16),
            pltpu.VMEM((2, TOK, OWN), BF16),
            pltpu.SemaphoreType.DMA((SEMS,)),
            pltpu.SemaphoreType.DMA((SEMS,)),
            pltpu.SemaphoreType.DMA((2,)),
        ],
        compiler_params=pltpu.CompilerParams(
            collective_id=0, has_side_effects=True, vmem_limit_bytes=63 * 1024 * 1024
        ),
    )(
        packed,
        query,
        keys,
        values,
        out_gate,
        gates,
        w_out,
        resid,
        head_gain[None],
        ffn_gain[None],
        taps,
    )


def solution(mesh):
    torus = Mesh(mesh.devices.reshape(4, 4, 4, 2), ("z", "x", "y", "c"))
    sp, tp = ("z", "x"), ("y", "c")
    placed = (
        P(sp, tp),
        P(sp, tp),
        P(sp, tp),
        P(sp, tp),
        P(sp, tp),
        P(tp, sp),
        P(tp, sp),
        P(sp),
        P(tp),
        P(tp, None),
        P(),
        P(sp, tp),
        P(sp, tp),
        P(None, tp),
        P(tp, sp),
    )
    return jax.shard_map(body, mesh=torus, in_specs=placed, out_specs=P(sp, tp), check_vma=False)
```

```python
import jax
import jax.numpy as jnp
from jax import lax
from jax.experimental import pallas as pl
from jax.experimental.pallas import tpu as pltpu
from jax.sharding import Mesh
from jax.sharding import PartitionSpec as P

MESH = pl.DeviceIdType.MESH
F32 = jnp.float32
BF16 = jnp.bfloat16
ABSENT = -1e30
DH = 96
TOK = 768
OWN = 384
HW = 192
MAIN = 1024
GW = 1152
LANES = 2176
ONE = 128
TWO = 64
EPS = 1e-6
SEMS = 224
scope = jax.named_scope


def mod4(v):
    return lax.rem(v + 8, 4)


def dot(a, b, **kw):
    return lax.dot_general(a, b, (((1,), (0,)), ((), ())), preferred_element_type=F32, **kw)


def dot_t(a, b, **kw):
    return lax.dot_general(a, b, (((1,), (1,)), ((), ())), preferred_element_type=F32, **kw)


def dot_c(a, b, **kw):
    return lax.dot_general(a, b, (((0,), (0,)), ((), ())), preferred_element_type=F32, **kw)


def kernel(
    wg_ref,
    wv_ref,
    wd_ref,
    q_hbm,
    k_hbm,
    v_hbm,
    og_hbm,
    wo_ref,
    resid_hbm,
    ig_ref,
    fg_ref,
    seg_ref,
    hg_ref,
    gain_ref,
    taps_ref,
    out_ref,
    W,
    WD1,
    WD2,
    TL,
    X,
    MIX,
    WO,
    WOT,
    QT,
    KT,
    VT,
    OG,
    RB,
    OI,
    NF,
    ST,
    SR,
    SS,
    RES,
    ACC,
    GT,
    EDGE,
    HD,
    SP,
    RP,
    PO,
    ZS,
    RL,
    RV,
    ssem,
    rsem,
    lsem,
):
    z, x = lax.axis_index("z"), lax.axis_index("x")
    y, c = lax.axis_index("y"), lax.axis_index("c")
    sp = z * 4 + x
    tp = y * 2 + c
    o = 1 - c
    table = {}
    started = []

    def slot(key):
        return table.setdefault(key, len(table))

    def send(key, src, dst, dev):
        i = slot(key)
        d = pltpu.make_async_remote_copy(
            src_ref=src,
            dst_ref=dst,
            send_sem=ssem.at[i],
            recv_sem=rsem.at[i],
            device_id=dev,
            device_id_type=MESH,
        )
        d.start()
        started.append(d)

    partner = (z, x, y, o)

    def recv(key, dst):
        i = slot(key)
        pltpu.make_async_remote_copy(
            src_ref=dst,
            dst_ref=dst,
            send_sem=ssem.at[i],
            recv_sem=rsem.at[i],
            device_id=partner,
            device_id_type=MESH,
        ).wait_recv()

    def at_sp(n):
        s = lax.rem(sp + n + 16, 16)
        return (s // 4, lax.rem(s, 4), y, c)

    def at_x(d):
        return (z, mod4(x + d), y, c)

    def at_z(d):
        return (mod4(z + d), x, y, c)

    def at_y(d):
        return (z, x, mod4(y + d), c)

    def at_tp(n):
        t = lax.rem(tp + n, 8)
        return (z, x, t // 2, lax.rem(t, 2))

    peers = [at_x(1), at_x(-1), at_z(1), at_z(-1)]
    peers += [at_tp(n) for n in range(1, 8)]
    peers += [at_sp(n) for n in (1, 2, 3, -1, -2, -3)]
    barrier = pltpu.get_barrier_semaphore()
    for dev in peers:
        pl.semaphore_signal(barrier, inc=1, device_id=dev, device_id_type=MESH)

    local = []

    def bring(src, dst):
        d = pltpu.make_async_copy(src, dst, lsem.at[len(local)])
        d.start()
        local.append(d)

    own_w = pl.ds(pl.multiple_of(sp * HW, 16), HW)
    bring(wg_ref.at[:, 0:MAIN], W.at[own_w, 0:MAIN])
    bring(wv_ref.at[:, 0:MAIN], W.at[own_w, GW:LANES])
    for n, ref in enumerate((wg_ref, wv_ref, wd_ref)):
        bring(ref.at[:, MAIN : MAIN + 32], TL.at[n])
    bring(k_hbm, KT)
    bring(v_hbm, VT)
    bring(q_hbm, QT)
    bring(og_hbm, OG)
    bring(wd_ref.at[0:ONE, 0:MAIN], WD1.at[pl.ds(pl.multiple_of(sp * ONE, 16), ONE), :])
    bring(wd_ref.at[ONE:HW, 0:MAIN], WD2.at[pl.ds(pl.multiple_of(sp * TWO, 16), TWO), :])
    bring(resid_hbm, RB)
    bring(
        wo_ref.at[:, pl.ds(pl.multiple_of(tp * OWN, 128), OWN)],
        WO.at[pl.ds(pl.multiple_of(tp * HW, 16), HW), :],
    )

    def stage(name, ref, stride, rows, lanes, cut, first):
        x_first = first == "x"
        prim = at_x if x_first else at_z
        secd = at_z if x_first else at_x
        steps = (0, -1, 1, 2)

        def place(dp, ds, half=None):
            zz, xx = (mod4(z + ds), mod4(x + dp)) if x_first else (mod4(z + dp), mod4(x + ds))
            r0, nr = rows
            if half is not None:
                r0, nr = r0 + (cut[0] if half else 0), cut[half]
            row = pl.multiple_of((zz * 4 + xx) * stride + r0, 16)
            return ref.at[pl.ds(row, nr), pl.ds(lanes[0], lanes[1])]

        def primary():
            for d in (1, -1):
                send((name, "p", d), place(0, 0), place(0, 0), prim(d))

        def second(m):
            p = place(steps[m], 0)
            for d in (1, -1):
                send((name, "s", d, m), p, p, secd(d))

        def relay():
            for d in (1, -1):
                recv((name, "p", d), place(-d, 0))
                p = place(-d, 0, 0 if d == 1 else 1)
                send((name, "pf", d), p, p, prim(d))

        def across(m):
            for d in (1, -1):
                recv((name, "s", d, m), place(steps[m], -d))
                p = place(steps[m], -d, 0 if d == 1 else 1)
                send((name, "sf", d, m), p, p, secd(d))

        def far():
            for d in (1, -1):
                recv((name, "pf", d), place(2, 0, 0 if d == 1 else 1))
            second(3)

        def done():
            for m in range(4):
                for d in (1, -1):
                    recv((name, "sf", d, m), place(steps[m], 2, 0 if d == 1 else 1))

        return primary, second, relay, across, far, done

    def run(stages, what, *args):
        k = ("primary", "second", "relay", "across", "far", "done").index(what)
        for st in stages:
            st[k](*args)

    gv = (
        stage("g", W, HW, (0, HW), (0, GW), (96, 96), "x"),
        stage("v", W, HW, (0, HW), (GW, MAIN), (96, 96), "z"),
    )
    d1 = (
        stage("d1a", WD1, ONE, (0, 48), (0, MAIN), (32, 16), "x"),
        stage("d1b", WD1, ONE, (48, 80), (0, MAIN), (48, 32), "z"),
    )
    d2 = (
        stage("d2a", WD2, TWO, (0, 32), (0, MAIN), (16, 16), "x"),
        stage("d2b", WD2, TWO, (32, 32), (0, MAIN), (16, 16), "z"),
    )

    def over_tp(name, blk):
        def g0():
            b = blk(y, c)
            for d in (1, -1):
                send((name, "y", d), b, b, at_y(d))
            send((name, "o"), b, b, partner)

        def g1():
            for d in (1, -1):
                src = mod4(y - d)
                recv((name, "y", d), blk(src, c))
                h = blk(src, c, 0 if d == 1 else 1)
                send((name, "f", d), h, h, at_y(d))
            for d in (1, -1):
                src = mod4(y - d)
                send((name, "of", d), blk(src, c), blk(src, c), partner)

        def g2():
            far = mod4(y + 2)
            for d in (1, -1):
                h = blk(far, c, 0 if d == 1 else 1)
                recv((name, "f", d), h)
                send((name, "oh", d), h, h, partner)

        def g3():
            far = mod4(y + 2)
            recv((name, "o"), blk(y, o))
            for d in (1, -1):
                recv((name, "of", d), blk(mod4(y - d), o))
                recv((name, "oh", d), blk(far, o, 0 if d == 1 else 1))

        return g0, g1, g2, g3

    def mix_block(yy, cc, half=None):
        r0, nr = (0, HW) if half is None else (half * DH, DH)
        return MIX.at[pl.ds(pl.multiple_of((yy * 2 + cc) * HW + r0, 16), nr), :]

    def x_block(yy, cc, half=None):
        rows = slice(None) if half is None else pl.ds(half * OWN, OWN)
        return X.at[rows, pl.ds(pl.multiple_of((yy * 2 + cc) * OWN, 128), OWN)]

    mix_g = over_tp("m", mix_block)
    x_g = over_tp("x", x_block)

    for d in local[:5]:
        d.wait()
    tails = jnp.concatenate([TL[0], TL[1], TL[2], jnp.zeros((HW, 32), BF16)], axis=1)
    W[own_w, MAIN:GW] = tails
    with scope("barrier"):
        pl.semaphore_wait(barrier, len(peers))
    run(gv[1:], "primary")
    run(gv[:1], "primary")
    for n in range(1, 8):
        t = lax.rem(tp + n, 8)
        src = wo_ref.at[:, pl.ds(pl.multiple_of(t * OWN, 128), OWN)]
        dst = WO.at[pl.ds(pl.multiple_of(tp * HW, 16), HW), :]
        send(("w", n), src, dst, at_tp(n))

    lane = lax.broadcasted_iota(jnp.int32, (8, TOK), 1)
    row8 = lax.broadcasted_iota(jnp.int32, (8, TOK), 0)
    seg = seg_ref[...].astype(F32)
    fg = jnp.where(row8 == 0, fg_ref[0:1], fg_ref[1:2])
    e = jnp.exp(-jnp.abs(fg))
    log1p = jnp.where(e < 1e-2, e * (1.0 - e * (0.5 - e * (1.0 / 3.0))), jnp.log(1.0 + e))
    cum = jnp.minimum(fg, 0.0) - log1p
    shift = 1
    while shift < TOK:
        cum = cum + jnp.where(lane >= shift, pltpu.roll(cum, shift, 1), 0.0)
        shift *= 2
    b = [ig_ref[h : h + 1] - cum[h : h + 1] for h in range(2)]
    end = [cum[h : h + 1, TOK - 1 :] for h in range(2)]
    first, last, second_last = seg[:, :1], seg[:, TOK - 1 :], seg[:, TOK - 2 : TOK - 1]
    for d in local[5:9]:
        d.wait()
    ST[...] = jnp.zeros_like(ST)
    peak = []
    for h in range(2):
        hs = slice(h * DH, h * DH + DH)
        top = jnp.max(jnp.where(seg == last, b[h], ABSENT), axis=1, keepdims=True)
        peak.append(top)
        w = jnp.where(seg == last, jnp.exp(jnp.minimum(b[h] - top, 0.0)), 0.0) * DH**-0.5
        ST[hs, 0:DH] = dot_t(VT[hs, :], (KT[hs, :].astype(F32) * w).astype(BF16))
    meta_row = lax.broadcasted_iota(jnp.int32, (8, 128), 0)
    meta = jnp.zeros((8, 128), F32)
    for n, value in enumerate((end[0] + peak[0], end[1] + peak[1], end[0], end[1], first, last, second_last)):
        meta = jnp.where(meta_row == n, value, meta)
    ST[HW : HW + 8, :] = meta
    for n in range(1, 5):
        send(("st", n), ST, SR.at[n - 1], at_sp(n))
    run(gv, "second", 0)

    rows = jnp.where(row8 == 0, b[0], jnp.where(row8 == 1, b[1], seg))
    cols = jnp.transpose(jnp.concatenate([rows, jnp.zeros((120, TOK), F32)], axis=0))
    seg_c = cols[:, 2:3]
    tops = [[], []]
    for i in range(3):
        t0, ns = i * 256, (i + 1) * 256
        ts = slice(t0, t0 + 256)
        s_at = lax.broadcasted_iota(jnp.int32, (ns, 256), 0)
        t_at = lax.broadcasted_iota(jnp.int32, (ns, 256), 1) + t0
        mask = (seg_c[:ns] == seg[:, ts]) & (s_at <= t_at)
        for h in range(2):
            hs = slice(h * DH, h * DH + DH)
            masked = jnp.where(mask, cols[:ns, h : h + 1], ABSENT)
            top = jnp.max(masked, axis=0, keepdims=True)
            scores = dot_c(KT[hs, 0:ns], QT[hs, ts]) * (jnp.exp(masked - top) * DH**-0.5)
            OI[hs, ts] = dot(VT[hs, 0:ns], scores.astype(BF16))
            tops[h].append(top)

    with scope("relay"):
        run(gv, "relay")
        run(gv, "second", 1)
        run(gv, "second", 2)

    dec = [jnp.zeros((1, 128), F32)] * 2
    cand = [[], []]
    first_l = jnp.broadcast_to(first, (1, 128))
    with scope("state"):
        for n in range(1, 5):
            recv(("st", n), SR.at[n - 1])
    for n in range(1, 5):
        m = SR[n - 1, HW : HW + 8, :]
        valid = (m[5:6] == first_l) & (sp >= n)
        for h in range(2):
            cand[h].append(jnp.where(valid, m[h : h + 1] + dec[h], ABSENT))
            dec[h] = dec[h] + m[2 + h : 3 + h]
    gain_at = lax.broadcasted_iota(jnp.int32, (HW, HW), 0) == lax.broadcasted_iota(jnp.int32, (HW, HW), 1)
    gain_c = jnp.sum(jnp.where(gain_at, hg_ref[...], 0.0), axis=1, keepdims=True)
    for h in range(2):
        hs = slice(h * DH, h * DH + DH)
        pin = jnp.maximum(
            jnp.maximum(cand[h][0], cand[h][1]), jnp.maximum(cand[h][2], cand[h][3])
        )
        state = jnp.zeros((DH, 128), F32)
        for n in range(4):
            state = state + jnp.exp(cand[h][n] - pin) * SR[n, hs, :]
        inter = dot(state[:, 0:DH].astype(BF16), QT[hs, :])
        m_in = jnp.concatenate(tops[h], axis=1)
        m_pin = jnp.where(seg == first, pin[:, :1], ABSENT)
        m_all = jnp.maximum(m_in, m_pin)
        memory = jnp.exp(m_in - m_all) * OI[hs, :] + jnp.exp(m_pin - m_all) * inter
        mean = jnp.sum(memory * memory, axis=0, keepdims=True) * (1.0 / DH)
        mix = memory * lax.rsqrt(mean + 1.0) * gain_c[hs] * jax.nn.sigmoid(OG[hs, :].astype(F32))
        MIX[pl.ds(pl.multiple_of(tp * HW + h * DH, 16), DH), :] = mix.astype(BF16)
    with scope("mix0"):
        mix_g[0]()
    with scope("across0"):
        run(gv, "across", 0)

    before = SR[0, HW : HW + 8, :]
    there = sp >= 1
    last_before = jnp.where(there, before[5:6, :1], -1.0)
    second_before = jnp.where(there, before[6:7, :1], -1.0)
    seg8 = jnp.broadcast_to(seg, (8, TOK))
    one_back = jnp.where(lane == 0, last_before, pltpu.roll(seg8, 1, 1))
    two_back = jnp.where(
        lane == 0, second_before, jnp.where(lane == 1, last_before, pltpu.roll(seg8, 2, 1))
    )
    flags = jnp.where(
        row8 == 0, jnp.where(one_back == seg, 1.0, 0.0), jnp.where(two_back == seg, 1.0, 0.0)
    )
    NF[...] = jnp.transpose(jnp.concatenate([flags, jnp.zeros((120, TOK), F32)], axis=0))
    with scope("wo"):
        for d in local[9:]:
            d.wait()
        for n in range(1, 8):
            t = lax.rem(tp + 8 - n, 8)
            recv(("w", n), WO.at[pl.ds(pl.multiple_of(t * HW, 16), HW), :])
        WOT[...] = jnp.transpose(WO[...])

    with scope("mix1"):
        mix_g[1]()
    with scope("far"):
        run(gv, "far")
    with scope("mix2"):
        mix_g[2]()
    with scope("mix3"):
        mix_g[3]()

    gain = gain_ref[:, pl.ds(pl.multiple_of(tp * OWN, 128), OWN)]
    res = RB[...].astype(F32) + jnp.transpose(dot(WOT[...], MIX[...]))
    RES[...] = res
    X[:, pl.ds(pl.multiple_of(tp * OWN, 128), OWN)] = (res * gain).astype(BF16)
    x_g[0]()
    SS[tp] = dot_t(jnp.ones((8, OWN), F32), res * res, precision=lax.Precision.HIGHEST)
    for n in range(1, 8):
        send(("q", n), SS.at[tp], SS.at[tp], at_tp(n))
    with scope("across1"):
        run(gv, "across", 1)
    with scope("across2"):
        run(gv, "across", 2)
    with scope("x1"):
        x_g[1]()
    with scope("x2"):
        x_g[2]()
    with scope("x3"):
        x_g[3]()
    with scope("across3"):
        run(gv, "across", 3)
        run(d1, "primary")
        run(d1, "second", 0)
    with scope("sq"):
        total = SS[tp]
        for n in range(1, 8):
            t = lax.rem(tp + 8 - n, 8)
            recv(("q", n), SS.at[t])
            total = total + SS[t]
    scale_row = lax.rsqrt(total * (1.0 / 3072.0) + EPS)
    NF[:, 2:3] = jnp.transpose(jnp.concatenate([scale_row, jnp.zeros((120, TOK), F32)], axis=0))[:, 0:1]

    def tile256(n, at):
        return pl.ds(pl.multiple_of(n * 256 + at, 128), 256)

    def by_row(lanes, steps):
        acc = None
        for d in steps:
            k = pl.ds(pl.multiple_of(mod4(z + d) * 768, 128), 768)
            part = dot(X[:, k], W[k, lanes])
            acc = part if acc is None else acc + part
        return acc

    def by_pair(lanes, which):
        acc = None
        for zz in range(4):
            k = pl.ds(pl.multiple_of(zz * 768 + which * OWN, 128), OWN)
            part = dot(X[:, k], W[k, lanes])
            acc = part if acc is None else acc + part
        return acc

    here = x // 2
    with scope("partial"):

        def early(n, _):
            ACC[:, tile256(n, 0)] = by_row(tile256(n, 0), (0, 1, -1))
            ACC[:, tile256(n, GW)] = by_pair(tile256(n, GW), here)
            return 0

        lax.fori_loop(0, 4, early, 0)
        ACC[:, MAIN:GW] = by_row(slice(MAIN, GW), (0, 1, -1))

    with scope("done"):
        run(gv, "done")
    with scope("d1relay"):
        run(d1, "relay")
        run(d1, "second", 1)
        run(d1, "second", 2)
    scale = NF[:, 2:3]
    with scope("gate"):

        def gate_tile(n, _):
            l = tile256(n, 0)
            GT[:, l] = ((ACC[:, l] + by_row(l, (2,))) * scale).astype(BF16)
            return 0

        lax.fori_loop(0, 4, gate_tile, 0)
        l = slice(MAIN, GW)
        GT[:, l] = ((ACC[:, l] + by_row(l, (2,))) * scale).astype(BF16)
    send(("e",), GT.at[TOK - 16 : TOK, :], EDGE, at_sp(1))
    with scope("d1across0"):
        run(d1, "across", 0)

    def hidden_of(lanes, width, taps, value):
        g = GT[:, lanes].astype(F32)
        edge = EDGE[:, lanes].astype(F32)
        t_at = lax.broadcasted_iota(jnp.int32, (TOK, width), 0)
        near = NF[:, 0:1] > 0.5
        far = NF[:, 1:2] > 0.5
        g1 = jnp.where(t_at == 0, edge[15:16], pltpu.roll(g, 1, 0))
        g2 = jnp.where(
            t_at == 0, edge[14:15], jnp.where(t_at == 1, edge[15:16], pltpu.roll(g, 2, 0))
        )
        conv = taps[2:3] * g + taps[1:2] * jnp.where(near, g1, 0.0) + taps[0:1] * jnp.where(far, g2, 0.0)
        return conv / (1.0 + jnp.exp(-conv)) * value

    def value_sum(n, _):
        l = tile256(n, GW)
        ACC[:, l] = ACC[:, l] + by_pair(l, 1 - here)
        return 0

    with scope("value"):
        lax.fori_loop(0, 4, value_sum, 0)
    with scope("d1far"):
        run(d1, "far")
    with scope("edge"):
        recv(("e",), EDGE)

    with scope("hidden"):

        def hidden_tile(n, _):
            value = (ACC[:, tile256(n, GW)] * scale).astype(BF16).astype(F32)
            l = tile256(n, 0)
            HD[:, l] = hidden_of(l, 256, taps_ref[:, l], value).astype(BF16)
            return 0

        lax.fori_loop(0, 4, hidden_tile, 0)
        tail = slice(MAIN, GW)
        taps_tail = jnp.concatenate([taps_ref[:, MAIN : MAIN + 32], jnp.zeros((3, 96), F32)], axis=1)
        value_tail = pltpu.roll(GT[:, tail].astype(F32), 96, 1)
        HD[:, tail] = pltpu.roll(hidden_of(tail, 128, taps_tail, value_tail), 64, 1).astype(BF16)
    with scope("d1rest"):
        run(d1, "across", 1)
        run(d1, "across", 2)
        run(d2, "primary")
        run(d2, "second", 0)
        run(d1, "across", 3)
        run(d2, "relay")
        run(d2, "second", 1)
        run(d2, "second", 2)
        run(d1, "done")

    def partial(p, yy, cc):
        j = yy * 2 + cc
        size = ONE if p == 0 else TWO
        ref = WD1 if p == 0 else WD2
        r = pl.ds(pl.multiple_of(j * 2 * size, 128), 2 * size)
        ends = []
        for k in range(2):
            at = (j * 2 + k) * HW + (0 if p == 0 else ONE)
            ends.append(W[pl.ds(pl.multiple_of(at, 16), size), MAIN:GW])
        return dot_t(HD[:, 0:MAIN], ref[r, :]) + dot_t(HD[:, MAIN:GW], jnp.concatenate(ends, axis=0))

    order = (2, 1, -1, 0)
    lanes_of = (pl.ds(0, 2 * ONE), pl.ds(2 * ONE, 2 * TWO))

    def reduce_part(p, between):
        l = lanes_of[p]

        def give(n):
            yy = mod4(y + order[n])
            SP[n, :, l] = partial(p, yy, o).astype(BF16)
            send(("sp", p, n), SP.at[n, :, l], RP.at[n, :, l], partner)

        give(0)
        for n, d in enumerate(order):
            if n < 3:
                give(n + 1)
            PO[n, :, l] = partial(p, mod4(y + d), c)
            with scope("sp%d" % n):
                recv(("sp", p, n), RP.at[n, :, l])
            both = PO[n, :, l] + RP[n, :, l].astype(F32)
            if d == 2:
                ZS[0, :, l] = both.astype(BF16)
                send(("rl", p, 1), ZS.at[0, pl.ds(0, OWN), l], RL.at[0, :, l], at_y(1))
                send(("rl", p, -1), ZS.at[0, pl.ds(OWN, OWN), l], RL.at[1, :, l], at_y(-1))
            else:
                PO[n, :, l] = both
                if d != 0:
                    r = pl.ds(OWN if d == 1 else 0, OWN)
                    ZS[n, r, l] = PO[n, r, l].astype(BF16)
                    send(("rv", p, d), ZS.at[n, r, l], RV.at[n - 1, r, l], at_y(d))
            between[n]()
        for n, d in ((1, 1), (2, -1)):
            r = pl.ds(0 if d == 1 else OWN, OWN)
            with scope("rl"):
                recv(("rl", p, d), RL.at[n - 1, :, l])
            ZS[n, r, l] = (PO[n, r, l] + RL[n - 1, :, l].astype(F32)).astype(BF16)
            send(("rw", p, d), ZS.at[n, r, l], RV.at[n - 1, r, l], at_y(d))

    def collect(p):
        l = lanes_of[p]
        for n, d in ((1, 1), (2, -1)):
            with scope("rv"):
                recv(("rv", p, d), RV.at[n - 1, pl.ds(OWN if d == 1 else 0, OWN), l])
                recv(("rw", p, d), RV.at[n - 1, pl.ds(0 if d == 1 else OWN, OWN), l])
        return PO[3, :, l] + RV[0, :, l].astype(F32) + RV[1, :, l].astype(F32)

    nothing = lambda: None
    with scope("reduce1"):
        reduce_part(
            0,
            [
                lambda: run(d2, "across", 0),
                lambda: run(d2, "far"),
                lambda: run(d2, "across", 1),
                lambda: run(d2, "across", 2),
            ],
        )
    with scope("d2rest"):
        run(d2, "across", 3)
        run(d2, "done")
    with scope("reduce2"):
        reduce_part(1, [nothing] * 4)
    with scope("final"):
        wide = collect(0)
        slim = collect(1)
        turned = pltpu.roll(wide[:, ONE:], 64, 1)
        low = lax.broadcasted_iota(jnp.int32, (TOK, 128), 1) < 64
        out_ref[:, 0:128] = (RES[:, 0:128] + wide[:, :ONE]).astype(BF16)
        out_ref[:, 128:256] = (RES[:, 128:256] + jnp.where(low, slim, turned)).astype(BF16)
        out_ref[:, 256:384] = (RES[:, 256:384] + jnp.where(low, turned, slim)).astype(BF16)
        for d in started:
            d.wait_send()


def body(
    resid,
    query,
    keys,
    values,
    out_gate,
    in_gate,
    forget,
    doc_ids,
    head_gain,
    w_out,
    ffn_gain,
    w_gate,
    w_value,
    conv_taps,
    w_down,
):
    vmem = pl.BlockSpec(memory_space=pltpu.VMEM)
    hbm = pl.BlockSpec(memory_space=pl.ANY)
    return pl.pallas_call(
        kernel,
        out_shape=jax.ShapeDtypeStruct((TOK, OWN), BF16),
        in_specs=[hbm] * 9 + [vmem] * 6,
        out_specs=vmem,
        scratch_shapes=[
            pltpu.VMEM((3072, LANES), BF16),
            pltpu.VMEM((16 * ONE, MAIN), BF16),
            pltpu.VMEM((16 * TWO, MAIN), BF16),
            pltpu.VMEM((3, HW, 32), BF16),
            pltpu.VMEM((TOK, 3072), BF16),
            pltpu.VMEM((1536, TOK), BF16),
            pltpu.VMEM((1536, OWN), BF16),
            pltpu.VMEM((OWN, 1536), BF16),
            pltpu.VMEM((HW, TOK), BF16),
            pltpu.VMEM((HW, TOK), BF16),
            pltpu.VMEM((HW, TOK), BF16),
            pltpu.VMEM((HW, TOK), BF16),
            pltpu.VMEM((TOK, OWN), BF16),
            pltpu.VMEM((HW, TOK), F32),
            pltpu.VMEM((TOK, 128), F32),
            pltpu.VMEM((200, 128), F32),
            pltpu.VMEM((4, 200, 128), F32),
            pltpu.VMEM((8, 8, TOK), F32),
            pltpu.VMEM((TOK, OWN), F32),
            pltpu.VMEM((TOK, LANES), F32),
            pltpu.VMEM((TOK, GW), BF16),
            pltpu.VMEM((16, GW), BF16),
            pltpu.VMEM((TOK, GW), BF16),
            pltpu.VMEM((4, TOK, OWN), BF16),
            pltpu.VMEM((4, TOK, OWN), BF16),
            pltpu.VMEM((4, TOK, OWN), F32),
            pltpu.VMEM((3, TOK, OWN), BF16),
            pltpu.VMEM((2, OWN, OWN), BF16),
            pltpu.VMEM((2, TOK, OWN), BF16),
            pltpu.SemaphoreType.DMA((SEMS,)),
            pltpu.SemaphoreType.DMA((SEMS,)),
            pltpu.SemaphoreType.DMA((16,)),
        ],
        compiler_params=pltpu.CompilerParams(
            collective_id=0, has_side_effects=True, vmem_limit_bytes=63 * 1024 * 1024
        ),
    )(
        w_gate,
        w_value,
        w_down.T,
        query.T,
        keys.T,
        values.T,
        out_gate.T,
        w_out,
        resid,
        in_gate,
        forget,
        doc_ids[None],
        head_gain[None],
        ffn_gain[None],
        conv_taps,
    )


def solution(mesh):
    torus = Mesh(mesh.devices.reshape(4, 4, 4, 2), ("z", "x", "y", "c"))
    sp, tp = ("z", "x"), ("y", "c")
    placed = (
        P(sp, tp),
        P(sp, tp),
        P(sp, tp),
        P(sp, tp),
        P(sp, tp),
        P(tp, sp),
        P(tp, sp),
        P(sp),
        P(tp),
        P(tp, None),
        P(),
        P(sp, tp),
        P(sp, tp),
        P(None, tp),
        P(tp, sp),
    )
    return jax.shard_map(body, mesh=torus, in_specs=placed, out_specs=P(sp, tp), check_vma=False)
```

```python
import jax
import jax.numpy as jnp
from jax import lax
from jax.experimental import pallas as pl
from jax.experimental.pallas import tpu as pltpu
from jax.sharding import Mesh
from jax.sharding import PartitionSpec as P

MESH = pl.DeviceIdType.MESH
F32 = jnp.float32
BF16 = jnp.bfloat16
ABSENT = -1e30
DH = 96
TOK = 768
OWN = 384
HW = 192
MAIN = 1024
GW = 1152
LANES = 2176
PART = 64
EPS = 1e-6
VLIM = 60
SEMS = 104
scope = jax.named_scope


def mod4(v):
    return lax.rem(v + 8, 4)


def dot(a, b, **kw):
    return lax.dot_general(a, b, (((1,), (0,)), ((), ())), preferred_element_type=F32, **kw)


def dot_t(a, b, **kw):
    return lax.dot_general(a, b, (((1,), (1,)), ((), ())), preferred_element_type=F32, **kw)


def dot_c(a, b, **kw):
    return lax.dot_general(a, b, (((0,), (0,)), ((), ())), preferred_element_type=F32, **kw)


def kernel(
    wg_ref,
    wv_ref,
    wd_ref,
    q_hbm,
    k_hbm,
    v_hbm,
    og_hbm,
    wo_ref,
    resid_hbm,
    ig_hbm,
    fg_hbm,
    seg_hbm,
    hg_hbm,
    gain_hbm,
    taps_hbm,
    out_ref,
    W,
    ig_ref,
    fg_ref,
    seg_ref,
    hg_ref,
    gain_ref,
    taps_ref,
    WD0,
    WD1,
    WD2,
    TL,
    X,
    MIX,
    WO,
    WOT,
    QT,
    KT,
    VT,
    OG,
    RB,
    OI,
    NF,
    ST,
    SR,
    MT,
    MR,
    SS,
    RES,
    ACC,
    GT,
    EDGE,
    HD,
    SP,
    RP,
    ZS,
    RL,
    RV,
    sems,
    lsem,
):
    z, x = lax.axis_index("z"), lax.axis_index("x")
    y, c = lax.axis_index("y"), lax.axis_index("c")
    sp = z * 4 + x
    tp = y * 2 + c
    o = 1 - c
    table = {}
    rkey_any = "w"

    def slot(key):
        return table.setdefault(key, len(table))

    def copy(rkey, skey, src, dst, dev):
        return pltpu.make_async_remote_copy(
            src_ref=src,
            dst_ref=dst,
            send_sem=sems.at[slot(("S", skey))],
            recv_sem=sems.at[slot(("R", rkey))],
            device_id=dev,
            device_id_type=MESH,
        )

    def send(rkey, skey, src, dst, dev):
        copy(rkey, skey, src, dst, dev).start()

    partner = (z, x, y, o)

    def recv(rkey, span):
        copy(rkey, rkey_any, span, span, partner).wait_recv()

    def sent(skey, span):
        copy(rkey_any, skey, span, span, partner).wait_send()

    def at_sp(n):
        s = lax.rem(sp + n + 16, 16)
        return (s // 4, lax.rem(s, 4), y, c)

    def at_x(d):
        return (z, mod4(x + d), y, c)

    def at_z(d):
        return (mod4(z + d), x, y, c)

    def at_y(d):
        return (z, x, mod4(y + d), c)

    def at_tp(n):
        t = lax.rem(tp + n, 8)
        return (z, x, t // 2, lax.rem(t, 2))

    peers = [at_x(1), at_x(-1), at_z(1), at_z(-1)]
    peers += [at_tp(n) for n in range(1, 8)]
    peers += [at_sp(n) for n in (1, 2, 3, -1, -2, -3)]
    barrier = pltpu.get_barrier_semaphore()
    for dev in peers:
        pl.semaphore_signal(barrier, inc=1, device_id=dev, device_id_type=MESH)

    local = []

    def bring(src, dst):
        d = pltpu.make_async_copy(src, dst, lsem.at[len(local)])
        d.start()
        local.append(d)

    own_w = pl.ds(pl.multiple_of(sp * HW, 16), HW)
    bring(wg_ref.at[:, 0:MAIN], W.at[own_w, 0:MAIN])
    bring(wv_ref.at[:, 0:MAIN], W.at[own_w, GW:LANES])
    for n, ref in enumerate((wg_ref, wv_ref, wd_ref)):
        bring(ref.at[:, MAIN : MAIN + 32], TL.at[n])
    bring(fg_hbm, fg_ref)
    bring(ig_hbm, ig_ref)
    bring(seg_hbm, seg_ref)
    bring(k_hbm, KT)
    bring(v_hbm, VT)
    bring(q_hbm, QT)
    bring(og_hbm, OG)
    for n, ref in enumerate((WD0, WD1, WD2)):
        bring(
            wd_ref.at[n * PART : (n + 1) * PART, 0:MAIN],
            ref.at[pl.ds(pl.multiple_of(sp * PART, 16), PART), :],
        )
    bring(hg_hbm, hg_ref)
    bring(gain_hbm, gain_ref)
    bring(taps_hbm, taps_ref)
    bring(resid_hbm, RB)
    bring(
        wo_ref.at[:, pl.ds(pl.multiple_of(tp * OWN, 128), OWN)],
        WO.at[pl.ds(pl.multiple_of(tp * HW, 16), HW), :],
    )

    def stage(name, ref, stride, rows, lanes, by_lanes, first):
        x_first = first == "x"
        prim = at_x if x_first else at_z
        secd = at_z if x_first else at_x
        steps = (0, -1, 1, 2)

        def place(dp, ds, half=None):
            zz, xx = (mod4(z + ds), mod4(x + dp)) if x_first else (mod4(z + dp), mod4(x + ds))
            (r0, nr), (l0, nl) = rows, lanes
            if half is not None and by_lanes:
                l0, nl = l0 + half * nl // 2, nl // 2
            elif half is not None:
                r0, nr = r0 + half * nr // 2, nr // 2
            row = pl.multiple_of((zz * 4 + xx) * stride + r0, 16)
            return ref.at[pl.ds(row, nr), pl.ds(l0, nl)]

        def span(k):
            return ref.at[pl.ds(0, k * rows[1]), pl.ds(lanes[0], lanes[1])]

        def primary():
            for d in (1, -1):
                send((name, "p"), name, place(0, 0), place(0, 0), prim(d))

        def second(m):
            p = place(steps[m], 0)
            for d in (1, -1):
                send((name, "s", m), name, p, p, secd(d))

        def relay():
            recv((name, "p"), span(2))
            for d in (1, -1):
                p = place(-d, 0, 0 if d == 1 else 1)
                send((name, "pf"), name, p, p, prim(d))

        def across(m):
            recv((name, "s", m), span(2))
            for d in (1, -1):
                p = place(steps[m], -d, 0 if d == 1 else 1)
                send((name, "sf"), name, p, p, secd(d))

        def far():
            recv((name, "pf"), span(1))
            second(3)

        def done():
            recv((name, "sf"), span(4))

        def out():
            sent(name, span(15))

        return primary, second, relay, across, far, done, out

    def run(stages, what, *args):
        k = ("primary", "second", "relay", "across", "far", "done", "out").index(what)
        for st in stages:
            st[k](*args)

    gv = (
        stage("g", W, HW, (0, HW), (0, GW), False, "x"),
        stage("v", W, HW, (0, HW), (GW, MAIN), False, "z"),
    )

    def down_stage(n, ref, cut):
        return (
            stage(("da", n), ref, PART, (0, cut), (0, MAIN), True, "x"),
            stage(("db", n), ref, PART, (cut, PART - cut), (0, MAIN), True, "z"),
        )

    d0, d1, d2 = down_stage(0, WD0, 16), down_stage(1, WD1, 32), down_stage(2, WD2, 32)

    def over_tp(name, blk, span):
        def g0():
            b = blk(y, c)
            for d in (1, -1):
                send((name, "y"), name, b, b, at_y(d))
            send((name, "o"), name, b, b, partner)

        def g1():
            recv((name, "y"), span(2))
            for d in (1, -1):
                h = blk(mod4(y - d), c, 0 if d == 1 else 1)
                send((name, "f"), name, h, h, at_y(d))
            for d in (1, -1):
                b = blk(mod4(y - d), c)
                send((name, "o"), name, b, b, partner)

        def g2():
            recv((name, "f"), span(1))
            b = blk(mod4(y + 2), c)
            send((name, "o"), name, b, b, partner)

        def g3():
            recv((name, "o"), span(4))

        def out():
            sent(name, span(7))

        return g0, g1, g2, g3, out

    def mix_block(yy, cc, half=None):
        r0, nr = (0, HW) if half is None else (half * DH, DH)
        return MIX.at[pl.ds(pl.multiple_of((yy * 2 + cc) * HW + r0, 16), nr), :]

    def x_block(yy, cc, half=None):
        rows = slice(None) if half is None else pl.ds(half * OWN, OWN)
        return X.at[rows, pl.ds(pl.multiple_of((yy * 2 + cc) * OWN, 128), OWN)]

    mix_g = over_tp("m", mix_block, lambda k: MIX.at[pl.ds(0, k * HW), :])
    x_g = over_tp("x", x_block, lambda k: X.at[:, pl.ds(0, k * OWN)])

    for d in local[:5]:
        d.wait()
    tails = jnp.concatenate([TL[0], TL[1], TL[2], jnp.zeros((HW, 32), BF16)], axis=1)
    W[own_w, MAIN:GW] = tails
    with scope("barrier"):
        pl.semaphore_wait(barrier, len(peers))
    run(gv[1:], "primary")
    run(gv[:1], "primary")
    for n in range(1, 8):
        t = lax.rem(tp + n, 8)
        src = wo_ref.at[:, pl.ds(pl.multiple_of(t * OWN, 128), OWN)]
        dst = WO.at[pl.ds(pl.multiple_of(tp * HW, 16), HW), :]
        send("w", "w", src, dst, at_tp(n))

    lane = lax.broadcasted_iota(jnp.int32, (8, TOK), 1)
    row8 = lax.broadcasted_iota(jnp.int32, (8, TOK), 0)
    for d in local[5:8]:
        d.wait()
    seg = seg_ref[...].reshape(1, TOK).astype(F32)
    fg = jnp.where(row8 == 0, fg_ref[0:1], fg_ref[1:2])
    e = jnp.exp(-jnp.abs(fg))
    log1p = jnp.where(e < 1e-2, e * (1.0 - e * (0.5 - e * (1.0 / 3.0))), jnp.log(1.0 + e))
    cum = jnp.minimum(fg, 0.0) - log1p
    shift = 1
    while shift < TOK:
        cum = cum + jnp.where(lane >= shift, pltpu.roll(cum, shift, 1), 0.0)
        shift *= 2
    b = [ig_ref[h : h + 1] - cum[h : h + 1] for h in range(2)]
    end = [cum[h : h + 1, TOK - 1 :] for h in range(2)]
    first, last, second_last = seg[:, :1], seg[:, TOK - 1 :], seg[:, TOK - 2 : TOK - 1]
    for d in local[8:12]:
        d.wait()
    ST[...] = jnp.zeros_like(ST)
    peak = []
    for h in range(2):
        hs = slice(h * DH, h * DH + DH)
        top = jnp.max(jnp.where(seg == last, b[h], ABSENT), axis=1, keepdims=True)
        peak.append(top)
        w = jnp.where(seg == last, jnp.exp(jnp.minimum(b[h] - top, 0.0)), 0.0) * DH**-0.5
        ST[hs, 0:DH] = dot_t(VT[hs, :], (KT[hs, :].astype(F32) * w).astype(BF16)).astype(BF16)
    meta_row = lax.broadcasted_iota(jnp.int32, (8, 128), 0)
    meta = jnp.zeros((8, 128), F32)
    for n, value in enumerate((end[0] + peak[0], end[1] + peak[1], end[0], end[1], first, last, second_last)):
        meta = jnp.where(meta_row == n, value, meta)
    MT[...] = meta
    for n in range(1, 5):
        send("st", "st", ST, SR.at[n - 1], at_sp(n))
        send("mt", "mt", MT, MR.at[n - 1], at_sp(n))
    run(gv, "second", 0)

    rows = jnp.where(row8 == 0, b[0], jnp.where(row8 == 1, b[1], seg))
    cols = jnp.transpose(jnp.concatenate([rows, jnp.zeros((120, TOK), F32)], axis=0))
    seg_c = cols[:, 2:3]
    tops = [[], []]
    for i in range(3):
        t0, ns = i * 256, (i + 1) * 256
        ts = slice(t0, t0 + 256)
        s_at = lax.broadcasted_iota(jnp.int32, (ns, 256), 0)
        t_at = lax.broadcasted_iota(jnp.int32, (ns, 256), 1) + t0
        mask = (seg_c[:ns] == seg[:, ts]) & (s_at <= t_at)
        for h in range(2):
            hs = slice(h * DH, h * DH + DH)
            masked = jnp.where(mask, cols[:ns, h : h + 1], ABSENT)
            top = jnp.max(masked, axis=0, keepdims=True)
            scores = dot_c(KT[hs, 0:ns], QT[hs, ts]) * (jnp.exp(masked - top) * DH**-0.5)
            OI[hs, ts] = dot(VT[hs, 0:ns], scores.astype(BF16))
            tops[h].append(top)

    with scope("relay"):
        run(gv, "relay")
        run(gv, "second", 1)
        run(gv, "second", 2)

    dec = [jnp.zeros((1, 128), F32)] * 2
    cand = [[], []]
    first_l = jnp.broadcast_to(first, (1, 128))
    with scope("state"):
        recv("st", SR)
        recv("mt", MR)
    for n in range(1, 5):
        m = MR[n - 1]
        valid = (m[5:6] == first_l) & (sp >= n)
        for h in range(2):
            cand[h].append(jnp.where(valid, m[h : h + 1] + dec[h], ABSENT))
            dec[h] = dec[h] + m[2 + h : 3 + h]
    for d in local[12:18]:
        d.wait()
    gain_at = lax.broadcasted_iota(jnp.int32, (HW, HW), 0) == lax.broadcasted_iota(jnp.int32, (HW, HW), 1)
    gain_c = jnp.sum(jnp.where(gain_at, hg_ref[...], 0.0), axis=1, keepdims=True)
    for h in range(2):
        hs = slice(h * DH, h * DH + DH)
        pin = jnp.maximum(
            jnp.maximum(cand[h][0], cand[h][1]), jnp.maximum(cand[h][2], cand[h][3])
        )
        state = jnp.zeros((DH, 128), F32)
        for n in range(4):
            state = state + jnp.exp(cand[h][n] - pin) * SR[n, hs, :].astype(F32)
        inter = dot(state[:, 0:DH].astype(BF16), QT[hs, :])
        m_in = jnp.concatenate(tops[h], axis=1)
        m_pin = jnp.where(seg == first, pin[:, :1], ABSENT)
        m_all = jnp.maximum(m_in, m_pin)
        memory = jnp.exp(m_in - m_all) * OI[hs, :] + jnp.exp(m_pin - m_all) * inter
        mean = jnp.sum(memory * memory, axis=0, keepdims=True) * (1.0 / DH)
        mix = memory * lax.rsqrt(mean + 1.0) * gain_c[hs] * jax.nn.sigmoid(OG[hs, :].astype(F32))
        MIX[pl.ds(pl.multiple_of(tp * HW + h * DH, 16), DH), :] = mix.astype(BF16)
    with scope("mix0"):
        mix_g[0]()
    with scope("across0"):
        run(gv, "across", 0)

    before = MR[0]
    there = sp >= 1
    last_before = jnp.where(there, before[5:6, :1], -1.0)
    second_before = jnp.where(there, before[6:7, :1], -1.0)
    seg8 = jnp.broadcast_to(seg, (8, TOK))
    one_back = jnp.where(lane == 0, last_before, pltpu.roll(seg8, 1, 1))
    two_back = jnp.where(
        lane == 0, second_before, jnp.where(lane == 1, last_before, pltpu.roll(seg8, 2, 1))
    )
    flags = jnp.where(
        row8 == 0, jnp.where(one_back == seg, 1.0, 0.0), jnp.where(two_back == seg, 1.0, 0.0)
    )
    NF[...] = jnp.transpose(jnp.concatenate([flags, jnp.zeros((120, TOK), F32)], axis=0))
    with scope("wo"):
        for d in local[18:]:
            d.wait()
        recv("w", WO.at[pl.ds(0, 7 * HW), :])
        WOT[...] = jnp.transpose(WO[...])

    with scope("mix1"):
        mix_g[1]()
    with scope("far"):
        run(gv, "far")
    with scope("mix2"):
        mix_g[2]()
    with scope("mix3"):
        mix_g[3]()

    gain = gain_ref[:, pl.ds(pl.multiple_of(tp * OWN, 128), OWN)]
    res = RB[...].astype(F32) + jnp.transpose(dot(WOT[...], MIX[...]))
    RES[...] = res
    X[:, pl.ds(pl.multiple_of(tp * OWN, 128), OWN)] = (res * gain).astype(BF16)
    x_g[0]()
    SS[tp] = dot_t(jnp.ones((8, OWN), F32), res * res, precision=lax.Precision.HIGHEST)
    for n in range(1, 8):
        send("q", "q", SS.at[tp], SS.at[tp], at_tp(n))
    with scope("across1"):
        run(gv, "across", 1)
    with scope("across2"):
        run(gv, "across", 2)
    with scope("x1"):
        x_g[1]()
    with scope("x2"):
        x_g[2]()
    with scope("x3"):
        x_g[3]()
    run(d0, "primary")
    run(d0, "second", 0)
    with scope("across3"):
        run(gv, "across", 3)
    with scope("sq"):
        recv("q", SS.at[pl.ds(0, 7)])
        total = SS[0]
        for n in range(1, 8):
            total = total + SS[n]
    scale_row = lax.rsqrt(total * (1.0 / 3072.0) + EPS)
    NF[:, 2:3] = jnp.transpose(jnp.concatenate([scale_row, jnp.zeros((120, TOK), F32)], axis=0))[:, 0:1]

    def tile256(n, at):
        return pl.ds(pl.multiple_of(n * 256 + at, 128), 256)

    def by_row(lanes, steps):
        acc = None
        for d in steps:
            k = pl.ds(pl.multiple_of(mod4(z + d) * 768, 128), 768)
            part = dot(X[:, k], W[k, lanes])
            acc = part if acc is None else acc + part
        return acc

    def by_pair(lanes, which):
        acc = None
        for zz in range(4):
            k = pl.ds(pl.multiple_of(zz * 768 + which * OWN, 128), OWN)
            part = dot(X[:, k], W[k, lanes])
            acc = part if acc is None else acc + part
        return acc

    here = x // 2
    with scope("partial"):

        def early(n, _):
            ACC[:, tile256(n, 0)] = by_row(tile256(n, 0), (0, 1, -1))
            ACC[:, tile256(n, GW)] = by_pair(tile256(n, GW), here)
            return 0

        lax.fori_loop(0, 4, early, 0)
        ACC[:, MAIN:GW] = by_row(slice(MAIN, GW), (0, 1, -1))

    with scope("d0relay"):
        run(d0, "relay")
        run(d0, "second", 1)
        run(d0, "second", 2)
    with scope("done"):
        run(gv, "done")
    with scope("p1"):
        run(d0, "across", 0)
        run(d0, "far")
        run(d1, "primary")
        run(d1, "second", 0)
    scale = NF[:, 2:3]
    with scope("gate"):

        def gate_tile(n, _):
            l = tile256(n, 0)
            GT[:, l] = ((ACC[:, l] + by_row(l, (2,))) * scale).astype(BF16)
            return 0

        lax.fori_loop(0, 4, gate_tile, 0)
        l = slice(MAIN, GW)
        GT[:, l] = ((ACC[:, l] + by_row(l, (2,))) * scale).astype(BF16)
    send("e", "e", GT.at[TOK - 16 : TOK, :], EDGE, at_sp(1))
    with scope("p2"):
        run(d0, "across", 1)
        run(d1, "relay")
        run(d1, "second", 1)
        run(d1, "second", 2)

    def hidden_of(lanes, width, taps, value):
        g = GT[:, lanes].astype(F32)
        edge = EDGE[:, lanes].astype(F32)
        t_at = lax.broadcasted_iota(jnp.int32, (TOK, width), 0)
        near = NF[:, 0:1] > 0.5
        far = NF[:, 1:2] > 0.5
        g1 = jnp.where(t_at == 0, edge[15:16], pltpu.roll(g, 1, 0))
        g2 = jnp.where(
            t_at == 0, edge[14:15], jnp.where(t_at == 1, edge[15:16], pltpu.roll(g, 2, 0))
        )
        conv = taps[2:3] * g + taps[1:2] * jnp.where(near, g1, 0.0) + taps[0:1] * jnp.where(far, g2, 0.0)
        return conv / (1.0 + jnp.exp(-conv)) * value

    def value_sum(n, _):
        l = tile256(n, GW)
        ACC[:, l] = ACC[:, l] + by_pair(l, 1 - here)
        return 0

    with scope("value"):
        lax.fori_loop(0, 2, value_sum, 0)
    with scope("p3"):
        run(d0, "across", 2)
        run(d1, "across", 0)
    with scope("value"):
        lax.fori_loop(2, 4, value_sum, 0)
    with scope("p4"):
        run(d0, "across", 3)
        run(d1, "far")
        run(d2, "primary")
        run(d2, "second", 0)
    with scope("edge"):
        recv("e", EDGE)

    with scope("hidden"):

        def hidden_tile(n, _):
            value = (ACC[:, tile256(n, GW)] * scale).astype(BF16).astype(F32)
            l = tile256(n, 0)
            HD[:, l] = hidden_of(l, 256, taps_ref[:, l], value).astype(BF16)
            return 0

        lax.fori_loop(0, 4, hidden_tile, 0)
        tail = slice(MAIN, GW)
        taps_tail = jnp.concatenate([taps_ref[:, MAIN : MAIN + 32], jnp.zeros((3, 96), F32)], axis=1)
        value_tail = pltpu.roll(GT[:, tail].astype(F32), 96, 1)
        HD[:, tail] = pltpu.roll(hidden_of(tail, 128, taps_tail, value_tail), 64, 1).astype(BF16)
    with scope("p5"):
        run(d1, "across", 1)
        run(d2, "relay")
        run(d2, "second", 1)
        run(d2, "second", 2)
        run(d0, "done")

    downs = (WD0, WD1, WD2)

    def partials(p, da, db, cc):
        mains, ends = [], []
        for d in (da, db):
            j = mod4(y + d) * 2 + cc
            mains.append(downs[p][pl.ds(pl.multiple_of(j * 128, 128), 128), :])
            for k in range(2):
                at = pl.multiple_of((j * 2 + k) * HW + p * PART, 16)
                ends.append(W[pl.ds(at, PART), MAIN:GW])
        return dot_t(HD[:, 0:MAIN], jnp.concatenate(mains, axis=0)) + dot_t(
            HD[:, MAIN:GW], jnp.concatenate(ends, axis=0)
        )

    order = (2, 1, -1, 0)

    def at_po(p, m):
        return pl.ds(m * OWN + p * 128, 128)

    def give(p, n):
        both = partials(p, order[n], order[n + 1], o).astype(BF16)
        for k in range(2):
            SP[n + k, :, pl.ds(p * 128, 128)] = both[:, k * 128 : (k + 1) * 128]
            l = pl.ds(p * 128, 128)
            send(("sp", p, n), "sp", SP.at[n + k, :, l], RP.at[n + k, :, l], partner)

    def keep(p, n):
        l = pl.ds(p * 128, 128)
        mine = partials(p, order[n], order[n + 1], c)
        with scope("sp%d" % n):
            recv(("sp", p, n), RP.at[pl.ds(n, 2), :, l])
        for k in range(2):
            m, d = n + k, order[n + k]
            both = mine[:, k * 128 : (k + 1) * 128] + RP[m, :, l].astype(F32)
            if d == 2:
                ZS[0, :, l] = both.astype(BF16)
                send(("rl", p), "rl", ZS.at[0, pl.ds(0, OWN), l], RL.at[0, :, l], at_y(1))
                send(("rl", p), "rl", ZS.at[0, pl.ds(OWN, OWN), l], RL.at[1, :, l], at_y(-1))
            else:
                ACC[:, at_po(p, m)] = both
                if d != 0:
                    r = pl.ds(OWN if d == 1 else 0, OWN)
                    ZS[m, r, l] = both[OWN:, :].astype(BF16) if d == 1 else both[:OWN, :].astype(BF16)
                    send(("rv", p), "rv", ZS.at[m, r, l], RV.at[m - 1, r, l], at_y(d))

    def pass_on(p):
        l = pl.ds(p * 128, 128)
        with scope("rl"):
            recv(("rl", p), RL.at[:, :, l])
        for n, d in ((1, 1), (2, -1)):
            r = pl.ds(0 if d == 1 else OWN, OWN)
            ZS[n, r, l] = (ACC[r, at_po(p, n)] + RL[n - 1, :, l].astype(F32)).astype(BF16)
            send(("rv", p), "rv", ZS.at[n, r, l], RV.at[n - 1, r, l], at_y(d))

    def collect(p):
        l = pl.ds(p * 128, 128)
        with scope("rv%d" % p):
            recv(("rv", p), RV.at[:, :, l])
        return ACC[:, at_po(p, 3)] + RV[0, :, l].astype(F32) + RV[1, :, l].astype(F32)

    with scope("reduce0"):
        give(0, 0)
        run(d1, "across", 2)
        give(0, 2)
        run(d2, "across", 0)
        keep(0, 0)
        run(d1, "across", 3)
        keep(0, 2)
        run(d2, "far")
    with scope("p6"):
        run(d2, "across", 1)
        run(d1, "done")
        pass_on(0)
    with scope("reduce1"):
        give(1, 0)
        run(d2, "across", 2)
        give(1, 2)
        run(d2, "across", 3)
        keep(1, 0)
        keep(1, 2)
    with scope("p7"):
        pass_on(1)
        run(d2, "done")
    with scope("reduce2"):
        give(2, 0)
        give(2, 2)
        keep(2, 0)
        keep(2, 2)
        pass_on(2)
    with scope("final"):
        low = lax.broadcasted_iota(jnp.int32, (TOK, 128), 1) < 64
        part0 = collect(0)
        turned = pltpu.roll(collect(1), 64, 1)
        out_ref[:, 0:128] = (RES[:, 0:128] + jnp.where(low, part0, turned)).astype(BF16)
        part2 = collect(2)
        out_ref[:, 128:256] = (RES[:, 128:256] + jnp.where(low, part2, part0)).astype(BF16)
        out_ref[:, 256:384] = (RES[:, 256:384] + jnp.where(low, turned, part2)).astype(BF16)
    with scope("sent"):
        for part in (gv, d0, d1, d2):
            run(part, "out")
        mix_g[4]()
        x_g[4]()
        sent("w", WO.at[pl.ds(0, 7 * HW), :])
        sent("st", SR)
        sent("mt", MR)
        sent("q", SS.at[pl.ds(0, 7)])
        sent("e", EDGE)
        sent("sp", SP)
        sent("rl", RL)
        sent("rv", RV)


def body(
    resid,
    query,
    keys,
    values,
    out_gate,
    in_gate,
    forget,
    doc_ids,
    head_gain,
    w_out,
    ffn_gain,
    w_gate,
    w_value,
    conv_taps,
    w_down,
):
    vmem = pl.BlockSpec(memory_space=pltpu.VMEM)
    hbm = pl.BlockSpec(memory_space=pl.ANY)
    return pl.pallas_call(
        kernel,
        out_shape=jax.ShapeDtypeStruct((TOK, OWN), BF16),
        in_specs=[hbm] * 15,
        out_specs=vmem,
        scratch_shapes=[
            pltpu.VMEM((3072, LANES), BF16),
            pltpu.VMEM((2, TOK), F32),
            pltpu.VMEM((2, TOK), F32),
            pltpu.VMEM((TOK,), jnp.int32),
            pltpu.VMEM((1, HW), F32),
            pltpu.VMEM((1, 3072), F32),
            pltpu.VMEM((3, 1056), F32),
            pltpu.VMEM((16 * PART, MAIN), BF16),
            pltpu.VMEM((16 * PART, MAIN), BF16),
            pltpu.VMEM((16 * PART, MAIN), BF16),
            pltpu.VMEM((3, HW, 32), BF16),
            pltpu.VMEM((TOK, 3072), BF16),
            pltpu.VMEM((1536, TOK), BF16),
            pltpu.VMEM((1536, OWN), BF16),
            pltpu.VMEM((OWN, 1536), BF16),
            pltpu.VMEM((HW, TOK), BF16),
            pltpu.VMEM((HW, TOK), BF16),
            pltpu.VMEM((HW, TOK), BF16),
            pltpu.VMEM((HW, TOK), BF16),
            pltpu.VMEM((TOK, OWN), BF16),
            pltpu.VMEM((HW, TOK), F32),
            pltpu.VMEM((TOK, 128), F32),
            pltpu.VMEM((HW, 128), BF16),
            pltpu.VMEM((4, HW, 128), BF16),
            pltpu.VMEM((8, 128), F32),
            pltpu.VMEM((4, 8, 128), F32),
            pltpu.VMEM((8, 8, TOK), F32),
            pltpu.VMEM((TOK, OWN), F32),
            pltpu.VMEM((TOK, LANES), F32),
            pltpu.VMEM((TOK, GW), BF16),
            pltpu.VMEM((16, GW), BF16),
            pltpu.VMEM((TOK, GW), BF16),
            pltpu.VMEM((4, TOK, OWN), BF16),
            pltpu.VMEM((4, TOK, OWN), BF16),
            pltpu.VMEM((3, TOK, OWN), BF16),
            pltpu.VMEM((2, OWN, OWN), BF16),
            pltpu.VMEM((2, TOK, OWN), BF16),
            pltpu.SemaphoreType.DMA((SEMS,)),
            pltpu.SemaphoreType.DMA((20,)),
        ],
        compiler_params=pltpu.CompilerParams(
            collective_id=0, has_side_effects=True, vmem_limit_bytes=VLIM * 1024 * 1024
        ),
    )(
        w_gate,
        w_value,
        w_down.T,
        query.T,
        keys.T,
        values.T,
        out_gate.T,
        w_out,
        resid,
        in_gate,
        forget,
        doc_ids,
        head_gain[None],
        ffn_gain[None],
        conv_taps,
    )


def solution(mesh):
    torus = Mesh(mesh.devices.reshape(4, 4, 4, 2), ("z", "x", "y", "c"))
    sp, tp = ("z", "x"), ("y", "c")
    placed = (
        P(sp, tp),
        P(sp, tp),
        P(sp, tp),
        P(sp, tp),
        P(sp, tp),
        P(tp, sp),
        P(tp, sp),
        P(sp),
        P(tp),
        P(tp, None),
        P(),
        P(sp, tp),
        P(sp, tp),
        P(None, tp),
        P(tp, sp),
    )
    return jax.shard_map(body, mesh=torus, in_specs=placed, out_specs=P(sp, tp), check_vma=False)
```

```python
import jax
import jax.numpy as jnp
from jax import lax
from jax.experimental import pallas as pl
from jax.experimental.pallas import tpu as pltpu
from jax.sharding import Mesh
from jax.sharding import PartitionSpec as P

MESH = pl.DeviceIdType.MESH
F32 = jnp.float32
BF16 = jnp.bfloat16
ABSENT = -1e30
DH = 96
TOK = 768
OWN = 384
HW = 192
MAIN = 1024
GW = 1152
LANES = 2176
PART = 64
EPS = 1e-6
VLIM = 60
SEMS = 94
scope = jax.named_scope


def mod4(v):
    return lax.rem(v + 8, 4)


def dot(a, b, **kw):
    return lax.dot_general(a, b, (((1,), (0,)), ((), ())), preferred_element_type=F32, **kw)


def dot_t(a, b, **kw):
    return lax.dot_general(a, b, (((1,), (1,)), ((), ())), preferred_element_type=F32, **kw)


def dot_c(a, b, **kw):
    return lax.dot_general(a, b, (((0,), (0,)), ((), ())), preferred_element_type=F32, **kw)


def kernel(
    wg_ref,
    wv_ref,
    wd_ref,
    q_hbm,
    k_hbm,
    v_hbm,
    og_hbm,
    wo_ref,
    resid_hbm,
    ig_hbm,
    fg_hbm,
    seg_hbm,
    hg_hbm,
    gain_hbm,
    taps_hbm,
    out_ref,
    W,
    ig_ref,
    fg_ref,
    seg_ref,
    hg_ref,
    gain_ref,
    taps_ref,
    WD0,
    WD1,
    WD2,
    TL,
    X,
    MIX,
    WO,
    WOT,
    QT,
    KT,
    VT,
    OG,
    RB,
    OI,
    NF,
    ST,
    SR,
    MT,
    MR,
    SS,
    RES,
    ACC,
    GT,
    EDGE,
    HD,
    SP,
    RP,
    ZS,
    RL,
    RV,
    sems,
    lsem,
):
    z, x = lax.axis_index("z"), lax.axis_index("x")
    y, c = lax.axis_index("y"), lax.axis_index("c")
    sp = z * 4 + x
    tp = y * 2 + c
    o = 1 - c
    table = {}
    rkey_any = "w"

    def slot(key):
        return table.setdefault(key, len(table))

    def copy(rkey, skey, src, dst, dev):
        return pltpu.make_async_remote_copy(
            src_ref=src,
            dst_ref=dst,
            send_sem=sems.at[slot(("S", skey))],
            recv_sem=sems.at[slot(("R", rkey))],
            device_id=dev,
            device_id_type=MESH,
        )

    def send(rkey, skey, src, dst, dev):
        copy(rkey, skey, src, dst, dev).start()

    partner = (z, x, y, o)

    def recv(rkey, span):
        copy(rkey, rkey_any, span, span, partner).wait_recv()

    def sent(skey, span):
        copy(rkey_any, skey, span, span, partner).wait_send()

    def at_sp(n):
        s = lax.rem(sp + n + 16, 16)
        return (s // 4, lax.rem(s, 4), y, c)

    def at_x(d):
        return (z, mod4(x + d), y, c)

    def at_z(d):
        return (mod4(z + d), x, y, c)

    def at_y(d):
        return (z, x, mod4(y + d), c)

    def at_tp(n):
        t = lax.rem(tp + n, 8)
        return (z, x, t // 2, lax.rem(t, 2))

    peers = [at_x(1), at_x(-1), at_z(1), at_z(-1)]
    peers += [at_tp(n) for n in range(1, 8)]
    peers += [at_sp(n) for n in (1, 2, 3, -1, -2, -3)]
    barrier = pltpu.get_barrier_semaphore()
    for dev in peers:
        pl.semaphore_signal(barrier, inc=1, device_id=dev, device_id_type=MESH)

    local = []

    def bring(src, dst):
        d = pltpu.make_async_copy(src, dst, lsem.at[len(local)])
        d.start()
        local.append(d)

    own_w = pl.ds(pl.multiple_of(sp * HW, 16), HW)
    bring(wg_ref.at[:, 0:MAIN], W.at[own_w, 0:MAIN])
    bring(wv_ref.at[:, 0:MAIN], W.at[own_w, GW:LANES])
    for n, ref in enumerate((wg_ref, wv_ref, wd_ref)):
        bring(ref.at[:, MAIN : MAIN + 32], TL.at[n])
    bring(fg_hbm, fg_ref)
    bring(ig_hbm, ig_ref)
    bring(seg_hbm, seg_ref)
    bring(k_hbm, KT)
    bring(v_hbm, VT)
    bring(q_hbm, QT)
    bring(og_hbm, OG)
    for n, ref in enumerate((WD0, WD1, WD2)):
        bring(
            wd_ref.at[n * PART : (n + 1) * PART, 0:MAIN],
            ref.at[pl.ds(pl.multiple_of(sp * PART, 16), PART), :],
        )
    bring(hg_hbm, hg_ref)
    bring(gain_hbm, gain_ref)
    bring(taps_hbm, taps_ref)
    bring(resid_hbm, RB)
    bring(
        wo_ref.at[:, pl.ds(pl.multiple_of(tp * OWN, 128), OWN)],
        WO.at[pl.ds(pl.multiple_of(tp * HW, 16), HW), :],
    )

    def stage(name, ref, stride, rows, lanes, by_lanes, first):
        x_first = first == "x"
        prim = at_x if x_first else at_z
        secd = at_z if x_first else at_x
        steps = (0, -1, 1, 2)

        def place(dp, ds, half=None):
            zz, xx = (mod4(z + ds), mod4(x + dp)) if x_first else (mod4(z + dp), mod4(x + ds))
            (r0, nr), (l0, nl) = rows, lanes
            if half is not None and by_lanes:
                l0, nl = l0 + half * nl // 2, nl // 2
            elif half is not None:
                r0, nr = r0 + half * nr // 2, nr // 2
            row = pl.multiple_of((zz * 4 + xx) * stride + r0, 16)
            return ref.at[pl.ds(row, nr), pl.ds(l0, nl)]

        def span(k):
            return ref.at[pl.ds(0, k * rows[1]), pl.ds(lanes[0], lanes[1])]

        def primary():
            for d in (1, -1):
                send((name, "p"), name, place(0, 0), place(0, 0), prim(d))

        def second(m):
            p = place(steps[m], 0)
            for d in (1, -1):
                send((name, "s", m), name, p, p, secd(d))

        def relay():
            recv((name, "p"), span(2))
            for d in (1, -1):
                p = place(-d, 0, 0 if d == 1 else 1)
                send((name, "pf"), name, p, p, prim(d))

        def across(m):
            recv((name, "s", m), span(2))
            for d in (1, -1):
                p = place(steps[m], -d, 0 if d == 1 else 1)
                send((name, "sf"), name, p, p, secd(d))

        def far():
            recv((name, "pf"), span(1))
            second(3)

        def done():
            recv((name, "sf"), span(4))

        def out():
            sent(name, span(15))

        return primary, second, relay, across, far, done, out

    def run(stages, what, *args):
        k = ("primary", "second", "relay", "across", "far", "done", "out").index(what)
        for st in stages:
            st[k](*args)

    gv = (
        stage("g", W, HW, (0, HW), (0, GW), False, "x"),
        stage("v", W, HW, (0, HW), (GW, MAIN), False, "z"),
    )

    def down_stage(n, ref, cut):
        return (
            stage(("da", n), ref, PART, (0, cut), (0, MAIN), True, "x"),
            stage(("db", n), ref, PART, (cut, PART - cut), (0, MAIN), True, "z"),
        )

    d0, d1, d2 = down_stage(0, WD0, 16), down_stage(1, WD1, 32), down_stage(2, WD2, 32)

    def over_tp(name, blk, span):
        def g0():
            b = blk(y, c)
            for d in (1, -1):
                send((name, "y"), name, b, b, at_y(d))
            send((name, "o"), name, b, b, partner)

        def g1():
            recv((name, "y"), span(2))
            for d in (1, -1):
                h = blk(mod4(y - d), c, 0 if d == 1 else 1)
                send((name, "f"), name, h, h, at_y(d))
            for d in (1, -1):
                b = blk(mod4(y - d), c)
                send((name, "o"), name, b, b, partner)

        def g2():
            recv((name, "f"), span(1))
            b = blk(mod4(y + 2), c)
            send((name, "o"), name, b, b, partner)

        def g3():
            recv((name, "o"), span(4))

        def out():
            sent(name, span(7))

        return g0, g1, g2, g3, out

    def mix_block(yy, cc, half=None):
        r0, nr = (0, HW) if half is None else (half * DH, DH)
        return MIX.at[pl.ds(pl.multiple_of((yy * 2 + cc) * HW + r0, 16), nr), :]

    def x_block(yy, cc, half=None):
        rows = slice(None) if half is None else pl.ds(half * OWN, OWN)
        return X.at[rows, pl.ds(pl.multiple_of((yy * 2 + cc) * OWN, 128), OWN)]

    mix_g = over_tp("m", mix_block, lambda k: MIX.at[pl.ds(0, k * HW), :])
    x_g = over_tp("x", x_block, lambda k: X.at[:, pl.ds(0, k * OWN)])

    for d in local[:5]:
        d.wait()
    tails = jnp.concatenate([TL[0], TL[1], TL[2], jnp.zeros((HW, 32), BF16)], axis=1)
    W[own_w, MAIN:GW] = tails
    with scope("barrier"):
        pl.semaphore_wait(barrier, len(peers))
    run(gv[1:], "primary")
    run(gv[:1], "primary")
    for n in range(1, 8):
        t = lax.rem(tp + n, 8)
        src = wo_ref.at[:, pl.ds(pl.multiple_of(t * OWN, 128), OWN)]
        dst = WO.at[pl.ds(pl.multiple_of(tp * HW, 16), HW), :]
        send("w", "w", src, dst, at_tp(n))

    lane = lax.broadcasted_iota(jnp.int32, (8, TOK), 1)
    row8 = lax.broadcasted_iota(jnp.int32, (8, TOK), 0)
    for d in local[5:8]:
        d.wait()
    seg = seg_ref[...].reshape(1, TOK).astype(F32)
    fg = jnp.where(row8 == 0, fg_ref[0:1], fg_ref[1:2])
    e = jnp.exp(-jnp.abs(fg))
    log1p = jnp.where(e < 1e-2, e * (1.0 - e * (0.5 - e * (1.0 / 3.0))), jnp.log(1.0 + e))
    cum = jnp.minimum(fg, 0.0) - log1p
    shift = 1
    while shift < TOK:
        cum = cum + jnp.where(lane >= shift, pltpu.roll(cum, shift, 1), 0.0)
        shift *= 2
    b = [ig_ref[h : h + 1] - cum[h : h + 1] for h in range(2)]
    end = [cum[h : h + 1, TOK - 1 :] for h in range(2)]
    first, last, second_last = seg[:, :1], seg[:, TOK - 1 :], seg[:, TOK - 2 : TOK - 1]
    for d in local[8:12]:
        d.wait()
    ST[...] = jnp.zeros_like(ST)
    peak = []
    for h in range(2):
        hs = slice(h * DH, h * DH + DH)
        top = jnp.max(jnp.where(seg == last, b[h], ABSENT), axis=1, keepdims=True)
        peak.append(top)
        w = jnp.where(seg == last, jnp.exp(jnp.minimum(b[h] - top, 0.0)), 0.0) * DH**-0.5
        ST[hs, 0:DH] = dot_t(VT[hs, :], (KT[hs, :].astype(F32) * w).astype(BF16)).astype(BF16)
    meta_row = lax.broadcasted_iota(jnp.int32, (8, 128), 0)
    meta = jnp.zeros((8, 128), F32)
    for n, value in enumerate((end[0] + peak[0], end[1] + peak[1], end[0], end[1], first, last, second_last)):
        meta = jnp.where(meta_row == n, value, meta)
    MT[...] = meta
    for n in range(1, 5):
        send("st", "st", ST, SR.at[n - 1], at_sp(n))
        send("mt", "mt", MT, MR.at[n - 1], at_sp(n))
    run(gv, "second", 0)

    rows = jnp.where(row8 == 0, b[0], jnp.where(row8 == 1, b[1], seg))
    cols = jnp.transpose(jnp.concatenate([rows, jnp.zeros((120, TOK), F32)], axis=0))
    seg_c = cols[:, 2:3]
    tops = [[], []]
    for i in range(3):
        t0, ns = i * 256, (i + 1) * 256
        ts = slice(t0, t0 + 256)
        s_at = lax.broadcasted_iota(jnp.int32, (ns, 256), 0)
        t_at = lax.broadcasted_iota(jnp.int32, (ns, 256), 1) + t0
        mask = (seg_c[:ns] == seg[:, ts]) & (s_at <= t_at)
        for h in range(2):
            hs = slice(h * DH, h * DH + DH)
            masked = jnp.where(mask, cols[:ns, h : h + 1], ABSENT)
            top = jnp.max(masked, axis=0, keepdims=True)
            scores = dot_c(KT[hs, 0:ns], QT[hs, ts]) * (jnp.exp(masked - top) * DH**-0.5)
            OI[hs, ts] = dot(VT[hs, 0:ns], scores.astype(BF16))
            tops[h].append(top)

    with scope("relay"):
        run(gv, "relay")
        run(gv, "second", 1)
        run(gv, "second", 2)

    dec = [jnp.zeros((1, 128), F32)] * 2
    cand = [[], []]
    first_l = jnp.broadcast_to(first, (1, 128))
    with scope("state"):
        recv("st", SR)
        recv("mt", MR)
    for n in range(1, 5):
        m = MR[n - 1]
        valid = (m[5:6] == first_l) & (sp >= n)
        for h in range(2):
            cand[h].append(jnp.where(valid, m[h : h + 1] + dec[h], ABSENT))
            dec[h] = dec[h] + m[2 + h : 3 + h]
    for d in local[12:18]:
        d.wait()
    gain_at = lax.broadcasted_iota(jnp.int32, (HW, HW), 0) == lax.broadcasted_iota(jnp.int32, (HW, HW), 1)
    gain_c = jnp.sum(jnp.where(gain_at, hg_ref[...], 0.0), axis=1, keepdims=True)
    for h in range(2):
        hs = slice(h * DH, h * DH + DH)
        pin = jnp.maximum(
            jnp.maximum(cand[h][0], cand[h][1]), jnp.maximum(cand[h][2], cand[h][3])
        )
        state = jnp.zeros((DH, 128), F32)
        for n in range(4):
            state = state + jnp.exp(cand[h][n] - pin) * SR[n, hs, :].astype(F32)
        inter = dot(state[:, 0:DH].astype(BF16), QT[hs, :])
        m_in = jnp.concatenate(tops[h], axis=1)
        m_pin = jnp.where(seg == first, pin[:, :1], ABSENT)
        m_all = jnp.maximum(m_in, m_pin)
        memory = jnp.exp(m_in - m_all) * OI[hs, :] + jnp.exp(m_pin - m_all) * inter
        mean = jnp.sum(memory * memory, axis=0, keepdims=True) * (1.0 / DH)
        mix = memory * lax.rsqrt(mean + 1.0) * gain_c[hs] * jax.nn.sigmoid(OG[hs, :].astype(F32))
        MIX[pl.ds(pl.multiple_of(tp * HW + h * DH, 16), DH), :] = mix.astype(BF16)
    with scope("mix0"):
        mix_g[0]()
    with scope("across0"):
        run(gv, "across", 0)

    before = MR[0]
    there = sp >= 1
    last_before = jnp.where(there, before[5:6, :1], -1.0)
    second_before = jnp.where(there, before[6:7, :1], -1.0)
    seg8 = jnp.broadcast_to(seg, (8, TOK))
    one_back = jnp.where(lane == 0, last_before, pltpu.roll(seg8, 1, 1))
    two_back = jnp.where(
        lane == 0, second_before, jnp.where(lane == 1, last_before, pltpu.roll(seg8, 2, 1))
    )
    flags = jnp.where(
        row8 == 0, jnp.where(one_back == seg, 1.0, 0.0), jnp.where(two_back == seg, 1.0, 0.0)
    )
    NF[...] = jnp.transpose(jnp.concatenate([flags, jnp.zeros((120, TOK), F32)], axis=0))
    with scope("wo"):
        for d in local[18:]:
            d.wait()
        recv("w", WO.at[pl.ds(0, 7 * HW), :])
        WOT[...] = jnp.transpose(WO[...])

    with scope("mix1"):
        mix_g[1]()
    with scope("far"):
        run(gv, "far")
    with scope("mix2"):
        mix_g[2]()
    with scope("mix3"):
        mix_g[3]()

    gain = gain_ref[:, pl.ds(pl.multiple_of(tp * OWN, 128), OWN)]
    res = RB[...].astype(F32) + jnp.transpose(dot(WOT[...], MIX[...]))
    RES[...] = res
    X[:, pl.ds(pl.multiple_of(tp * OWN, 128), OWN)] = (res * gain).astype(BF16)
    x_g[0]()
    SS[tp] = dot_t(jnp.ones((8, OWN), F32), res * res, precision=lax.Precision.HIGHEST)
    for n in range(1, 8):
        send("q", "q", SS.at[tp], SS.at[tp], at_tp(n))
    with scope("across1"):
        run(gv, "across", 1)
    with scope("across2"):
        run(gv, "across", 2)
    with scope("x1"):
        x_g[1]()
    with scope("x2"):
        x_g[2]()
    with scope("x3"):
        x_g[3]()
    run(d0, "primary")
    run(d0, "second", 0)
    with scope("across3"):
        run(gv, "across", 3)
    with scope("sq"):
        recv("q", SS.at[pl.ds(0, 7)])
        total = SS[0]
        for n in range(1, 8):
            total = total + SS[n]
    scale_row = lax.rsqrt(total * (1.0 / 3072.0) + EPS)
    NF[:, 2:3] = jnp.transpose(jnp.concatenate([scale_row, jnp.zeros((120, TOK), F32)], axis=0))[:, 0:1]

    def tile256(n, at):
        return pl.ds(pl.multiple_of(n * 256 + at, 128), 256)

    def by_row(lanes, steps):
        acc = None
        for d in steps:
            k = pl.ds(pl.multiple_of(mod4(z + d) * 768, 128), 768)
            part = dot(X[:, k], W[k, lanes])
            acc = part if acc is None else acc + part
        return acc

    def by_pair(lanes, which):
        acc = None
        for zz in range(4):
            k = pl.ds(pl.multiple_of(zz * 768 + which * OWN, 128), OWN)
            part = dot(X[:, k], W[k, lanes])
            acc = part if acc is None else acc + part
        return acc

    here = x // 2
    with scope("partial"):

        def early(n, _):
            ACC[:, tile256(n, 0)] = by_row(tile256(n, 0), (0, 1, -1))
            ACC[:, tile256(n, GW)] = by_pair(tile256(n, GW), here)
            return 0

        lax.fori_loop(0, 4, early, 0)
        ACC[:, MAIN:GW] = by_row(slice(MAIN, GW), (0, 1, -1))

    with scope("d0relay"):
        run(d0, "relay")
        run(d0, "second", 1)
        run(d0, "second", 2)
        run(d1, "primary")
        run(d1, "second", 0)
    with scope("done"):
        run(gv, "done")
    with scope("p1"):
        run(d0, "across", 0)
        run(d0, "far")
    scale = NF[:, 2:3]
    with scope("gate"):

        def gate_tile(n, _):
            l = tile256(n, 0)
            GT[:, l] = ((ACC[:, l] + by_row(l, (2,))) * scale).astype(BF16)
            return 0

        lax.fori_loop(0, 4, gate_tile, 0)
        l = slice(MAIN, GW)
        GT[:, l] = ((ACC[:, l] + by_row(l, (2,))) * scale).astype(BF16)
    send("e", "e", GT.at[TOK - 16 : TOK, :], EDGE, at_sp(1))
    with scope("p2"):
        run(d0, "across", 1)
        run(d0, "across", 2)

    def hidden_of(lanes, width, taps, value):
        g = GT[:, lanes].astype(F32)
        edge = EDGE[:, lanes].astype(F32)
        t_at = lax.broadcasted_iota(jnp.int32, (TOK, width), 0)
        near = NF[:, 0:1] > 0.5
        far = NF[:, 1:2] > 0.5
        g1 = jnp.where(t_at == 0, edge[15:16], pltpu.roll(g, 1, 0))
        g2 = jnp.where(
            t_at == 0, edge[14:15], jnp.where(t_at == 1, edge[15:16], pltpu.roll(g, 2, 0))
        )
        conv = taps[2:3] * g + taps[1:2] * jnp.where(near, g1, 0.0) + taps[0:1] * jnp.where(far, g2, 0.0)
        return conv / (1.0 + jnp.exp(-conv)) * value

    def value_sum(n, _):
        l = tile256(n, GW)
        ACC[:, l] = ACC[:, l] + by_pair(l, 1 - here)
        return 0

    with scope("value"):
        lax.fori_loop(0, 2, value_sum, 0)
    with scope("p3"):
        run(d1, "relay")
    with scope("value"):
        lax.fori_loop(2, 4, value_sum, 0)
    with scope("p4"):
        run(d0, "across", 3)
        run(d1, "second", 1)
        run(d1, "second", 2)
        run(d2, "primary")
        run(d2, "second", 0)
        run(d1, "across", 0)
    with scope("edge"):
        recv("e", EDGE)

    with scope("hidden"):

        def hidden_tile(n, _):
            value = (ACC[:, tile256(n, GW)] * scale).astype(BF16).astype(F32)
            l = tile256(n, 0)
            HD[:, l] = hidden_of(l, 256, taps_ref[:, l], value).astype(BF16)
            return 0

        lax.fori_loop(0, 4, hidden_tile, 0)
        tail = slice(MAIN, GW)
        taps_tail = jnp.concatenate([taps_ref[:, MAIN : MAIN + 32], jnp.zeros((3, 96), F32)], axis=1)
        value_tail = pltpu.roll(GT[:, tail].astype(F32), 96, 1)
        HD[:, tail] = pltpu.roll(hidden_of(tail, 128, taps_tail, value_tail), 64, 1).astype(BF16)
    with scope("p5"):
        run(d1, "far")
        run(d0, "done")

    downs = (WD0, WD1, WD2)

    def partials(p, cc):
        mains, ends = [], []
        for d in order:
            j = mod4(y + d) * 2 + cc
            mains.append(downs[p][pl.ds(pl.multiple_of(j * 128, 128), 128), :])
            for k in range(2):
                at = pl.multiple_of((j * 2 + k) * HW + p * PART, 16)
                ends.append(W[pl.ds(at, PART), MAIN:GW])
        return dot_t(HD[:, 0:MAIN], jnp.concatenate(mains, axis=0)) + dot_t(
            HD[:, MAIN:GW], jnp.concatenate(ends, axis=0)
        )

    order = (2, 1, -1, 0)

    def at_po(p, m):
        return pl.ds(m * OWN + p * 128, 128)

    def give(p):
        l = pl.ds(p * 128, 128)
        both = partials(p, o).astype(BF16)
        for n in range(4):
            SP[n, :, l] = both[:, n * 128 : (n + 1) * 128]
            send(("sp", p), "sp", SP.at[n, :, l], RP.at[n, :, l], partner)

    def keep(p):
        l = pl.ds(p * 128, 128)
        mine = partials(p, c)
        with scope("sp"):
            recv(("sp", p), RP.at[:, :, l])
        for n, d in enumerate(order):
            both = mine[:, n * 128 : (n + 1) * 128] + RP[n, :, l].astype(F32)
            if d == 2:
                ZS[0, :, l] = both.astype(BF16)
                send(("rl", p), "rl", ZS.at[0, pl.ds(0, OWN), l], RL.at[0, :, l], at_y(1))
                send(("rl", p), "rl", ZS.at[0, pl.ds(OWN, OWN), l], RL.at[1, :, l], at_y(-1))
            else:
                ACC[:, at_po(p, n)] = both
                if d != 0:
                    r = pl.ds(OWN if d == 1 else 0, OWN)
                    ZS[n, r, l] = both[OWN:, :].astype(BF16) if d == 1 else both[:OWN, :].astype(BF16)
                    send(("rv", p), "rv", ZS.at[n, r, l], RV.at[n - 1, r, l], at_y(d))

    def pass_on(p):
        l = pl.ds(p * 128, 128)
        with scope("rl"):
            recv(("rl", p), RL.at[:, :, l])
        for n, d in ((1, 1), (2, -1)):
            r = pl.ds(0 if d == 1 else OWN, OWN)
            ZS[n, r, l] = (ACC[r, at_po(p, n)] + RL[n - 1, :, l].astype(F32)).astype(BF16)
            send(("rv", p), "rv", ZS.at[n, r, l], RV.at[n - 1, r, l], at_y(d))

    def collect(p):
        l = pl.ds(p * 128, 128)
        with scope("rv%d" % p):
            recv(("rv", p), RV.at[:, :, l])
        return ACC[:, at_po(p, 3)] + RV[0, :, l].astype(F32) + RV[1, :, l].astype(F32)

    with scope("give0"):
        give(0)
    with scope("p6"):
        run(d1, "across", 1)
        run(d2, "relay")
        run(d2, "second", 1)
        run(d2, "second", 2)
    with scope("keep0"):
        keep(0)
    with scope("p7"):
        run(d1, "across", 2)
        run(d1, "across", 3)
        run(d2, "across", 0)
        run(d2, "far")
    with scope("p8"):
        run(d2, "across", 1)
        run(d1, "done")
    with scope("give1"):
        give(1)
    with scope("p8b"):
        run(d2, "across", 2)
        run(d2, "across", 3)
    with scope("pass0"):
        pass_on(0)
    with scope("keep1"):
        keep(1)
    with scope("p10"):
        run(d2, "done")
    with scope("give2"):
        give(2)
    with scope("pass1"):
        pass_on(1)
    with scope("keep2"):
        keep(2)
    with scope("pass2"):
        pass_on(2)
    with scope("final0"):
        low = lax.broadcasted_iota(jnp.int32, (TOK, 128), 1) < 64
        part0 = collect(0)
        turned = pltpu.roll(collect(1), 64, 1)
        out_ref[:, 0:128] = (RES[:, 0:128] + jnp.where(low, part0, turned)).astype(BF16)
        RES[:, 128:256] = RES[:, 128:256] + jnp.where(low, ACC[:, at_po(2, 3)], part0)
        RES[:, 256:384] = RES[:, 256:384] + jnp.where(low, turned, ACC[:, at_po(2, 3)])
    with scope("final"):
        l = pl.ds(256, 128)
        with scope("rv2"):
            recv(("rv", 2), RV.at[:, :, l])
        part2 = RV[0, :, l].astype(F32) + RV[1, :, l].astype(F32)
        out_ref[:, 128:256] = (RES[:, 128:256] + jnp.where(low, part2, 0.0)).astype(BF16)
        out_ref[:, 256:384] = (RES[:, 256:384] + jnp.where(low, 0.0, part2)).astype(BF16)
    with scope("sent"):
        for part in (gv, d0, d1, d2):
            run(part, "out")
        mix_g[4]()
        x_g[4]()
        sent("w", WO.at[pl.ds(0, 7 * HW), :])
        sent("st", SR)
        sent("mt", MR)
        sent("q", SS.at[pl.ds(0, 7)])
        sent("e", EDGE)
        sent("sp", SP)
        sent("rl", RL)
        sent("rv", RV)
    if len(table) != SEMS:
        raise ValueError(len(table))


def body(
    resid,
    query,
    keys,
    values,
    out_gate,
    in_gate,
    forget,
    doc_ids,
    head_gain,
    w_out,
    ffn_gain,
    w_gate,
    w_value,
    conv_taps,
    w_down,
):
    vmem = pl.BlockSpec(memory_space=pltpu.VMEM)
    hbm = pl.BlockSpec(memory_space=pl.ANY)
    return pl.pallas_call(
        kernel,
        out_shape=pltpu.VMEM((TOK, OWN), BF16),
        in_specs=[hbm] * 15,
        out_specs=vmem,
        scratch_shapes=[
            pltpu.VMEM((3072, LANES), BF16),
            pltpu.VMEM((2, TOK), F32),
            pltpu.VMEM((2, TOK), F32),
            pltpu.VMEM((TOK,), jnp.int32),
            pltpu.VMEM((1, HW), F32),
            pltpu.VMEM((1, 3072), F32),
            pltpu.VMEM((3, 1056), F32),
            pltpu.VMEM((16 * PART, MAIN), BF16),
            pltpu.VMEM((16 * PART, MAIN), BF16),
            pltpu.VMEM((16 * PART, MAIN), BF16),
            pltpu.VMEM((3, HW, 32), BF16),
            pltpu.VMEM((TOK, 3072), BF16),
            pltpu.VMEM((1536, TOK), BF16),
            pltpu.VMEM((1536, OWN), BF16),
            pltpu.VMEM((OWN, 1536), BF16),
            pltpu.VMEM((HW, TOK), BF16),
            pltpu.VMEM((HW, TOK), BF16),
            pltpu.VMEM((HW, TOK), BF16),
            pltpu.VMEM((HW, TOK), BF16),
            pltpu.VMEM((TOK, OWN), BF16),
            pltpu.VMEM((HW, TOK), F32),
            pltpu.VMEM((TOK, 128), F32),
            pltpu.VMEM((HW, 128), BF16),
            pltpu.VMEM((4, HW, 128), BF16),
            pltpu.VMEM((8, 128), F32),
            pltpu.VMEM((4, 8, 128), F32),
            pltpu.VMEM((8, 8, TOK), F32),
            pltpu.VMEM((TOK, OWN), F32),
            pltpu.VMEM((TOK, LANES), F32),
            pltpu.VMEM((TOK, GW), BF16),
            pltpu.VMEM((16, GW), BF16),
            pltpu.VMEM((TOK, GW), BF16),
            pltpu.VMEM((4, TOK, OWN), BF16),
            pltpu.VMEM((4, TOK, OWN), BF16),
            pltpu.VMEM((3, TOK, OWN), BF16),
            pltpu.VMEM((2, OWN, OWN), BF16),
            pltpu.VMEM((2, TOK, OWN), BF16),
            pltpu.SemaphoreType.DMA((SEMS,)),
            pltpu.SemaphoreType.DMA((20,)),
        ],
        compiler_params=pltpu.CompilerParams(
            collective_id=0, has_side_effects=True, vmem_limit_bytes=VLIM * 1024 * 1024
        ),
    )(
        w_gate,
        w_value,
        w_down.T,
        query.T,
        keys.T,
        values.T,
        out_gate.T,
        w_out,
        resid,
        in_gate,
        forget,
        doc_ids,
        head_gain[None],
        ffn_gain[None],
        conv_taps,
    )


def solution(mesh):
    torus = Mesh(mesh.devices.reshape(4, 4, 4, 2), ("z", "x", "y", "c"))
    sp, tp = ("z", "x"), ("y", "c")
    placed = (
        P(sp, tp),
        P(sp, tp),
        P(sp, tp),
        P(sp, tp),
        P(sp, tp),
        P(tp, sp),
        P(tp, sp),
        P(sp),
        P(tp),
        P(tp, None),
        P(),
        P(sp, tp),
        P(sp, tp),
        P(None, tp),
        P(tp, sp),
    )
    return jax.shard_map(body, mesh=torus, in_specs=placed, out_specs=P(sp, tp), check_vma=False)
```

```python
import jax
import jax.numpy as jnp
from jax import lax
from jax.experimental import pallas as pl
from jax.experimental.pallas import tpu as pltpu
from jax.sharding import Mesh
from jax.sharding import PartitionSpec as P

MESH = pl.DeviceIdType.MESH
F32 = jnp.float32
BF16 = jnp.bfloat16
ABSENT = -1e30
DH = 96
TOK = 768
OWN = 384
HW = 192
MAIN = 1024
GW = 1152
LANES = 2176
PART = 64
EPS = 1e-6
EVERY, FAR, REST = (0, 1, 2, 3), (0,), (1, 2, 3)
VLIM = 60
SEMS = 95
scope = jax.named_scope


def mod4(v):
    return lax.rem(v + 8, 4)


def dot(a, b, **kw):
    return lax.dot_general(a, b, (((1,), (0,)), ((), ())), preferred_element_type=F32, **kw)


def dot_t(a, b, **kw):
    return lax.dot_general(a, b, (((1,), (1,)), ((), ())), preferred_element_type=F32, **kw)


def dot_c(a, b, **kw):
    return lax.dot_general(a, b, (((0,), (0,)), ((), ())), preferred_element_type=F32, **kw)


def kernel(
    wg_ref,
    wv_ref,
    wd_ref,
    q_hbm,
    k_hbm,
    v_hbm,
    og_hbm,
    wo_ref,
    resid_hbm,
    ig_hbm,
    fg_hbm,
    seg_hbm,
    hg_hbm,
    gain_hbm,
    taps_hbm,
    out_ref,
    W,
    ig_ref,
    fg_ref,
    seg_ref,
    hg_ref,
    gain_ref,
    taps_ref,
    WD0,
    WD1,
    WD2,
    TL,
    X,
    MIX,
    WO,
    WOT,
    QT,
    KT,
    VT,
    OG,
    RB,
    OI,
    NF,
    ST,
    SR,
    MT,
    MR,
    SS,
    RES,
    ACC,
    GT,
    EDGE,
    HD,
    SP,
    RP,
    ZS,
    RL,
    RV,
    sems,
    lsem,
):
    z, x = lax.axis_index("z"), lax.axis_index("x")
    y, c = lax.axis_index("y"), lax.axis_index("c")
    sp = z * 4 + x
    tp = y * 2 + c
    o = 1 - c
    table = {}
    rkey_any = "w"

    def slot(key):
        return table.setdefault(key, len(table))

    def copy(rkey, skey, src, dst, dev):
        return pltpu.make_async_remote_copy(
            src_ref=src,
            dst_ref=dst,
            send_sem=sems.at[slot(("S", skey))],
            recv_sem=sems.at[slot(("R", rkey))],
            device_id=dev,
            device_id_type=MESH,
        )

    def send(rkey, skey, src, dst, dev):
        copy(rkey, skey, src, dst, dev).start()

    partner = (z, x, y, o)

    def recv(rkey, span):
        copy(rkey, rkey_any, span, span, partner).wait_recv()

    def sent(skey, span):
        copy(rkey_any, skey, span, span, partner).wait_send()

    def at_sp(n):
        s = lax.rem(sp + n + 16, 16)
        return (s // 4, lax.rem(s, 4), y, c)

    def at_x(d):
        return (z, mod4(x + d), y, c)

    def at_z(d):
        return (mod4(z + d), x, y, c)

    def at_y(d):
        return (z, x, mod4(y + d), c)

    def at_tp(n):
        t = lax.rem(tp + n, 8)
        return (z, x, t // 2, lax.rem(t, 2))

    peers = [at_x(1), at_x(-1), at_z(1), at_z(-1)]
    peers += [at_tp(n) for n in range(1, 8)]
    peers += [at_sp(n) for n in (1, 2, 3, -1, -2, -3)]
    barrier = pltpu.get_barrier_semaphore()
    for dev in peers:
        pl.semaphore_signal(barrier, inc=1, device_id=dev, device_id_type=MESH)

    local = []

    def bring(src, dst):
        d = pltpu.make_async_copy(src, dst, lsem.at[len(local)])
        d.start()
        local.append(d)

    own_w = pl.ds(pl.multiple_of(sp * HW, 16), HW)
    bring(wg_ref.at[:, 0:MAIN], W.at[own_w, 0:MAIN])
    bring(wv_ref.at[:, 0:MAIN], W.at[own_w, GW:LANES])
    for n, ref in enumerate((wg_ref, wv_ref, wd_ref)):
        bring(ref.at[:, MAIN : MAIN + 32], TL.at[n])
    bring(fg_hbm, fg_ref)
    bring(ig_hbm, ig_ref)
    bring(seg_hbm, seg_ref)
    bring(k_hbm, KT)
    bring(v_hbm, VT)
    bring(q_hbm, QT)
    bring(og_hbm, OG)
    for n, ref in enumerate((WD0, WD1, WD2)):
        bring(
            wd_ref.at[n * PART : (n + 1) * PART, 0:MAIN],
            ref.at[pl.ds(pl.multiple_of(sp * PART, 16), PART), :],
        )
    bring(hg_hbm, hg_ref)
    bring(gain_hbm, gain_ref)
    bring(taps_hbm, taps_ref)
    bring(resid_hbm, RB)
    bring(
        wo_ref.at[:, pl.ds(pl.multiple_of(tp * OWN, 128), OWN)],
        WO.at[pl.ds(pl.multiple_of(tp * HW, 16), HW), :],
    )

    def stage(name, ref, stride, rows, lanes, by_lanes, first):
        x_first = first == "x"
        prim = at_x if x_first else at_z
        secd = at_z if x_first else at_x
        steps = (0, -1, 1, 2)

        def place(dp, ds, half=None, shift=0):
            zz, xx = (mod4(z + ds), mod4(x + dp)) if x_first else (mod4(z + dp), mod4(x + ds))
            (r0, nr), (l0, nl) = rows, lanes
            if half is not None and by_lanes:
                l0, nl = l0 + half * nl // 2, nl // 2
            elif half is not None:
                upper = nr // 2 - shift
                r0, nr = (r0 + upper, nr - upper) if half else (r0, upper)
            row = pl.multiple_of((zz * 4 + xx) * stride + r0, 16)
            return ref.at[pl.ds(row, nr), pl.ds(l0, nl)]

        def span(k):
            return ref.at[pl.ds(0, k * rows[1]), pl.ds(lanes[0], lanes[1])]

        def primary():
            for d in (1, -1):
                send((name, "p"), name, place(0, 0), place(0, 0), prim(d))

        def second(m):
            p = place(steps[m], 0)
            for d in (1, -1):
                send((name, "s", m), name, p, p, secd(d))

        def relay():
            recv((name, "p"), span(2))
            for d in (1, -1):
                p = place(-d, 0, 0 if d == 1 else 1)
                send((name, "pf"), name, p, p, prim(d))

        def across(m):
            recv((name, "s", m), span(2))
            for d in (1, -1):
                p = place(steps[m], -d, 0 if d == 1 else 1, 16 if m in (1, 2) else 0)
                send((name, "sf"), name, p, p, secd(d))

        def far():
            recv((name, "pf"), span(1))
            second(3)

        def done():
            recv((name, "sf"), span(4))

        def out():
            sent(name, span(15))

        return primary, second, relay, across, far, done, out

    def run(stages, what, *args):
        k = ("primary", "second", "relay", "across", "far", "done", "out").index(what)
        for st in stages:
            st[k](*args)

    gv = (
        stage("g", W, HW, (0, HW), (0, GW), False, "x"),
        stage("v", W, HW, (0, HW), (GW, MAIN), False, "z"),
    )

    def down_stage(n, ref, cut):
        return (
            stage(("da", n), ref, PART, (0, cut), (0, MAIN), True, "x"),
            stage(("db", n), ref, PART, (cut, PART - cut), (0, MAIN), True, "z"),
        )

    d0, d1, d2 = down_stage(0, WD0, 16), down_stage(1, WD1, 32), down_stage(2, WD2, 32)

    def over_tp(name, blk, span):
        def g0():
            b = blk(y, c)
            for d in (1, -1):
                send((name, "y"), name, b, b, at_y(d))
            send((name, "o"), name, b, b, partner)

        def g1():
            recv((name, "y"), span(2))
            for d in (1, -1):
                h = blk(mod4(y - d), c, 0 if d == 1 else 1)
                send((name, "f"), name, h, h, at_y(d))
            for d in (1, -1):
                b = blk(mod4(y - d), c)
                send((name, "o"), name, b, b, partner)

        def g2():
            recv((name, "f"), span(1))
            b = blk(mod4(y + 2), c)
            send((name, "o"), name, b, b, partner)

        def g3():
            recv((name, "o"), span(4))

        def out():
            sent(name, span(7))

        return g0, g1, g2, g3, out

    def mix_block(yy, cc, half=None):
        r0, nr = (0, HW) if half is None else (half * DH, DH)
        return MIX.at[pl.ds(pl.multiple_of((yy * 2 + cc) * HW + r0, 16), nr), :]

    def x_block(yy, cc, half=None):
        rows = slice(None) if half is None else pl.ds(half * OWN, OWN)
        return X.at[rows, pl.ds(pl.multiple_of((yy * 2 + cc) * OWN, 128), OWN)]

    mix_g = over_tp("m", mix_block, lambda k: MIX.at[pl.ds(0, k * HW), :])
    x_g = over_tp("x", x_block, lambda k: X.at[:, pl.ds(0, k * OWN)])

    for d in local[:5]:
        d.wait()
    tails = jnp.concatenate([TL[0], TL[1], TL[2], jnp.zeros((HW, 32), BF16)], axis=1)
    W[own_w, MAIN:GW] = tails
    with scope("barrier"):
        pl.semaphore_wait(barrier, len(peers))
    run(gv[1:], "primary")
    run(gv[:1], "primary")
    for n in range(1, 8):
        t = lax.rem(tp + n, 8)
        src = wo_ref.at[:, pl.ds(pl.multiple_of(t * OWN, 128), OWN)]
        dst = WO.at[pl.ds(pl.multiple_of(tp * HW, 16), HW), :]
        send("w", "w", src, dst, at_tp(n))

    lane = lax.broadcasted_iota(jnp.int32, (8, TOK), 1)
    row8 = lax.broadcasted_iota(jnp.int32, (8, TOK), 0)
    for d in local[5:8]:
        d.wait()
    seg = seg_ref[...].reshape(1, TOK).astype(F32)
    fg = jnp.where(row8 == 0, fg_ref[0:1], fg_ref[1:2])
    e = jnp.exp(-jnp.abs(fg))
    log1p = jnp.where(e < 1e-2, e * (1.0 - e * (0.5 - e * (1.0 / 3.0))), jnp.log(1.0 + e))
    cum = jnp.minimum(fg, 0.0) - log1p
    shift = 1
    while shift < TOK:
        cum = cum + jnp.where(lane >= shift, pltpu.roll(cum, shift, 1), 0.0)
        shift *= 2
    b = [ig_ref[h : h + 1] - cum[h : h + 1] for h in range(2)]
    end = [cum[h : h + 1, TOK - 1 :] for h in range(2)]
    first, last, second_last = seg[:, :1], seg[:, TOK - 1 :], seg[:, TOK - 2 : TOK - 1]
    for d in local[8:12]:
        d.wait()
    ST[...] = jnp.zeros_like(ST)
    peak = []
    for h in range(2):
        hs = slice(h * DH, h * DH + DH)
        top = jnp.max(jnp.where(seg == last, b[h], ABSENT), axis=1, keepdims=True)
        peak.append(top)
        w = jnp.where(seg == last, jnp.exp(jnp.minimum(b[h] - top, 0.0)), 0.0) * DH**-0.5
        ST[hs, 0:DH] = dot_t(VT[hs, :], (KT[hs, :].astype(F32) * w).astype(BF16)).astype(BF16)
    meta_row = lax.broadcasted_iota(jnp.int32, (8, 128), 0)
    meta = jnp.zeros((8, 128), F32)
    for n, value in enumerate((end[0] + peak[0], end[1] + peak[1], end[0], end[1], first, last, second_last)):
        meta = jnp.where(meta_row == n, value, meta)
    MT[...] = meta
    for n in range(1, 5):
        send("st", "st", ST, SR.at[n - 1], at_sp(n))
        send("mt", "mt", MT, MR.at[n - 1], at_sp(n))
    run(gv, "second", 0)

    rows = jnp.where(row8 == 0, b[0], jnp.where(row8 == 1, b[1], seg))
    cols = jnp.transpose(jnp.concatenate([rows, jnp.zeros((120, TOK), F32)], axis=0))
    seg_c = cols[:, 2:3]
    tops = [[], []]
    for i in range(3):
        t0, ns = i * 256, (i + 1) * 256
        ts = slice(t0, t0 + 256)
        s_at = lax.broadcasted_iota(jnp.int32, (ns, 256), 0)
        t_at = lax.broadcasted_iota(jnp.int32, (ns, 256), 1) + t0
        mask = (seg_c[:ns] == seg[:, ts]) & (s_at <= t_at)
        for h in range(2):
            hs = slice(h * DH, h * DH + DH)
            masked = jnp.where(mask, cols[:ns, h : h + 1], ABSENT)
            top = jnp.max(masked, axis=0, keepdims=True)
            scores = dot_c(KT[hs, 0:ns], QT[hs, ts]) * (jnp.exp(masked - top) * DH**-0.5)
            OI[hs, ts] = dot(VT[hs, 0:ns], scores.astype(BF16))
            tops[h].append(top)

    with scope("relay"):
        run(gv, "relay")
        run(gv, "second", 1)
        run(gv, "second", 2)

    dec = [jnp.zeros((1, 128), F32)] * 2
    cand = [[], []]
    first_l = jnp.broadcast_to(first, (1, 128))
    with scope("state"):
        recv("st", SR)
        recv("mt", MR)
    for n in range(1, 5):
        m = MR[n - 1]
        valid = (m[5:6] == first_l) & (sp >= n)
        for h in range(2):
            cand[h].append(jnp.where(valid, m[h : h + 1] + dec[h], ABSENT))
            dec[h] = dec[h] + m[2 + h : 3 + h]
    for d in local[12:18]:
        d.wait()
    gain_at = lax.broadcasted_iota(jnp.int32, (HW, HW), 0) == lax.broadcasted_iota(jnp.int32, (HW, HW), 1)
    gain_c = jnp.sum(jnp.where(gain_at, hg_ref[...], 0.0), axis=1, keepdims=True)
    for h in range(2):
        hs = slice(h * DH, h * DH + DH)
        pin = jnp.maximum(
            jnp.maximum(cand[h][0], cand[h][1]), jnp.maximum(cand[h][2], cand[h][3])
        )
        state = jnp.zeros((DH, 128), F32)
        for n in range(4):
            state = state + jnp.exp(cand[h][n] - pin) * SR[n, hs, :].astype(F32)
        inter = dot(state[:, 0:DH].astype(BF16), QT[hs, :])
        m_in = jnp.concatenate(tops[h], axis=1)
        m_pin = jnp.where(seg == first, pin[:, :1], ABSENT)
        m_all = jnp.maximum(m_in, m_pin)
        memory = jnp.exp(m_in - m_all) * OI[hs, :] + jnp.exp(m_pin - m_all) * inter
        mean = jnp.sum(memory * memory, axis=0, keepdims=True) * (1.0 / DH)
        mix = memory * lax.rsqrt(mean + 1.0) * gain_c[hs] * jax.nn.sigmoid(OG[hs, :].astype(F32))
        MIX[pl.ds(pl.multiple_of(tp * HW + h * DH, 16), DH), :] = mix.astype(BF16)
    with scope("mix0"):
        mix_g[0]()
    with scope("across0"):
        run(gv, "across", 0)

    before = MR[0]
    there = sp >= 1
    last_before = jnp.where(there, before[5:6, :1], -1.0)
    second_before = jnp.where(there, before[6:7, :1], -1.0)
    seg8 = jnp.broadcast_to(seg, (8, TOK))
    one_back = jnp.where(lane == 0, last_before, pltpu.roll(seg8, 1, 1))
    two_back = jnp.where(
        lane == 0, second_before, jnp.where(lane == 1, last_before, pltpu.roll(seg8, 2, 1))
    )
    flags = jnp.where(
        row8 == 0, jnp.where(one_back == seg, 1.0, 0.0), jnp.where(two_back == seg, 1.0, 0.0)
    )
    NF[...] = jnp.transpose(jnp.concatenate([flags, jnp.zeros((120, TOK), F32)], axis=0))
    with scope("wo"):
        for d in local[18:]:
            d.wait()
        recv("w", WO.at[pl.ds(0, 7 * HW), :])
        WOT[...] = jnp.transpose(WO[...])

    with scope("mix1"):
        mix_g[1]()
    with scope("far"):
        run(gv, "far")
    with scope("mix2"):
        mix_g[2]()
    with scope("mix3"):
        mix_g[3]()

    gain = gain_ref[:, pl.ds(pl.multiple_of(tp * OWN, 128), OWN)]
    res = RB[...].astype(F32) + jnp.transpose(dot(WOT[...], MIX[...]))
    RES[...] = res
    X[:, pl.ds(pl.multiple_of(tp * OWN, 128), OWN)] = (res * gain).astype(BF16)
    x_g[0]()
    SS[tp] = dot_t(jnp.ones((8, OWN), F32), res * res, precision=lax.Precision.HIGHEST)
    for n in range(1, 8):
        send("q", "q", SS.at[tp], SS.at[tp], at_tp(n))
    with scope("across1"):
        run(gv, "across", 1)
    with scope("across2"):
        run(gv, "across", 2)
    with scope("x1"):
        x_g[1]()
    with scope("x2"):
        x_g[2]()
    with scope("x3"):
        x_g[3]()
    run(d0, "primary")
    run(d0, "second", 0)
    with scope("across3"):
        run(gv, "across", 3)
    with scope("sq"):
        recv("q", SS.at[pl.ds(0, 7)])
        total = SS[0]
        for n in range(1, 8):
            total = total + SS[n]
    scale_row = lax.rsqrt(total * (1.0 / 3072.0) + EPS)
    NF[:, 2:3] = jnp.transpose(jnp.concatenate([scale_row, jnp.zeros((120, TOK), F32)], axis=0))[:, 0:1]

    def tile256(n, at):
        return pl.ds(pl.multiple_of(n * 256 + at, 128), 256)

    def by_row(lanes, steps):
        acc = None
        for d in steps:
            k = pl.ds(pl.multiple_of(mod4(z + d) * 768, 128), 768)
            part = dot(X[:, k], W[k, lanes])
            acc = part if acc is None else acc + part
        return acc

    def by_pair(lanes, which):
        acc = None
        for zz in range(4):
            k = pl.ds(pl.multiple_of(zz * 768 + which * OWN, 128), OWN)
            part = dot(X[:, k], W[k, lanes])
            acc = part if acc is None else acc + part
        return acc

    here = x // 2
    with scope("partial"):

        def early(n, _):
            ACC[:, tile256(n, 0)] = by_row(tile256(n, 0), (0, 1, -1))
            ACC[:, tile256(n, GW)] = by_pair(tile256(n, GW), here)
            return 0

        lax.fori_loop(0, 4, early, 0)
        ACC[:, MAIN:GW] = by_row(slice(MAIN, GW), (0, 1, -1))

    with scope("d0relay"):
        run(d0, "relay")
        run(d0, "second", 1)
        run(d0, "second", 2)
        run(d1, "primary")
        run(d1, "second", 0)
    with scope("done"):
        run(gv, "done")
    with scope("p1"):
        run(d0, "across", 0)
        run(d0, "far")
    scale = NF[:, 2:3]
    with scope("gate"):

        def gate_tile(n, _):
            l = tile256(n, 0)
            GT[:, l] = ((ACC[:, l] + by_row(l, (2,))) * scale).astype(BF16)
            return 0

        lax.fori_loop(0, 4, gate_tile, 0)
        l = slice(MAIN, GW)
        GT[:, l] = ((ACC[:, l] + by_row(l, (2,))) * scale).astype(BF16)
    send("e", "e", GT.at[TOK - 16 : TOK, :], EDGE, at_sp(1))
    with scope("p2"):
        run(d0, "across", 1)
        run(d0, "across", 2)

    def hidden_of(lanes, width, taps, value):
        g = GT[:, lanes].astype(F32)
        edge = EDGE[:, lanes].astype(F32)
        t_at = lax.broadcasted_iota(jnp.int32, (TOK, width), 0)
        near = NF[:, 0:1] > 0.5
        far = NF[:, 1:2] > 0.5
        g1 = jnp.where(t_at == 0, edge[15:16], pltpu.roll(g, 1, 0))
        g2 = jnp.where(
            t_at == 0, edge[14:15], jnp.where(t_at == 1, edge[15:16], pltpu.roll(g, 2, 0))
        )
        conv = taps[2:3] * g + taps[1:2] * jnp.where(near, g1, 0.0) + taps[0:1] * jnp.where(far, g2, 0.0)
        return conv / (1.0 + jnp.exp(-conv)) * value

    def value_sum(n, _):
        l = tile256(n, GW)
        ACC[:, l] = ACC[:, l] + by_pair(l, 1 - here)
        return 0

    with scope("value"):
        lax.fori_loop(0, 2, value_sum, 0)
    with scope("p3"):
        run(d1, "relay")
    with scope("value"):
        lax.fori_loop(2, 4, value_sum, 0)
    with scope("p4"):
        run(d0, "across", 3)
        run(d1, "second", 1)
        run(d1, "second", 2)
        run(d2, "primary")
        run(d2, "second", 0)
        run(d1, "across", 0)
    with scope("edge"):
        recv("e", EDGE)

    with scope("hidden"):

        def hidden_tile(n, _):
            value = (ACC[:, tile256(n, GW)] * scale).astype(BF16).astype(F32)
            l = tile256(n, 0)
            HD[:, l] = hidden_of(l, 256, taps_ref[:, l], value).astype(BF16)
            return 0

        lax.fori_loop(0, 4, hidden_tile, 0)
        tail = slice(MAIN, GW)
        taps_tail = jnp.concatenate([taps_ref[:, MAIN : MAIN + 32], jnp.zeros((3, 96), F32)], axis=1)
        value_tail = pltpu.roll(GT[:, tail].astype(F32), 96, 1)
        HD[:, tail] = pltpu.roll(hidden_of(tail, 128, taps_tail, value_tail), 64, 1).astype(BF16)
    with scope("p5"):
        run(d1, "far")
        run(d0, "done")

    downs = (WD0, WD1, WD2)

    def partials(p, cc, which):
        mains, ends = [], []
        for n in which:
            j = mod4(y + order[n]) * 2 + cc
            mains.append(downs[p][pl.ds(pl.multiple_of(j * 128, 128), 128), :])
            for k in range(2):
                at = pl.multiple_of((j * 2 + k) * HW + p * PART, 16)
                ends.append(W[pl.ds(at, PART), MAIN:GW])
        return dot_t(HD[:, 0:MAIN], jnp.concatenate(mains, axis=0)) + dot_t(
            HD[:, MAIN:GW], jnp.concatenate(ends, axis=0)
        )

    order = (2, 1, -1, 0)

    def at_po(p, m):
        return pl.ds(m * OWN + p * 128, 128)

    def give(p, which):
        l = pl.ds(p * 128, 128)
        both = partials(p, o, which).astype(BF16)
        for k, n in enumerate(which):
            SP[n, :, l] = both[:, k * 128 : (k + 1) * 128]
            send(("sp", p, which), "sp", SP.at[n, :, l], RP.at[n, :, l], partner)

    def keep(p, which):
        l = pl.ds(p * 128, 128)
        mine = partials(p, c, which)
        with scope("sp"):
            recv(("sp", p, which), RP.at[pl.ds(which[0], len(which)), :, l])
        for k, n in enumerate(which):
            d = order[n]
            both = mine[:, k * 128 : (k + 1) * 128] + RP[n, :, l].astype(F32)
            if d == 2:
                ZS[0, :, l] = both.astype(BF16)
                send(("rl", p), "rl", ZS.at[0, pl.ds(0, OWN), l], RL.at[0, :, l], at_y(1))
                send(("rl", p), "rl", ZS.at[0, pl.ds(OWN, OWN), l], RL.at[1, :, l], at_y(-1))
            else:
                ACC[:, at_po(p, n)] = both
                if d != 0:
                    r = pl.ds(OWN if d == 1 else 0, OWN)
                    ZS[n, r, l] = both[OWN:, :].astype(BF16) if d == 1 else both[:OWN, :].astype(BF16)
                    send(("rv", p), "rv", ZS.at[n, r, l], RV.at[n - 1, r, l], at_y(d))

    def pass_on(p):
        l = pl.ds(p * 128, 128)
        with scope("rl"):
            recv(("rl", p), RL.at[:, :, l])
        for n, d in ((1, 1), (2, -1)):
            r = pl.ds(0 if d == 1 else OWN, OWN)
            ZS[n, r, l] = (ACC[r, at_po(p, n)] + RL[n - 1, :, l].astype(F32)).astype(BF16)
            send(("rv", p), "rv", ZS.at[n, r, l], RV.at[n - 1, r, l], at_y(d))

    def collect(p):
        l = pl.ds(p * 128, 128)
        with scope("rv%d" % p):
            recv(("rv", p), RV.at[:, :, l])
        return ACC[:, at_po(p, 3)] + RV[0, :, l].astype(F32) + RV[1, :, l].astype(F32)

    with scope("give0"):
        give(0, EVERY)
    with scope("p6"):
        run(d1, "across", 1)
        run(d2, "relay")
        run(d2, "second", 1)
    with scope("keep0"):
        keep(0, EVERY)
    with scope("p7"):
        run(d1, "across", 2)
        run(d1, "across", 3)
        run(d2, "second", 2)
        run(d2, "across", 0)
        run(d2, "far")
    with scope("p8"):
        run(d2, "across", 1)
        run(d1, "done")
    with scope("give1"):
        give(1, EVERY)
    with scope("p8b"):
        run(d2, "across", 2)
        run(d2, "across", 3)
    with scope("pass0"):
        pass_on(0)
    with scope("keep1"):
        keep(1, EVERY)
    with scope("p10"):
        run(d2, "done")
    with scope("give2"):
        give(2, FAR)
        give(2, REST)
    with scope("keep2"):
        keep(2, FAR)
    with scope("pass1"):
        pass_on(1)
    with scope("keep2r"):
        keep(2, REST)
    with scope("pass2"):
        pass_on(2)
    with scope("final0"):
        low = lax.broadcasted_iota(jnp.int32, (TOK, 128), 1) < 64
        part0 = collect(0)
        turned = pltpu.roll(collect(1), 64, 1)
        out_ref[:, 0:128] = (RES[:, 0:128] + jnp.where(low, part0, turned)).astype(BF16)
        RES[:, 128:256] = RES[:, 128:256] + jnp.where(low, ACC[:, at_po(2, 3)], part0)
        RES[:, 256:384] = RES[:, 256:384] + jnp.where(low, turned, ACC[:, at_po(2, 3)])
    with scope("final"):
        l = pl.ds(256, 128)
        with scope("rv2"):
            recv(("rv", 2), RV.at[:, :, l])
        part2 = RV[0, :, l].astype(F32) + RV[1, :, l].astype(F32)
        out_ref[:, 128:256] = (RES[:, 128:256] + jnp.where(low, part2, 0.0)).astype(BF16)
        out_ref[:, 256:384] = (RES[:, 256:384] + jnp.where(low, 0.0, part2)).astype(BF16)
    with scope("sent"):
        for part in (gv, d0, d1, d2):
            run(part, "out")
        mix_g[4]()
        x_g[4]()
        sent("w", WO.at[pl.ds(0, 7 * HW), :])
        sent("st", SR)
        sent("mt", MR)
        sent("q", SS.at[pl.ds(0, 7)])
        sent("e", EDGE)
        sent("sp", SP)
        sent("rl", RL)
        sent("rv", RV)
    if len(table) != SEMS:
        raise ValueError(len(table))


def body(
    resid,
    query,
    keys,
    values,
    out_gate,
    in_gate,
    forget,
    doc_ids,
    head_gain,
    w_out,
    ffn_gain,
    w_gate,
    w_value,
    conv_taps,
    w_down,
):
    vmem = pl.BlockSpec(memory_space=pltpu.VMEM)
    hbm = pl.BlockSpec(memory_space=pl.ANY)
    return pl.pallas_call(
        kernel,
        out_shape=pltpu.VMEM((TOK, OWN), BF16),
        in_specs=[hbm] * 15,
        out_specs=vmem,
        scratch_shapes=[
            pltpu.VMEM((3072, LANES), BF16),
            pltpu.VMEM((2, TOK), F32),
            pltpu.VMEM((2, TOK), F32),
            pltpu.VMEM((TOK,), jnp.int32),
            pltpu.VMEM((1, HW), F32),
            pltpu.VMEM((1, 3072), F32),
            pltpu.VMEM((3, 1056), F32),
            pltpu.VMEM((16 * PART, MAIN), BF16),
            pltpu.VMEM((16 * PART, MAIN), BF16),
            pltpu.VMEM((16 * PART, MAIN), BF16),
            pltpu.VMEM((3, HW, 32), BF16),
            pltpu.VMEM((TOK, 3072), BF16),
            pltpu.VMEM((1536, TOK), BF16),
            pltpu.VMEM((1536, OWN), BF16),
            pltpu.VMEM((OWN, 1536), BF16),
            pltpu.VMEM((HW, TOK), BF16),
            pltpu.VMEM((HW, TOK), BF16),
            pltpu.VMEM((HW, TOK), BF16),
            pltpu.VMEM((HW, TOK), BF16),
            pltpu.VMEM((TOK, OWN), BF16),
            pltpu.VMEM((HW, TOK), F32),
            pltpu.VMEM((TOK, 128), F32),
            pltpu.VMEM((HW, 128), BF16),
            pltpu.VMEM((4, HW, 128), BF16),
            pltpu.VMEM((8, 128), F32),
            pltpu.VMEM((4, 8, 128), F32),
            pltpu.VMEM((8, 8, TOK), F32),
            pltpu.VMEM((TOK, OWN), F32),
            pltpu.VMEM((TOK, LANES), F32),
            pltpu.VMEM((TOK, GW), BF16),
            pltpu.VMEM((16, GW), BF16),
            pltpu.VMEM((TOK, GW), BF16),
            pltpu.VMEM((4, TOK, OWN), BF16),
            pltpu.VMEM((4, TOK, OWN), BF16),
            pltpu.VMEM((3, TOK, OWN), BF16),
            pltpu.VMEM((2, OWN, OWN), BF16),
            pltpu.VMEM((2, TOK, OWN), BF16),
            pltpu.SemaphoreType.DMA((SEMS,)),
            pltpu.SemaphoreType.DMA((20,)),
        ],
        compiler_params=pltpu.CompilerParams(
            collective_id=0, has_side_effects=True, vmem_limit_bytes=VLIM * 1024 * 1024
        ),
    )(
        w_gate,
        w_value,
        w_down.T,
        query.T,
        keys.T,
        values.T,
        out_gate.T,
        w_out,
        resid,
        in_gate,
        forget,
        doc_ids,
        head_gain[None],
        ffn_gain[None],
        conv_taps,
    )


def solution(mesh):
    torus = Mesh(mesh.devices.reshape(4, 4, 4, 2), ("z", "x", "y", "c"))
    sp, tp = ("z", "x"), ("y", "c")
    placed = (
        P(sp, tp),
        P(sp, tp),
        P(sp, tp),
        P(sp, tp),
        P(sp, tp),
        P(tp, sp),
        P(tp, sp),
        P(sp),
        P(tp),
        P(tp, None),
        P(),
        P(sp, tp),
        P(sp, tp),
        P(None, tp),
        P(tp, sp),
    )
    return jax.shard_map(body, mesh=torus, in_specs=placed, out_specs=P(sp, tp), check_vma=False)
```

```python
import jax
import jax.numpy as jnp
from jax import lax
from jax.experimental import pallas as pl
from jax.experimental.pallas import tpu as pltpu
from jax.sharding import Mesh
from jax.sharding import PartitionSpec as P

MESH = pl.DeviceIdType.MESH
F32 = jnp.float32
BF16 = jnp.bfloat16
ABSENT = -1e30
DH = 96
TOK = 768
OWN = 384
HW = 192
MAIN = 1024
GW = 1152
LANES = 2176
PART = 64
EPS = 1e-6
EVERY, FAR, REST = (0, 1, 2, 3), (0,), (1, 2, 3)
VLIM = 60
SEMS = 61
scope = jax.named_scope


def mod4(v):
    return lax.rem(v + 8, 4)


def dot(a, b, **kw):
    return lax.dot_general(a, b, (((1,), (0,)), ((), ())), preferred_element_type=F32, **kw)


def dot_t(a, b, **kw):
    return lax.dot_general(a, b, (((1,), (1,)), ((), ())), preferred_element_type=F32, **kw)


def dot_c(a, b, **kw):
    return lax.dot_general(a, b, (((0,), (0,)), ((), ())), preferred_element_type=F32, **kw)


def kernel(
    wg_ref,
    wv_ref,
    wd_ref,
    q_hbm,
    k_hbm,
    v_hbm,
    og_hbm,
    wo_ref,
    resid_hbm,
    ig_hbm,
    fg_hbm,
    seg_hbm,
    hg_hbm,
    gain_hbm,
    taps_hbm,
    out_ref,
    W,
    ig_ref,
    fg_ref,
    seg_ref,
    hg_ref,
    gain_ref,
    taps_ref,
    WD0,
    WD1,
    WD2,
    TL,
    X,
    MIX,
    WO,
    WOT,
    QT,
    KT,
    VT,
    OG,
    RB,
    OI,
    NF,
    ST,
    SR,
    MT,
    MR,
    SS,
    RES,
    ACC,
    GT,
    EDGE,
    HD,
    SP,
    RP,
    ZS,
    RL,
    RV,
    sems,
    lsem,
):
    z, x = lax.axis_index("z"), lax.axis_index("x")
    y, c = lax.axis_index("y"), lax.axis_index("c")
    sp = z * 4 + x
    tp = y * 2 + c
    o = 1 - c
    table = {}
    rkey_any = "w"

    def slot(key):
        return table.setdefault(key, len(table))

    def copy(rkey, skey, src, dst, dev):
        return pltpu.make_async_remote_copy(
            src_ref=src,
            dst_ref=dst,
            send_sem=sems.at[slot(("S", skey))],
            recv_sem=sems.at[slot(("R", rkey))],
            device_id=dev,
            device_id_type=MESH,
        )

    def send(rkey, skey, src, dst, dev):
        copy(rkey, skey, src, dst, dev).start()

    partner = (z, x, y, o)

    def recv(rkey, span):
        copy(rkey, rkey_any, span, span, partner).wait_recv()

    def sent(skey, span):
        copy(rkey_any, skey, span, span, partner).wait_send()

    def at_sp(n):
        s = lax.rem(sp + n + 16, 16)
        return (s // 4, lax.rem(s, 4), y, c)

    def at_x(d):
        return (z, mod4(x + d), y, c)

    def at_z(d):
        return (mod4(z + d), x, y, c)

    def at_y(d):
        return (z, x, mod4(y + d), c)

    def at_tp(n):
        t = lax.rem(tp + n, 8)
        return (z, x, t // 2, lax.rem(t, 2))

    peers = [at_x(1), at_x(-1), at_z(1), at_z(-1)]
    peers += [at_tp(n) for n in range(1, 8)]
    peers += [at_sp(n) for n in (1, 2, 3, -1, -2, -3)]
    barrier = pltpu.get_barrier_semaphore()
    for dev in peers:
        pl.semaphore_signal(barrier, inc=1, device_id=dev, device_id_type=MESH)

    groups = ["main", "tail", "fg", "ig", "seg", "heads", "down", "hg", "gain", "taps", "resid", "wo"]

    def bring(group, src, dst):
        pltpu.make_async_copy(src, dst, lsem.at[groups.index(group)]).start()

    def landed(group, span):
        pltpu.make_async_copy(span, span, lsem.at[groups.index(group)]).wait()

    own_w = pl.ds(pl.multiple_of(sp * HW, 16), HW)
    bring("main", wg_ref.at[:, 0:MAIN], W.at[own_w, 0:MAIN])
    bring("main", wv_ref.at[:, 0:MAIN], W.at[own_w, GW:LANES])
    for n, ref in enumerate((wg_ref, wv_ref, wd_ref)):
        bring("tail", ref.at[:, MAIN : MAIN + 32], TL.at[n])
    bring("fg", fg_hbm, fg_ref)
    bring("ig", ig_hbm, ig_ref)
    bring("seg", seg_hbm, seg_ref)
    bring("heads", k_hbm, KT)
    bring("heads", v_hbm, VT)
    bring("heads", q_hbm, QT)
    bring("heads", og_hbm, OG)
    for n, ref in enumerate((WD0, WD1, WD2)):
        bring(
            "down",
            wd_ref.at[n * PART : (n + 1) * PART, 0:MAIN],
            ref.at[pl.ds(pl.multiple_of(sp * PART, 16), PART), :],
        )
    bring("hg", hg_hbm, hg_ref)
    bring("gain", gain_hbm, gain_ref)
    bring("taps", taps_hbm, taps_ref)
    bring("resid", resid_hbm, RB)
    bring(
        "wo",
        wo_ref.at[:, pl.ds(pl.multiple_of(tp * OWN, 128), OWN)],
        WO.at[pl.ds(pl.multiple_of(tp * HW, 16), HW), :],
    )

    def stage(gather, ref, stride, rows, lanes, by_lanes, first):
        x_first = first == "x"
        prim = at_x if x_first else at_z
        secd = at_z if x_first else at_x
        steps = (0, -1, 1, 2)
        group = "gv" if ref is W else "dn"

        def place(dp, ds, half=None, shift=0):
            zz, xx = (mod4(z + ds), mod4(x + dp)) if x_first else (mod4(z + dp), mod4(x + ds))
            (r0, nr), (l0, nl) = rows, lanes
            if half is not None and by_lanes:
                l0, nl = l0 + half * nl // 2, nl // 2
            elif half is not None:
                upper = nr // 2 - shift
                r0, nr = (r0 + upper, nr - upper) if half else (r0, upper)
            row = pl.multiple_of((zz * 4 + xx) * stride + r0, 16)
            return ref.at[pl.ds(row, nr), pl.ds(l0, nl)]

        def primary():
            for d in (1, -1):
                send((gather, "p"), group, place(0, 0), place(0, 0), prim(d))

        def second(m):
            p = place(steps[m], 0)
            for d in (1, -1):
                send((gather, "s", m), group, p, p, secd(d))

        def relay():
            for d in (1, -1):
                p = place(-d, 0, 0 if d == 1 else 1)
                send((gather, "pf"), group, p, p, prim(d))

        def across(m):
            for d in (1, -1):
                p = place(steps[m], -d, 0 if d == 1 else 1, 16 if m in (1, 2) else 0)
                send((gather, "sf"), group, p, p, secd(d))

        def far():
            second(3)

        return primary, second, relay, across, far

    awaited = {"relay": ("p", 2), "across": ("s", 2), "far": ("pf", 1), "done": ("sf", 4)}

    def run(gather, what, *args, only=(0, 1)):
        name, ref, rows, parts = gather
        if what in awaited:
            tag, count = awaited[what]
            recv((name, tag, *args), ref.at[pl.ds(0, count * rows), :])
        if what != "done":
            k = ("primary", "second", "relay", "across", "far").index(what)
            for n in only:
                parts[n][k](*args)

    gv = (
        "gv",
        W,
        HW,
        (
            stage("gv", W, HW, (0, HW), (0, GW), False, "x"),
            stage("gv", W, HW, (0, HW), (GW, MAIN), False, "z"),
        ),
    )

    def down_stage(n, ref, cut):
        parts = (
            stage(n, ref, PART, (0, cut), (0, MAIN), True, "x"),
            stage(n, ref, PART, (cut, PART - cut), (0, MAIN), True, "z"),
        )
        return n, ref, PART, parts

    d0, d1, d2 = down_stage(0, WD0, 16), down_stage(1, WD1, 32), down_stage(2, WD2, 32)

    def over_tp(name, blk, span):
        def g0():
            b = blk(y, c)
            for d in (1, -1):
                send((name, "y"), name, b, b, at_y(d))
            send((name, "o"), name, b, b, partner)

        def g1():
            recv((name, "y"), span(2))
            for d in (1, -1):
                h = blk(mod4(y - d), c, 0 if d == 1 else 1)
                send((name, "f"), name, h, h, at_y(d))
            for d in (1, -1):
                b = blk(mod4(y - d), c)
                send((name, "o"), name, b, b, partner)

        def g2():
            recv((name, "f"), span(1))
            b = blk(mod4(y + 2), c)
            send((name, "o"), name, b, b, partner)

        def g3():
            recv((name, "o"), span(4))

        def out():
            sent(name, span(7))

        return g0, g1, g2, g3, out

    def mix_block(yy, cc, half=None):
        r0, nr = (0, HW) if half is None else (half * DH, DH)
        return MIX.at[pl.ds(pl.multiple_of((yy * 2 + cc) * HW + r0, 16), nr), :]

    def x_block(yy, cc, half=None):
        rows = slice(None) if half is None else pl.ds(half * OWN, OWN)
        return X.at[rows, pl.ds(pl.multiple_of((yy * 2 + cc) * OWN, 128), OWN)]

    mix_g = over_tp("m", mix_block, lambda k: MIX.at[pl.ds(0, k * HW), :])
    x_g = over_tp("x", x_block, lambda k: X.at[:, pl.ds(0, k * OWN)])

    landed("main", W.at[0 : 2 * HW, 0:MAIN])
    landed("tail", TL)
    tails = jnp.concatenate([TL[0], TL[1], TL[2], jnp.zeros((HW, 32), BF16)], axis=1)
    W[own_w, MAIN:GW] = tails
    with scope("barrier"):
        pl.semaphore_wait(barrier, len(peers))
    run(gv, "primary", only=(1, 0))
    for n in range(1, 8):
        t = lax.rem(tp + n, 8)
        src = wo_ref.at[:, pl.ds(pl.multiple_of(t * OWN, 128), OWN)]
        dst = WO.at[pl.ds(pl.multiple_of(tp * HW, 16), HW), :]
        send("w", "w", src, dst, at_tp(n))

    lane = lax.broadcasted_iota(jnp.int32, (8, TOK), 1)
    row8 = lax.broadcasted_iota(jnp.int32, (8, TOK), 0)
    landed("fg", fg_ref)
    landed("ig", ig_ref)
    landed("seg", seg_ref)
    seg = seg_ref[...].reshape(1, TOK).astype(F32)
    fg = jnp.where(row8 == 0, fg_ref[0:1], fg_ref[1:2])
    e = jnp.exp(-jnp.abs(fg))
    log1p = jnp.where(e < 1e-2, e * (1.0 - e * (0.5 - e * (1.0 / 3.0))), jnp.log(1.0 + e))
    cum = jnp.minimum(fg, 0.0) - log1p
    shift = 1
    while shift < TOK:
        cum = cum + jnp.where(lane >= shift, pltpu.roll(cum, shift, 1), 0.0)
        shift *= 2
    b = [ig_ref[h : h + 1] - cum[h : h + 1] for h in range(2)]
    end = [cum[h : h + 1, TOK - 1 :] for h in range(2)]
    first, last, second_last = seg[:, :1], seg[:, TOK - 1 :], seg[:, TOK - 2 : TOK - 1]
    landed("heads", MIX.at[0 : 4 * HW, :])
    ST[...] = jnp.zeros_like(ST)
    peak = []
    for h in range(2):
        hs = slice(h * DH, h * DH + DH)
        top = jnp.max(jnp.where(seg == last, b[h], ABSENT), axis=1, keepdims=True)
        peak.append(top)
        w = jnp.where(seg == last, jnp.exp(jnp.minimum(b[h] - top, 0.0)), 0.0) * DH**-0.5
        ST[hs, 0:DH] = dot_t(VT[hs, :], (KT[hs, :].astype(F32) * w).astype(BF16)).astype(BF16)
    meta_row = lax.broadcasted_iota(jnp.int32, (8, 128), 0)
    meta = jnp.zeros((8, 128), F32)
    for n, value in enumerate((end[0] + peak[0], end[1] + peak[1], end[0], end[1], first, last, second_last)):
        meta = jnp.where(meta_row == n, value, meta)
    MT[...] = meta
    for n in range(1, 5):
        send("st", "st", ST, SR.at[n - 1], at_sp(n))
        send("mt", "mt", MT, MR.at[n - 1], at_sp(n))
    run(gv, "second", 0)

    rows = jnp.where(row8 == 0, b[0], jnp.where(row8 == 1, b[1], seg))
    cols = jnp.transpose(jnp.concatenate([rows, jnp.zeros((120, TOK), F32)], axis=0))
    seg_c = cols[:, 2:3]
    tops = [[], []]
    for i in range(3):
        t0, ns = i * 256, (i + 1) * 256
        ts = slice(t0, t0 + 256)
        s_at = lax.broadcasted_iota(jnp.int32, (ns, 256), 0)
        t_at = lax.broadcasted_iota(jnp.int32, (ns, 256), 1) + t0
        mask = (seg_c[:ns] == seg[:, ts]) & (s_at <= t_at)
        for h in range(2):
            hs = slice(h * DH, h * DH + DH)
            masked = jnp.where(mask, cols[:ns, h : h + 1], ABSENT)
            top = jnp.max(masked, axis=0, keepdims=True)
            scores = dot_c(KT[hs, 0:ns], QT[hs, ts]) * (jnp.exp(masked - top) * DH**-0.5)
            OI[hs, ts] = dot(VT[hs, 0:ns], scores.astype(BF16))
            tops[h].append(top)

    with scope("relay"):
        run(gv, "relay")
        run(gv, "second", 1)
        run(gv, "second", 2)

    dec = [jnp.zeros((1, 128), F32)] * 2
    cand = [[], []]
    first_l = jnp.broadcast_to(first, (1, 128))
    with scope("state"):
        recv("st", SR)
        recv("mt", MR)
    for n in range(1, 5):
        m = MR[n - 1]
        valid = (m[5:6] == first_l) & (sp >= n)
        for h in range(2):
            cand[h].append(jnp.where(valid, m[h : h + 1] + dec[h], ABSENT))
            dec[h] = dec[h] + m[2 + h : 3 + h]
    landed("down", WD0.at[0:HW, :])
    landed("hg", hg_ref)
    landed("gain", gain_ref)
    landed("taps", taps_ref)
    gain_at = lax.broadcasted_iota(jnp.int32, (HW, HW), 0) == lax.broadcasted_iota(jnp.int32, (HW, HW), 1)
    gain_c = jnp.sum(jnp.where(gain_at, hg_ref[...], 0.0), axis=1, keepdims=True)
    for h in range(2):
        hs = slice(h * DH, h * DH + DH)
        pin = jnp.maximum(
            jnp.maximum(cand[h][0], cand[h][1]), jnp.maximum(cand[h][2], cand[h][3])
        )
        state = jnp.zeros((DH, 128), F32)
        for n in range(4):
            state = state + jnp.exp(cand[h][n] - pin) * SR[n, hs, :].astype(F32)
        inter = dot(state[:, 0:DH].astype(BF16), QT[hs, :])
        m_in = jnp.concatenate(tops[h], axis=1)
        m_pin = jnp.where(seg == first, pin[:, :1], ABSENT)
        m_all = jnp.maximum(m_in, m_pin)
        memory = jnp.exp(m_in - m_all) * OI[hs, :] + jnp.exp(m_pin - m_all) * inter
        mean = jnp.sum(memory * memory, axis=0, keepdims=True) * (1.0 / DH)
        mix = memory * lax.rsqrt(mean + 1.0) * gain_c[hs] * jax.nn.sigmoid(OG[hs, :].astype(F32))
        MIX[pl.ds(pl.multiple_of(tp * HW + h * DH, 16), DH), :] = mix.astype(BF16)
    with scope("mix0"):
        mix_g[0]()
    with scope("across0"):
        run(gv, "across", 0)

    before = MR[0]
    there = sp >= 1
    last_before = jnp.where(there, before[5:6, :1], -1.0)
    second_before = jnp.where(there, before[6:7, :1], -1.0)
    seg8 = jnp.broadcast_to(seg, (8, TOK))
    one_back = jnp.where(lane == 0, last_before, pltpu.roll(seg8, 1, 1))
    two_back = jnp.where(
        lane == 0, second_before, jnp.where(lane == 1, last_before, pltpu.roll(seg8, 2, 1))
    )
    flags = jnp.where(
        row8 == 0, jnp.where(one_back == seg, 1.0, 0.0), jnp.where(two_back == seg, 1.0, 0.0)
    )
    NF[...] = jnp.transpose(jnp.concatenate([flags, jnp.zeros((120, TOK), F32)], axis=0))
    with scope("wo"):
        landed("resid", RB)
        landed("wo", WO.at[0:HW, :])
        recv("w", WO.at[pl.ds(0, 7 * HW), :])
        WOT[...] = jnp.transpose(WO[...])

    with scope("mix1"):
        mix_g[1]()
    with scope("far"):
        run(gv, "far")
    with scope("mix2"):
        mix_g[2]()
    with scope("mix3"):
        mix_g[3]()

    gain = gain_ref[:, pl.ds(pl.multiple_of(tp * OWN, 128), OWN)]
    res = RB[...].astype(F32) + jnp.transpose(dot(WOT[...], MIX[...]))
    RES[...] = res
    X[:, pl.ds(pl.multiple_of(tp * OWN, 128), OWN)] = (res * gain).astype(BF16)
    x_g[0]()
    SS[tp] = dot_t(jnp.ones((8, OWN), F32), res * res, precision=lax.Precision.HIGHEST)
    for n in range(1, 8):
        send("q", "q", SS.at[tp], SS.at[tp], at_tp(n))
    with scope("across1"):
        run(gv, "across", 1)
    with scope("across2"):
        run(gv, "across", 2)
    with scope("x1"):
        x_g[1]()
    with scope("x2"):
        x_g[2]()
    with scope("x3"):
        x_g[3]()
    run(d0, "primary")
    run(d0, "second", 0)
    with scope("across3"):
        run(gv, "across", 3)
    with scope("sq"):
        recv("q", SS.at[pl.ds(0, 7)])
        total = SS[0]
        for n in range(1, 8):
            total = total + SS[n]
    scale_row = lax.rsqrt(total * (1.0 / 3072.0) + EPS)
    NF[:, 2:3] = jnp.transpose(jnp.concatenate([scale_row, jnp.zeros((120, TOK), F32)], axis=0))[:, 0:1]

    def tile256(n, at):
        return pl.ds(pl.multiple_of(n * 256 + at, 128), 256)

    def by_row(lanes, steps):
        acc = None
        for d in steps:
            k = pl.ds(pl.multiple_of(mod4(z + d) * 768, 128), 768)
            part = dot(X[:, k], W[k, lanes])
            acc = part if acc is None else acc + part
        return acc

    def by_pair(lanes, which):
        acc = None
        for zz in range(4):
            k = pl.ds(pl.multiple_of(zz * 768 + which * OWN, 128), OWN)
            part = dot(X[:, k], W[k, lanes])
            acc = part if acc is None else acc + part
        return acc

    here = x // 2
    with scope("partial"):

        def early(n, _):
            ACC[:, tile256(n, 0)] = by_row(tile256(n, 0), (0, 1, -1))
            ACC[:, tile256(n, GW)] = by_pair(tile256(n, GW), here)
            return 0

        lax.fori_loop(0, 4, early, 0)
        ACC[:, MAIN:GW] = by_row(slice(MAIN, GW), (0, 1, -1))

    with scope("d0relay"):
        run(d0, "relay")
        run(d0, "second", 1)
        run(d0, "second", 2)
        run(d1, "primary")
        run(d1, "second", 0)
    with scope("done"):
        run(gv, "done")
    with scope("p1"):
        run(d0, "across", 0)
        run(d0, "far")
    scale = NF[:, 2:3]
    with scope("gate"):

        def gate_tile(n, _):
            l = tile256(n, 0)
            GT[:, l] = ((ACC[:, l] + by_row(l, (2,))) * scale).astype(BF16)
            return 0

        lax.fori_loop(0, 4, gate_tile, 0)
        l = slice(MAIN, GW)
        GT[:, l] = ((ACC[:, l] + by_row(l, (2,))) * scale).astype(BF16)
    send("e", "e", GT.at[TOK - 16 : TOK, :], EDGE, at_sp(1))
    with scope("p2"):
        run(d0, "across", 1)
        run(d0, "across", 2)

    def hidden_of(lanes, width, taps, value):
        g = GT[:, lanes].astype(F32)
        edge = EDGE[:, lanes].astype(F32)
        t_at = lax.broadcasted_iota(jnp.int32, (TOK, width), 0)
        near = NF[:, 0:1] > 0.5
        far = NF[:, 1:2] > 0.5
        g1 = jnp.where(t_at == 0, edge[15:16], pltpu.roll(g, 1, 0))
        g2 = jnp.where(
            t_at == 0, edge[14:15], jnp.where(t_at == 1, edge[15:16], pltpu.roll(g, 2, 0))
        )
        conv = taps[2:3] * g + taps[1:2] * jnp.where(near, g1, 0.0) + taps[0:1] * jnp.where(far, g2, 0.0)
        return conv / (1.0 + jnp.exp(-conv)) * value

    def value_sum(n, _):
        l = tile256(n, GW)
        ACC[:, l] = ACC[:, l] + by_pair(l, 1 - here)
        return 0

    with scope("value"):
        lax.fori_loop(0, 2, value_sum, 0)
    with scope("p3"):
        run(d1, "relay")
    with scope("value"):
        lax.fori_loop(2, 4, value_sum, 0)
    with scope("p4"):
        run(d0, "across", 3)
        run(d2, "primary")
        run(d2, "second", 0)
        run(d1, "second", 1)
        run(d1, "second", 2)
        run(d1, "across", 0)
    with scope("edge"):
        recv("e", EDGE)

    with scope("hidden"):

        def hidden_tile(n, _):
            value = (ACC[:, tile256(n, GW)] * scale).astype(BF16).astype(F32)
            l = tile256(n, 0)
            HD[:, l] = hidden_of(l, 256, taps_ref[:, l], value).astype(BF16)
            return 0

        lax.fori_loop(0, 4, hidden_tile, 0)
        tail = slice(MAIN, GW)
        taps_tail = jnp.concatenate([taps_ref[:, MAIN : MAIN + 32], jnp.zeros((3, 96), F32)], axis=1)
        value_tail = pltpu.roll(GT[:, tail].astype(F32), 96, 1)
        HD[:, tail] = pltpu.roll(hidden_of(tail, 128, taps_tail, value_tail), 64, 1).astype(BF16)
    with scope("p5"):
        run(d1, "far")
        run(d0, "done")

    downs = (WD0, WD1, WD2)

    def partials(p, cc, which):
        mains, ends = [], []
        for n in which:
            j = mod4(y + order[n]) * 2 + cc
            mains.append(downs[p][pl.ds(pl.multiple_of(j * 128, 128), 128), :])
            for k in range(2):
                at = pl.multiple_of((j * 2 + k) * HW + p * PART, 16)
                ends.append(W[pl.ds(at, PART), MAIN:GW])
        return dot_t(HD[:, 0:MAIN], jnp.concatenate(mains, axis=0)) + dot_t(
            HD[:, MAIN:GW], jnp.concatenate(ends, axis=0)
        )

    order = (2, 1, -1, 0)

    def at_po(p, m):
        return pl.ds(m * OWN + p * 128, 128)

    def give(p, which):
        l = pl.ds(p * 128, 128)
        both = partials(p, o, which).astype(BF16)
        for k, n in enumerate(which):
            SP[n, :, l] = both[:, k * 128 : (k + 1) * 128]
            send(("sp", p, which), "sp", SP.at[n, :, l], RP.at[n, :, l], partner)

    def keep(p, which):
        l = pl.ds(p * 128, 128)
        mine = partials(p, c, which)
        with scope("sp"):
            recv(("sp", p, which), RP.at[pl.ds(which[0], len(which)), :, l])
        for k, n in enumerate(which):
            d = order[n]
            both = mine[:, k * 128 : (k + 1) * 128] + RP[n, :, l].astype(F32)
            if d == 2:
                ZS[0, :, l] = both.astype(BF16)
                send(("rl", p), "rl", ZS.at[0, pl.ds(0, OWN), l], RL.at[0, :, l], at_y(1))
                send(("rl", p), "rl", ZS.at[0, pl.ds(OWN, OWN), l], RL.at[1, :, l], at_y(-1))
            else:
                ACC[:, at_po(p, n)] = both
                if d != 0:
                    r = pl.ds(OWN if d == 1 else 0, OWN)
                    ZS[n, r, l] = both[OWN:, :].astype(BF16) if d == 1 else both[:OWN, :].astype(BF16)
                    send(("rv", p), "rv", ZS.at[n, r, l], RV.at[n - 1, r, l], at_y(d))

    def pass_on(p):
        l = pl.ds(p * 128, 128)
        with scope("rl"):
            recv(("rl", p), RL.at[:, :, l])
        for n, d in ((1, 1), (2, -1)):
            r = pl.ds(0 if d == 1 else OWN, OWN)
            ZS[n, r, l] = (ACC[r, at_po(p, n)] + RL[n - 1, :, l].astype(F32)).astype(BF16)
            send(("rv", p), "rv", ZS.at[n, r, l], RV.at[n - 1, r, l], at_y(d))

    def collect(p):
        l = pl.ds(p * 128, 128)
        with scope("rv%d" % p):
            recv(("rv", p), RV.at[:, :, l])
        return ACC[:, at_po(p, 3)] + RV[0, :, l].astype(F32) + RV[1, :, l].astype(F32)

    with scope("give0"):
        give(0, EVERY)
    with scope("p6"):
        run(d2, "relay")
        run(d2, "second", 1)
        run(d1, "across", 1)
    with scope("keep0"):
        keep(0, EVERY)
    with scope("p7"):
        run(d1, "across", 2)
        run(d1, "across", 3)
        run(d2, "second", 2)
        run(d2, "far")
        run(d2, "across", 0)
    with scope("p8"):
        run(d2, "across", 1)
        run(d1, "done")
    with scope("give1"):
        give(1, EVERY)
    with scope("p8b"):
        run(d2, "across", 2)
        run(d2, "across", 3)
    with scope("pass0"):
        pass_on(0)
    with scope("keep1"):
        keep(1, EVERY)
    with scope("p10"):
        run(d2, "done")
    with scope("give2"):
        give(2, FAR)
    with scope("keep2"):
        keep(2, FAR)
    with scope("give2r"):
        give(2, REST)
    with scope("pass1"):
        pass_on(1)
    with scope("keep2r"):
        keep(2, REST)
    with scope("pass2"):
        pass_on(2)
    with scope("final0"):
        low = lax.broadcasted_iota(jnp.int32, (TOK, 128), 1) < 64
        part0 = collect(0)
        turned = pltpu.roll(collect(1), 64, 1)
        out_ref[:, 0:128] = (RES[:, 0:128] + jnp.where(low, part0, turned)).astype(BF16)
        RES[:, 128:256] = RES[:, 128:256] + jnp.where(low, ACC[:, at_po(2, 3)], part0)
        RES[:, 256:384] = RES[:, 256:384] + jnp.where(low, turned, ACC[:, at_po(2, 3)])
    with scope("final"):
        l = pl.ds(256, 128)
        with scope("rv2"):
            recv(("rv", 2), RV.at[:, :, l])
        part2 = RV[0, :, l].astype(F32) + RV[1, :, l].astype(F32)
        out_ref[:, 128:256] = (RES[:, 128:256] + jnp.where(low, part2, 0.0)).astype(BF16)
        out_ref[:, 256:384] = (RES[:, 256:384] + jnp.where(low, 0.0, part2)).astype(BF16)
    with scope("sent"):
        sent("gv", W.at[pl.ds(0, 15 * HW), :])
        sent("dn", W.at[pl.ds(0, 15 * HW), pl.ds(0, MAIN)])
        mix_g[4]()
        x_g[4]()
        sent("w", WO.at[pl.ds(0, 7 * HW), :])
        sent("st", SR)
        sent("mt", MR)
        sent("q", SS.at[pl.ds(0, 7)])
        sent("e", EDGE)
        sent("sp", SP)
        sent("rl", RL)
        sent("rv", RV)
    if len(table) != SEMS:
        raise ValueError(len(table))


def body(
    resid,
    query,
    keys,
    values,
    out_gate,
    in_gate,
    forget,
    doc_ids,
    head_gain,
    w_out,
    ffn_gain,
    w_gate,
    w_value,
    conv_taps,
    w_down,
):
    vmem = pl.BlockSpec(memory_space=pltpu.VMEM)
    hbm = pl.BlockSpec(memory_space=pl.ANY)
    return pl.pallas_call(
        kernel,
        out_shape=pltpu.VMEM((TOK, OWN), BF16),
        in_specs=[hbm] * 15,
        out_specs=vmem,
        scratch_shapes=[
            pltpu.VMEM((3072, LANES), BF16),
            pltpu.VMEM((2, TOK), F32),
            pltpu.VMEM((2, TOK), F32),
            pltpu.VMEM((TOK,), jnp.int32),
            pltpu.VMEM((1, HW), F32),
            pltpu.VMEM((1, 3072), F32),
            pltpu.VMEM((3, 1056), F32),
            pltpu.VMEM((16 * PART, MAIN), BF16),
            pltpu.VMEM((16 * PART, MAIN), BF16),
            pltpu.VMEM((16 * PART, MAIN), BF16),
            pltpu.VMEM((3, HW, 32), BF16),
            pltpu.VMEM((TOK, 3072), BF16),
            pltpu.VMEM((1536, TOK), BF16),
            pltpu.VMEM((1536, OWN), BF16),
            pltpu.VMEM((OWN, 1536), BF16),
            pltpu.VMEM((HW, TOK), BF16),
            pltpu.VMEM((HW, TOK), BF16),
            pltpu.VMEM((HW, TOK), BF16),
            pltpu.VMEM((HW, TOK), BF16),
            pltpu.VMEM((TOK, OWN), BF16),
            pltpu.VMEM((HW, TOK), F32),
            pltpu.VMEM((TOK, 128), F32),
            pltpu.VMEM((HW, 128), BF16),
            pltpu.VMEM((4, HW, 128), BF16),
            pltpu.VMEM((8, 128), F32),
            pltpu.VMEM((4, 8, 128), F32),
            pltpu.VMEM((8, 8, TOK), F32),
            pltpu.VMEM((TOK, OWN), F32),
            pltpu.VMEM((TOK, LANES), F32),
            pltpu.VMEM((TOK, GW), BF16),
            pltpu.VMEM((16, GW), BF16),
            pltpu.VMEM((TOK, GW), BF16),
            pltpu.VMEM((4, TOK, OWN), BF16),
            pltpu.VMEM((4, TOK, OWN), BF16),
            pltpu.VMEM((3, TOK, OWN), BF16),
            pltpu.VMEM((2, OWN, OWN), BF16),
            pltpu.VMEM((2, TOK, OWN), BF16),
            pltpu.SemaphoreType.DMA((SEMS,)),
            pltpu.SemaphoreType.DMA((12,)),
        ],
        compiler_params=pltpu.CompilerParams(
            collective_id=0, has_side_effects=True, vmem_limit_bytes=VLIM * 1024 * 1024
        ),
    )(
        w_gate,
        w_value,
        w_down.T,
        query.T,
        keys.T,
        values.T,
        out_gate.T,
        w_out,
        resid,
        in_gate,
        forget,
        doc_ids,
        head_gain[None],
        ffn_gain[None],
        conv_taps,
    )


def solution(mesh):
    torus = Mesh(mesh.devices.reshape(4, 4, 4, 2), ("z", "x", "y", "c"))
    sp, tp = ("z", "x"), ("y", "c")
    placed = (
        P(sp, tp),
        P(sp, tp),
        P(sp, tp),
        P(sp, tp),
        P(sp, tp),
        P(tp, sp),
        P(tp, sp),
        P(sp),
        P(tp),
        P(tp, None),
        P(),
        P(sp, tp),
        P(sp, tp),
        P(None, tp),
        P(tp, sp),
    )
    return jax.shard_map(body, mesh=torus, in_specs=placed, out_specs=P(sp, tp), check_vma=False)
```

```python
import jax
import jax.numpy as jnp
from jax import lax
from jax.experimental import pallas as pl
from jax.experimental.pallas import tpu as pltpu
from jax.sharding import Mesh
from jax.sharding import PartitionSpec as P

MESH = pl.DeviceIdType.MESH
F32 = jnp.float32
BF16 = jnp.bfloat16
ABSENT = -1e30
DH = 96
TOK = 768
OWN = 384
HW = 192
MAIN = 1024
GW = 1152
LANES = 2176
PART = 64
EPS = 1e-6
EVERY, FAR, REST = (0, 1, 2, 3), (0,), (1, 2, 3)
VLIM = 60
SEMS = 61
scope = jax.named_scope


def mod4(v):
    return lax.rem(v + 8, 4)


def dot(a, b, **kw):
    return lax.dot_general(a, b, (((1,), (0,)), ((), ())), preferred_element_type=F32, **kw)


def dot_t(a, b, **kw):
    return lax.dot_general(a, b, (((1,), (1,)), ((), ())), preferred_element_type=F32, **kw)


def dot_c(a, b, **kw):
    return lax.dot_general(a, b, (((0,), (0,)), ((), ())), preferred_element_type=F32, **kw)


def kernel(
    wg_ref,
    wv_ref,
    wd_ref,
    q_hbm,
    k_hbm,
    v_hbm,
    og_hbm,
    wo_ref,
    resid_hbm,
    ig_hbm,
    fg_hbm,
    seg_hbm,
    hg_hbm,
    gain_hbm,
    taps_hbm,
    out_ref,
    W,
    ig_ref,
    fg_ref,
    seg_ref,
    hg_ref,
    gain_ref,
    taps_ref,
    WD0,
    WD1,
    WD2,
    TL,
    X,
    MIX,
    WO,
    WOT,
    QT,
    KT,
    VT,
    OG,
    RB,
    OI,
    NF,
    ST,
    SR,
    MT,
    MR,
    SS,
    RES,
    ACC,
    GT,
    EDGE,
    HD,
    SP,
    RP,
    ZS,
    RL,
    RV,
    sems,
    lsem,
):
    z, x = lax.axis_index("z"), lax.axis_index("x")
    y, c = lax.axis_index("y"), lax.axis_index("c")
    sp = z * 4 + x
    tp = y * 2 + c
    o = 1 - c
    table = {}
    rkey_any = "w"

    def slot(key):
        return table.setdefault(key, len(table))

    def copy(rkey, skey, src, dst, dev):
        return pltpu.make_async_remote_copy(
            src_ref=src,
            dst_ref=dst,
            send_sem=sems.at[slot(("S", skey))],
            recv_sem=sems.at[slot(("R", rkey))],
            device_id=dev,
            device_id_type=MESH,
        )

    def send(rkey, skey, src, dst, dev):
        copy(rkey, skey, src, dst, dev).start()

    partner = (z, x, y, o)

    def recv(rkey, span):
        copy(rkey, rkey_any, span, span, partner).wait_recv()

    def sent(skey, span):
        copy(rkey_any, skey, span, span, partner).wait_send()

    def at_sp(n):
        s = lax.rem(sp + n + 16, 16)
        return (s // 4, lax.rem(s, 4), y, c)

    def at_x(d):
        return (z, mod4(x + d), y, c)

    def at_z(d):
        return (mod4(z + d), x, y, c)

    def at_y(d):
        return (z, x, mod4(y + d), c)

    def at_tp(n):
        t = lax.rem(tp + n, 8)
        return (z, x, t // 2, lax.rem(t, 2))

    peers = [at_x(1), at_x(-1), at_z(1), at_z(-1)]
    peers += [at_tp(n) for n in range(1, 8)]
    peers += [at_sp(n) for n in (1, 2, 3, -1, -2, -3)]
    barrier = pltpu.get_barrier_semaphore()
    for dev in peers:
        pl.semaphore_signal(barrier, inc=1, device_id=dev, device_id_type=MESH)

    groups = ["main", "tail", "fg", "ig", "seg", "heads", "down", "hg", "gain", "taps", "resid", "wo"]

    def bring(group, src, dst):
        pltpu.make_async_copy(src, dst, lsem.at[groups.index(group)]).start()

    def landed(group, span):
        pltpu.make_async_copy(span, span, lsem.at[groups.index(group)]).wait()

    own_w = pl.ds(pl.multiple_of(sp * HW, 16), HW)
    bring("main", wg_ref.at[:, 0:MAIN], W.at[own_w, 0:MAIN])
    bring("main", wv_ref.at[:, 0:MAIN], W.at[own_w, GW:LANES])
    for n, ref in enumerate((wg_ref, wv_ref, wd_ref)):
        bring("tail", ref.at[:, MAIN : MAIN + 32], TL.at[n])
    bring("fg", fg_hbm, fg_ref)
    bring("ig", ig_hbm, ig_ref)
    bring("seg", seg_hbm, seg_ref)
    bring("heads", k_hbm, KT)
    bring("heads", v_hbm, VT)
    bring("heads", q_hbm, QT)
    bring("heads", og_hbm, OG)
    for n, ref in enumerate((WD0, WD1, WD2)):
        bring(
            "down",
            wd_ref.at[n * PART : (n + 1) * PART, 0:MAIN],
            ref.at[pl.ds(pl.multiple_of(sp * PART, 16), PART), :],
        )
    bring("hg", hg_hbm, hg_ref)
    bring("gain", gain_hbm, gain_ref)
    bring("taps", taps_hbm, taps_ref)
    bring("resid", resid_hbm, RB)
    bring(
        "wo",
        wo_ref.at[:, pl.ds(pl.multiple_of(tp * OWN, 128), OWN)],
        WO.at[pl.ds(pl.multiple_of(tp * HW, 16), HW), :],
    )

    def stage(gather, ref, stride, rows, lanes, by_lanes, first):
        x_first = first == "x"
        prim = at_x if x_first else at_z
        secd = at_z if x_first else at_x
        steps = (0, -1, 1, 2)
        group = "gv" if ref is W else "dn"

        def place(dp, ds, half=None, shift=0):
            zz, xx = (mod4(z + ds), mod4(x + dp)) if x_first else (mod4(z + dp), mod4(x + ds))
            (r0, nr), (l0, nl) = rows, lanes
            if half is not None and by_lanes:
                l0, nl = l0 + half * nl // 2, nl // 2
            elif half is not None:
                upper = nr // 2 - shift
                r0, nr = (r0 + upper, nr - upper) if half else (r0, upper)
            row = pl.multiple_of((zz * 4 + xx) * stride + r0, 16)
            return ref.at[pl.ds(row, nr), pl.ds(l0, nl)]

        def primary():
            for d in (1, -1):
                send((gather, "p"), group, place(0, 0), place(0, 0), prim(d))

        def second(m):
            p = place(steps[m], 0)
            for d in (1, -1):
                send((gather, "s", m), group, p, p, secd(d))

        def relay():
            for d in (1, -1):
                p = place(-d, 0, 0 if d == 1 else 1)
                send((gather, "pf"), group, p, p, prim(d))

        def across(m):
            for d in (1, -1):
                p = place(steps[m], -d, 0 if d == 1 else 1, 16 if m == 1 else 0)
                send((gather, "sf"), group, p, p, secd(d))

        def far():
            second(3)

        return primary, second, relay, across, far

    awaited = {"relay": ("p", 2), "across": ("s", 2), "far": ("pf", 1), "done": ("sf", 4)}

    def run(gather, what, *args, only=(0, 1)):
        name, ref, rows, parts = gather
        if what in awaited:
            tag, count = awaited[what]
            recv((name, tag, *args), ref.at[pl.ds(0, count * rows), :])
        if what != "done":
            k = ("primary", "second", "relay", "across", "far").index(what)
            for n in only:
                parts[n][k](*args)

    gv = (
        "gv",
        W,
        HW,
        (
            stage("gv", W, HW, (0, HW), (0, GW), False, "x"),
            stage("gv", W, HW, (0, HW), (GW, MAIN), False, "z"),
        ),
    )

    def down_stage(n, ref, cut):
        parts = (
            stage(n, ref, PART, (0, cut), (0, MAIN), True, "x"),
            stage(n, ref, PART, (cut, PART - cut), (0, MAIN), True, "z"),
        )
        return n, ref, PART, parts

    d0, d1, d2 = down_stage(0, WD0, 16), down_stage(1, WD1, 32), down_stage(2, WD2, 32)

    def over_tp(name, blk, span):
        def g0():
            b = blk(y, c)
            for d in (1, -1):
                send((name, "y"), name, b, b, at_y(d))
            send((name, "o"), name, b, b, partner)

        def g1():
            recv((name, "y"), span(2))
            for d in (1, -1):
                h = blk(mod4(y - d), c, 0 if d == 1 else 1)
                send((name, "f"), name, h, h, at_y(d))
            for d in (1, -1):
                b = blk(mod4(y - d), c)
                send((name, "o"), name, b, b, partner)

        def g2():
            recv((name, "f"), span(1))
            b = blk(mod4(y + 2), c)
            send((name, "o"), name, b, b, partner)

        def g3():
            recv((name, "o"), span(4))

        def out():
            sent(name, span(7))

        return g0, g1, g2, g3, out

    def mix_block(yy, cc, half=None):
        r0, nr = (0, HW) if half is None else (half * DH, DH)
        return MIX.at[pl.ds(pl.multiple_of((yy * 2 + cc) * HW + r0, 16), nr), :]

    def x_block(yy, cc, half=None):
        rows = slice(None) if half is None else pl.ds(half * OWN, OWN)
        return X.at[rows, pl.ds(pl.multiple_of((yy * 2 + cc) * OWN, 128), OWN)]

    mix_g = over_tp("m", mix_block, lambda k: MIX.at[pl.ds(0, k * HW), :])
    x_g = over_tp("x", x_block, lambda k: X.at[:, pl.ds(0, k * OWN)])

    landed("main", W.at[0 : 2 * HW, 0:MAIN])
    landed("tail", TL)
    tails = jnp.concatenate([TL[0], TL[1], TL[2], jnp.zeros((HW, 32), BF16)], axis=1)
    W[own_w, MAIN:GW] = tails
    with scope("barrier"):
        pl.semaphore_wait(barrier, len(peers))
    run(gv, "primary", only=(1, 0))
    for n in range(1, 8):
        t = lax.rem(tp + n, 8)
        src = wo_ref.at[:, pl.ds(pl.multiple_of(t * OWN, 128), OWN)]
        dst = WO.at[pl.ds(pl.multiple_of(tp * HW, 16), HW), :]
        send("w", "w", src, dst, at_tp(n))

    lane = lax.broadcasted_iota(jnp.int32, (8, TOK), 1)
    row8 = lax.broadcasted_iota(jnp.int32, (8, TOK), 0)
    landed("fg", fg_ref)
    landed("ig", ig_ref)
    landed("seg", seg_ref)
    seg = seg_ref[...].reshape(1, TOK).astype(F32)
    fg = jnp.where(row8 == 0, fg_ref[0:1], fg_ref[1:2])
    e = jnp.exp(-jnp.abs(fg))
    log1p = jnp.where(e < 1e-2, e * (1.0 - e * (0.5 - e * (1.0 / 3.0))), jnp.log(1.0 + e))
    cum = jnp.minimum(fg, 0.0) - log1p
    shift = 1
    while shift < TOK:
        cum = cum + jnp.where(lane >= shift, pltpu.roll(cum, shift, 1), 0.0)
        shift *= 2
    b = [ig_ref[h : h + 1] - cum[h : h + 1] for h in range(2)]
    end = [cum[h : h + 1, TOK - 1 :] for h in range(2)]
    first, last, second_last = seg[:, :1], seg[:, TOK - 1 :], seg[:, TOK - 2 : TOK - 1]
    landed("heads", MIX.at[0 : 4 * HW, :])
    peak, made = [], []
    for h in range(2):
        hs = slice(h * DH, h * DH + DH)
        top = jnp.max(jnp.where(seg == last, b[h], ABSENT), axis=1, keepdims=True)
        peak.append(top)
        w = jnp.where(seg == last, jnp.exp(jnp.minimum(b[h] - top, 0.0)), 0.0) * DH**-0.5
        made.append(
            jnp.concatenate(
                [dot_t(VT[hs, :], (KT[hs, :].astype(F32) * w).astype(BF16)), jnp.zeros((DH, 32), F32)],
                axis=1,
            )
        )
    lane96 = lax.broadcasted_iota(jnp.int32, (DH, 128), 1)
    lane48 = lax.broadcasted_iota(jnp.int32, (48, 128), 1)
    turned1 = pltpu.roll(made[1], 96, 1)
    ST[0:DH, :] = jnp.where(lane96 < DH, made[0], turned1).astype(BF16)
    ST[DH:144, :] = jnp.where(lane48 < 64, turned1[0:48], pltpu.roll(turned1[48:96], 64, 1)).astype(BF16)
    meta_row = lax.broadcasted_iota(jnp.int32, (8, 128), 0)
    meta = jnp.zeros((8, 128), F32)
    for n, value in enumerate((end[0] + peak[0], end[1] + peak[1], end[0], end[1], first, last, second_last)):
        meta = jnp.where(meta_row == n, value, meta)
    MT[...] = meta
    for n in range(1, 5):
        send("st", "st", ST, SR.at[n - 1], at_sp(n))
        send("mt", "mt", MT, MR.at[n - 1], at_sp(n))
    run(gv, "second", 0)

    rows = jnp.where(row8 == 0, b[0], jnp.where(row8 == 1, b[1], seg))
    cols = jnp.transpose(jnp.concatenate([rows, jnp.zeros((120, TOK), F32)], axis=0))
    seg_c = cols[:, 2:3]
    tops = [[], []]
    for i in range(3):
        t0, ns = i * 256, (i + 1) * 256
        ts = slice(t0, t0 + 256)
        s_at = lax.broadcasted_iota(jnp.int32, (ns, 256), 0)
        t_at = lax.broadcasted_iota(jnp.int32, (ns, 256), 1) + t0
        mask = (seg_c[:ns] == seg[:, ts]) & (s_at <= t_at)
        for h in range(2):
            hs = slice(h * DH, h * DH + DH)
            masked = jnp.where(mask, cols[:ns, h : h + 1], ABSENT)
            top = jnp.max(masked, axis=0, keepdims=True)
            scores = dot_c(KT[hs, 0:ns], QT[hs, ts]) * (jnp.exp(masked - top) * DH**-0.5)
            OI[hs, ts] = dot(VT[hs, 0:ns], scores.astype(BF16))
            tops[h].append(top)

    with scope("relay"):
        run(gv, "relay")
        run(gv, "second", 1)
        run(gv, "second", 2)

    dec = [jnp.zeros((1, 128), F32)] * 2
    cand = [[], []]
    first_l = jnp.broadcast_to(first, (1, 128))
    with scope("state"):
        recv("st", SR)
        recv("mt", MR)
    for n in range(1, 5):
        m = MR[n - 1]
        valid = (m[5:6] == first_l) & (sp >= n)
        for h in range(2):
            cand[h].append(jnp.where(valid, m[h : h + 1] + dec[h], ABSENT))
            dec[h] = dec[h] + m[2 + h : 3 + h]
    landed("down", WD0.at[0:HW, :])
    landed("hg", hg_ref)
    landed("gain", gain_ref)
    landed("taps", taps_ref)
    gain_at = lax.broadcasted_iota(jnp.int32, (HW, HW), 0) == lax.broadcasted_iota(jnp.int32, (HW, HW), 1)
    gain_c = jnp.sum(jnp.where(gain_at, hg_ref[...], 0.0), axis=1, keepdims=True)
    pins = [
        jnp.maximum(jnp.maximum(p[0], p[1]), jnp.maximum(p[2], p[3])) for p in cand
    ]
    upper, lower = jnp.zeros((DH, 128), F32), jnp.zeros((48, 128), F32)
    for n in range(4):
        f0, f1 = jnp.exp(cand[0][n] - pins[0]), jnp.exp(cand[1][n] - pins[1])
        upper = upper + jnp.where(lane96 < DH, f0, f1) * SR[n, 0:DH, :].astype(F32)
        lower = lower + f1 * SR[n, DH:144, :].astype(F32)
    lower = jnp.concatenate([lower, pltpu.roll(lower, 64, 1)], axis=0)
    second_state = jnp.where(lane96 >= DH, upper, jnp.where(lane96 < 64, lower, 0.0))
    states = [upper, pltpu.roll(second_state, 32, 1)]
    for h in range(2):
        hs = slice(h * DH, h * DH + DH)
        pin = pins[h]
        inter = dot(states[h][:, 0:DH].astype(BF16), QT[hs, :])
        m_in = jnp.concatenate(tops[h], axis=1)
        m_pin = jnp.where(seg == first, pin[:, :1], ABSENT)
        m_all = jnp.maximum(m_in, m_pin)
        memory = jnp.exp(m_in - m_all) * OI[hs, :] + jnp.exp(m_pin - m_all) * inter
        mean = jnp.sum(memory * memory, axis=0, keepdims=True) * (1.0 / DH)
        mix = memory * lax.rsqrt(mean + 1.0) * gain_c[hs] * jax.nn.sigmoid(OG[hs, :].astype(F32))
        MIX[pl.ds(pl.multiple_of(tp * HW + h * DH, 16), DH), :] = mix.astype(BF16)
    with scope("mix0"):
        mix_g[0]()
    with scope("across0"):
        run(gv, "across", 0)

    before = MR[0]
    there = sp >= 1
    last_before = jnp.where(there, before[5:6, :1], -1.0)
    second_before = jnp.where(there, before[6:7, :1], -1.0)
    seg8 = jnp.broadcast_to(seg, (8, TOK))
    one_back = jnp.where(lane == 0, last_before, pltpu.roll(seg8, 1, 1))
    two_back = jnp.where(
        lane == 0, second_before, jnp.where(lane == 1, last_before, pltpu.roll(seg8, 2, 1))
    )
    flags = jnp.where(
        row8 == 0, jnp.where(one_back == seg, 1.0, 0.0), jnp.where(two_back == seg, 1.0, 0.0)
    )
    NF[...] = jnp.transpose(jnp.concatenate([flags, jnp.zeros((120, TOK), F32)], axis=0))
    with scope("wo"):
        landed("resid", RB)
        landed("wo", WO.at[0:HW, :])
        recv("w", WO.at[pl.ds(0, 7 * HW), :])
        WOT[...] = jnp.transpose(WO[...])

    with scope("mix1"):
        mix_g[1]()
    with scope("far"):
        run(gv, "far")
    with scope("mix2"):
        mix_g[2]()
    with scope("mix3"):
        mix_g[3]()

    gain = gain_ref[:, pl.ds(pl.multiple_of(tp * OWN, 128), OWN)]
    res = RB[...].astype(F32) + jnp.transpose(dot(WOT[...], MIX[...]))
    RES[...] = res
    X[:, pl.ds(pl.multiple_of(tp * OWN, 128), OWN)] = (res * gain).astype(BF16)
    x_g[0]()
    SS[tp] = dot_t(jnp.ones((8, OWN), F32), res * res, precision=lax.Precision.HIGHEST)
    for n in range(1, 8):
        send("q", "q", SS.at[tp], SS.at[tp], at_tp(n))
    with scope("across1"):
        run(gv, "across", 1)
    with scope("across2"):
        run(gv, "across", 2)
    with scope("x1"):
        x_g[1]()
    with scope("x2"):
        x_g[2]()
    with scope("x3"):
        x_g[3]()
    run(d0, "primary")
    run(d0, "second", 0)
    with scope("across3"):
        run(gv, "across", 3)
    with scope("sq"):
        recv("q", SS.at[pl.ds(0, 7)])
        total = SS[0]
        for n in range(1, 8):
            total = total + SS[n]
    scale_row = lax.rsqrt(total * (1.0 / 3072.0) + EPS)
    NF[:, 2:3] = jnp.transpose(jnp.concatenate([scale_row, jnp.zeros((120, TOK), F32)], axis=0))[:, 0:1]

    def tile256(n, at):
        return pl.ds(pl.multiple_of(n * 256 + at, 128), 256)

    def by_row(lanes, steps):
        acc = None
        for d in steps:
            k = pl.ds(pl.multiple_of(mod4(z + d) * 768, 128), 768)
            part = dot(X[:, k], W[k, lanes])
            acc = part if acc is None else acc + part
        return acc

    def by_pair(lanes, which):
        acc = None
        for zz in range(4):
            k = pl.ds(pl.multiple_of(zz * 768 + which * OWN, 128), OWN)
            part = dot(X[:, k], W[k, lanes])
            acc = part if acc is None else acc + part
        return acc

    here = x // 2
    with scope("partial"):

        def early(n, _):
            ACC[:, tile256(n, 0)] = by_row(tile256(n, 0), (0, 1, -1))
            ACC[:, tile256(n, GW)] = by_pair(tile256(n, GW), here)
            return 0

        lax.fori_loop(0, 4, early, 0)
        ACC[:, MAIN:GW] = by_row(slice(MAIN, GW), (0, 1, -1))

    with scope("d0relay"):
        run(d0, "relay")
        run(d0, "second", 1)
        run(d0, "second", 2)
        run(d1, "primary")
        run(d1, "second", 0)
    with scope("done"):
        run(gv, "done")
    with scope("p1"):
        run(d0, "across", 0)
        run(d0, "far")
    scale = NF[:, 2:3]
    with scope("gate"):

        def gate_tile(n, _):
            l = tile256(n, 0)
            GT[:, l] = ((ACC[:, l] + by_row(l, (2,))) * scale).astype(BF16)
            return 0

        lax.fori_loop(0, 4, gate_tile, 0)
        l = slice(MAIN, GW)
        GT[:, l] = ((ACC[:, l] + by_row(l, (2,))) * scale).astype(BF16)
    send("e", "e", GT.at[TOK - 16 : TOK, :], EDGE, at_sp(1))
    with scope("p2"):
        run(d0, "across", 1)
        run(d0, "across", 2)

    def hidden_of(lanes, width, taps, value):
        g = GT[:, lanes].astype(F32)
        edge = EDGE[:, lanes].astype(F32)
        t_at = lax.broadcasted_iota(jnp.int32, (TOK, width), 0)
        near = NF[:, 0:1] > 0.5
        far = NF[:, 1:2] > 0.5
        g1 = jnp.where(t_at == 0, edge[15:16], pltpu.roll(g, 1, 0))
        g2 = jnp.where(
            t_at == 0, edge[14:15], jnp.where(t_at == 1, edge[15:16], pltpu.roll(g, 2, 0))
        )
        conv = taps[2:3] * g + taps[1:2] * jnp.where(near, g1, 0.0) + taps[0:1] * jnp.where(far, g2, 0.0)
        return conv / (1.0 + jnp.exp(-conv)) * value

    def value_sum(n, _):
        l = tile256(n, GW)
        ACC[:, l] = ACC[:, l] + by_pair(l, 1 - here)
        return 0

    with scope("value"):
        lax.fori_loop(0, 2, value_sum, 0)
    with scope("p3"):
        run(d1, "relay")
    with scope("value"):
        lax.fori_loop(2, 4, value_sum, 0)
    with scope("p4"):
        run(d0, "across", 3)
        run(d2, "primary")
        run(d2, "second", 0)
        run(d1, "second", 1)
        run(d1, "second", 2)
        run(d1, "across", 0)
    with scope("edge"):
        recv("e", EDGE)

    with scope("hidden"):

        def hidden_tile(n, _):
            value = (ACC[:, tile256(n, GW)] * scale).astype(BF16).astype(F32)
            l = tile256(n, 0)
            HD[:, l] = hidden_of(l, 256, taps_ref[:, l], value).astype(BF16)
            return 0

        lax.fori_loop(0, 4, hidden_tile, 0)
        tail = slice(MAIN, GW)
        taps_tail = jnp.concatenate([taps_ref[:, MAIN : MAIN + 32], jnp.zeros((3, 96), F32)], axis=1)
        value_tail = pltpu.roll(GT[:, tail].astype(F32), 96, 1)
        HD[:, tail] = pltpu.roll(hidden_of(tail, 128, taps_tail, value_tail), 64, 1).astype(BF16)
    with scope("p5"):
        run(d1, "far")
        run(d0, "done")

    downs = (WD0, WD1, WD2)

    def partials(p, cc, which):
        mains, ends = [], []
        for n in which:
            j = mod4(y + order[n]) * 2 + cc
            mains.append(downs[p][pl.ds(pl.multiple_of(j * 128, 128), 128), :])
            for k in range(2):
                at = pl.multiple_of((j * 2 + k) * HW + p * PART, 16)
                ends.append(W[pl.ds(at, PART), MAIN:GW])
        return dot_t(HD[:, 0:MAIN], jnp.concatenate(mains, axis=0)) + dot_t(
            HD[:, MAIN:GW], jnp.concatenate(ends, axis=0)
        )

    order = (2, 1, -1, 0)

    def at_po(p, m):
        return pl.ds(m * OWN + p * 128, 128)

    def give(p, which):
        l = pl.ds(p * 128, 128)
        both = partials(p, o, which).astype(BF16)
        for k, n in enumerate(which):
            SP[n, :, l] = both[:, k * 128 : (k + 1) * 128]
            send(("sp", p, which), "sp", SP.at[n, :, l], RP.at[n, :, l], partner)

    def keep(p, which):
        l = pl.ds(p * 128, 128)
        mine = partials(p, c, which)
        with scope("sp"):
            recv(("sp", p, which), RP.at[pl.ds(which[0], len(which)), :, l])
        for k, n in enumerate(which):
            d = order[n]
            both = mine[:, k * 128 : (k + 1) * 128] + RP[n, :, l].astype(F32)
            if d == 2:
                ZS[0, :, l] = both.astype(BF16)
                send(("rl", p), "rl", ZS.at[0, pl.ds(0, OWN), l], RL.at[0, :, l], at_y(1))
                send(("rl", p), "rl", ZS.at[0, pl.ds(OWN, OWN), l], RL.at[1, :, l], at_y(-1))
            else:
                ACC[:, at_po(p, n)] = both
                if d != 0:
                    r = pl.ds(OWN if d == 1 else 0, OWN)
                    ZS[n, r, l] = both[OWN:, :].astype(BF16) if d == 1 else both[:OWN, :].astype(BF16)
                    send(("rv", p), "rv", ZS.at[n, r, l], RV.at[n - 1, r, l], at_y(d))

    def pass_on(p):
        l = pl.ds(p * 128, 128)
        with scope("rl"):
            recv(("rl", p), RL.at[:, :, l])
        for n, d in ((1, 1), (2, -1)):
            r = pl.ds(0 if d == 1 else OWN, OWN)
            ZS[n, r, l] = (ACC[r, at_po(p, n)] + RL[n - 1, :, l].astype(F32)).astype(BF16)
            send(("rv", p), "rv", ZS.at[n, r, l], RV.at[n - 1, r, l], at_y(d))

    def collect(p):
        l = pl.ds(p * 128, 128)
        with scope("rv%d" % p):
            recv(("rv", p), RV.at[:, :, l])
        return ACC[:, at_po(p, 3)] + RV[0, :, l].astype(F32) + RV[1, :, l].astype(F32)

    with scope("give0"):
        give(0, EVERY)
    with scope("p6"):
        run(d2, "relay")
        run(d2, "second", 1)
        run(d1, "across", 1)
    with scope("keep0"):
        keep(0, EVERY)
    with scope("p7"):
        run(d1, "across", 2)
        run(d1, "across", 3)
        run(d2, "second", 2)
        run(d2, "far")
        run(d2, "across", 0)
    with scope("p8"):
        run(d2, "across", 1)
        run(d1, "done")
    with scope("give1"):
        give(1, EVERY)
    with scope("p8b"):
        run(d2, "across", 2)
        run(d2, "across", 3)
    with scope("pass0"):
        pass_on(0)
    with scope("keep1"):
        keep(1, EVERY)
    with scope("p10"):
        run(d2, "done")
    with scope("give2"):
        give(2, FAR)
    with scope("keep2"):
        keep(2, FAR)
    with scope("give2r"):
        give(2, REST)
    with scope("pass1"):
        pass_on(1)
    with scope("keep2r"):
        keep(2, REST)
    with scope("pass2"):
        pass_on(2)
    with scope("final0"):
        low = lax.broadcasted_iota(jnp.int32, (TOK, 128), 1) < 64
        part0 = collect(0)
        turned = pltpu.roll(collect(1), 64, 1)
        out_ref[:, 0:128] = (RES[:, 0:128] + jnp.where(low, part0, turned)).astype(BF16)
        RES[:, 128:256] = RES[:, 128:256] + jnp.where(low, ACC[:, at_po(2, 3)], part0)
        RES[:, 256:384] = RES[:, 256:384] + jnp.where(low, turned, ACC[:, at_po(2, 3)])
    with scope("final"):
        l = pl.ds(256, 128)
        with scope("rv2"):
            recv(("rv", 2), RV.at[:, :, l])
        part2 = RV[0, :, l].astype(F32) + RV[1, :, l].astype(F32)
        out_ref[:, 128:256] = (RES[:, 128:256] + jnp.where(low, part2, 0.0)).astype(BF16)
        out_ref[:, 256:384] = (RES[:, 256:384] + jnp.where(low, 0.0, part2)).astype(BF16)
    with scope("sent"):
        sent("gv", W.at[pl.ds(0, 15 * HW), :])
        sent("dn", W.at[pl.ds(0, 15 * HW), pl.ds(0, MAIN)])
        mix_g[4]()
        x_g[4]()
        sent("w", WO.at[pl.ds(0, 7 * HW), :])
        sent("st", SR)
        sent("mt", MR)
        sent("q", SS.at[pl.ds(0, 7)])
        sent("e", EDGE)
        sent("sp", SP)
        sent("rl", RL)
        sent("rv", RV)
    if len(table) != SEMS:
        raise ValueError(len(table))


def body(
    resid,
    query,
    keys,
    values,
    out_gate,
    in_gate,
    forget,
    doc_ids,
    head_gain,
    w_out,
    ffn_gain,
    w_gate,
    w_value,
    conv_taps,
    w_down,
):
    vmem = pl.BlockSpec(memory_space=pltpu.VMEM)
    hbm = pl.BlockSpec(memory_space=pl.ANY)
    return pl.pallas_call(
        kernel,
        out_shape=pltpu.VMEM((TOK, OWN), BF16),
        in_specs=[hbm] * 15,
        out_specs=vmem,
        scratch_shapes=[
            pltpu.VMEM((3072, LANES), BF16),
            pltpu.VMEM((2, TOK), F32),
            pltpu.VMEM((2, TOK), F32),
            pltpu.VMEM((TOK,), jnp.int32),
            pltpu.VMEM((1, HW), F32),
            pltpu.VMEM((1, 3072), F32),
            pltpu.VMEM((3, 1056), F32),
            pltpu.VMEM((16 * PART, MAIN), BF16),
            pltpu.VMEM((16 * PART, MAIN), BF16),
            pltpu.VMEM((16 * PART, MAIN), BF16),
            pltpu.VMEM((3, HW, 32), BF16),
            pltpu.VMEM((TOK, 3072), BF16),
            pltpu.VMEM((1536, TOK), BF16),
            pltpu.VMEM((1536, OWN), BF16),
            pltpu.VMEM((OWN, 1536), BF16),
            pltpu.VMEM((HW, TOK), BF16),
            pltpu.VMEM((HW, TOK), BF16),
            pltpu.VMEM((HW, TOK), BF16),
            pltpu.VMEM((HW, TOK), BF16),
            pltpu.VMEM((TOK, OWN), BF16),
            pltpu.VMEM((HW, TOK), F32),
            pltpu.VMEM((TOK, 128), F32),
            pltpu.VMEM((144, 128), BF16),
            pltpu.VMEM((4, 144, 128), BF16),
            pltpu.VMEM((8, 128), F32),
            pltpu.VMEM((4, 8, 128), F32),
            pltpu.VMEM((8, 8, TOK), F32),
            pltpu.VMEM((TOK, OWN), F32),
            pltpu.VMEM((TOK, LANES), F32),
            pltpu.VMEM((TOK, GW), BF16),
            pltpu.VMEM((16, GW), BF16),
            pltpu.VMEM((TOK, GW), BF16),
            pltpu.VMEM((4, TOK, OWN), BF16),
            pltpu.VMEM((4, TOK, OWN), BF16),
            pltpu.VMEM((3, TOK, OWN), BF16),
            pltpu.VMEM((2, OWN, OWN), BF16),
            pltpu.VMEM((2, TOK, OWN), BF16),
            pltpu.SemaphoreType.DMA((SEMS,)),
            pltpu.SemaphoreType.DMA((12,)),
        ],
        compiler_params=pltpu.CompilerParams(
            collective_id=0, has_side_effects=True, vmem_limit_bytes=VLIM * 1024 * 1024
        ),
    )(
        w_gate,
        w_value,
        w_down.T,
        query.T,
        keys.T,
        values.T,
        out_gate.T,
        w_out,
        resid,
        in_gate,
        forget,
        doc_ids,
        head_gain[None],
        ffn_gain[None],
        conv_taps,
    )


def solution(mesh):
    torus = Mesh(mesh.devices.reshape(4, 4, 4, 2), ("z", "x", "y", "c"))
    sp, tp = ("z", "x"), ("y", "c")
    placed = (
        P(sp, tp),
        P(sp, tp),
        P(sp, tp),
        P(sp, tp),
        P(sp, tp),
        P(tp, sp),
        P(tp, sp),
        P(sp),
        P(tp),
        P(tp, None),
        P(),
        P(sp, tp),
        P(sp, tp),
        P(None, tp),
        P(tp, sp),
    )
    return jax.shard_map(body, mesh=torus, in_specs=placed, out_specs=P(sp, tp), check_vma=False)
```
